128 devices in a mesh: pp: 4 (over x), fs: 4 (over y), tp: 8 (over z, core).
Axes of the slice: x: 4, y: 4, z: 4, core: 2. Of those that a mesh axis runs over, the one named last changes fastest.
Arguments:
- micro_in: bfloat16 [2, 96, 1024], P(None, 'pp', ('tp', 'fs')), may hold values from -6 to 6
- norm_gain: float32 [4, 1024], P('pp'), may hold values from 0.5 to 1.5
- proj_gate: bfloat16 [4, 1024, 8, 4, 64], P('pp', None, 'tp', 'fs'), may hold values from -0.1875 to 0.1875
- proj_value: bfloat16 [4, 1024, 8, 4, 64], P('pp', None, 'tp', 'fs'), may hold values from -0.1875 to 0.1875
- proj_write: bfloat16 [4, 1024, 8, 128], P('pp', None, 'tp'), may hold values from -0.1875 to 0.1875
- proj_read: bfloat16 [4, 1024, 8, 128], P('pp', None, 'tp'), may hold values from -0.1875 to 0.1875
- proj_step: bfloat16 [4, 1024, 2, 8, 4], P('pp', None, None, 'tp', 'fs'), may hold values from -0.1875 to 0.1875
- step_bias: float32 [4, 2, 8, 4], P('pp', None, 'tp', 'fs'), may hold values from -4.6 to -2.3
- decay_log: float32 [4, 2, 8, 4], P('pp', None, 'tp', 'fs'), may hold values from 0 to 2.77
- skip_gain: float32 [4, 8, 4], P('pp', 'tp', 'fs'), may hold values from 0.5 to 1.5
- conv_value: float32 [4, 5, 8, 4, 64], P('pp', None, 'tp', 'fs'), may hold values from -2.5 to 2.5
- conv_write: float32 [4, 5, 8, 128], P('pp', None, 'tp'), may hold values from -2.5 to 2.5
- conv_read: float32 [4, 5, 8, 128], P('pp', None, 'tp'), may hold values from -2.5 to 2.5
- proj_out: bfloat16 [4, 8, 4, 64, 1024], P('pp', 'tp', 'fs'), may hold values from -0.125 to 0.125
Outputs:
- mixed_out: bfloat16 [2, 96, 1024], P(None, 'pp', ('tp', 'fs'))
The draws below stay inside these ranges and needn't reach their ends.
All inputs are finite; a program needn't handle non-finite values.
Results may differ from the reference program's by a relative error of at most 0.025.
Values may be sent and summed in bfloat16 or wider, within the bound.
No kernel may reach another device: no remote copies, remote signals or barrier semaphores. Data moves between devices by JAX's collectives and lax.ppermute only.
A program may use at most 64 MiB of HBM per device.

```python
import jax
import jax.numpy as jnp
from jax import lax

D = 1024
GROUPS = 8
PER_GROUP = 4
HEAD = 64
STATE = 128
TAPS = 5
TOK = 96
SECTIONS = 4
MICRO = 2
INNER = 2048


def block_scale(key, shape, pieces, low, top_value):
    factor_of, own = 1.0, jax.random.fold_in(key, 6)
    for dim, shards_of in pieces:
        steps = jnp.exp(jax.random.uniform(jax.random.fold_in(own, dim), (shards_of,), jnp.float32, low / len(pieces), top_value / len(pieces)))
        factor_of = factor_of * jnp.repeat(steps, shape[dim] // shards_of).reshape([-1 if axis == dim else 1 for axis in range(len(shape))])
    return factor_of


def gaussian(stream_key, extent, scale, limit, split=(), held_as=jnp.bfloat16):
    factor_of = block_scale(stream_key, extent, split, -0.22, 0.18) if split else 1.0
    entries = jax.random.normal(stream_key, extent, jnp.float32) * scale * factor_of
    return jnp.minimum(jnp.maximum(entries, -limit), limit).astype(held_as)


def setup_inputs(seed: int = 0) -> dict:
    key_of = jax.random.split(jax.random.key(seed), 15)
    return {
        "micro_in": gaussian(key_of[0], (MICRO, TOK, D), 1.0, 6.0, ((1, 4), (2, 32))),
        "norm_gain": jnp.clip(1.0 + 0.1 * jax.random.normal(key_of[1], (SECTIONS, D), jnp.float32), 0.5, 1.5),
        "proj_gate": gaussian(key_of[2], (SECTIONS, D, GROUPS, PER_GROUP, HEAD), D ** -0.5, 0.1875, ((0, 4), (2, 8), (3, 4))),
        "proj_value": gaussian(key_of[3], (SECTIONS, D, GROUPS, PER_GROUP, HEAD), D ** -0.5, 0.1875, ((0, 4), (2, 8), (3, 4))),
        "proj_write": gaussian(key_of[4], (SECTIONS, D, GROUPS, STATE), D ** -0.5, 0.1875, ((0, 4), (2, 8))),
        "proj_read": gaussian(key_of[5], (SECTIONS, D, GROUPS, STATE), D ** -0.5, 0.1875, ((0, 4), (2, 8))),
        "proj_step": gaussian(key_of[6], (SECTIONS, D, 2, GROUPS, PER_GROUP), D ** -0.5, 0.1875, ((0, 4), (3, 8), (4, 4))),
        "step_bias": jnp.clip(-4.6 + 2.3 * jax.random.uniform(key_of[7], (SECTIONS, 2, GROUPS, PER_GROUP), jnp.float32) ** block_scale(key_of[7], (SECTIONS, 2, GROUPS, PER_GROUP), ((0, 4), (2, 8), (3, 4)), -0.2, 0.2), -4.6, -2.3),
        "decay_log": jnp.clip(2.77 * jax.random.uniform(key_of[8], (SECTIONS, 2, GROUPS, PER_GROUP), jnp.float32) ** block_scale(key_of[8], (SECTIONS, 2, GROUPS, PER_GROUP), ((0, 4), (2, 8), (3, 4)), -0.2, 0.2), 0.0, 2.77),
        "skip_gain": jnp.clip(1.0 + 0.1 * jax.random.normal(key_of[9], (SECTIONS, GROUPS, PER_GROUP), jnp.float32), 0.5, 1.5),
        "conv_value": gaussian(key_of[10], (SECTIONS, TAPS, GROUPS, PER_GROUP, HEAD), TAPS ** -0.5, 2.5, ((0, 4), (2, 8), (3, 4)), jnp.float32),
        "conv_write": gaussian(key_of[11], (SECTIONS, TAPS, GROUPS, STATE), TAPS ** -0.5, 2.5, ((0, 4), (2, 8)), jnp.float32),
        "conv_read": gaussian(key_of[12], (SECTIONS, TAPS, GROUPS, STATE), TAPS ** -0.5, 2.5, ((0, 4), (2, 8)), jnp.float32),
        "proj_out": gaussian(key_of[13], (SECTIONS, GROUPS, PER_GROUP, HEAD, D), INNER ** -0.5, 0.125, ((0, 4), (1, 8), (2, 4))),
    }


epsilon = 1e-06

def centred_conv(signal, conv_taps):
    span_width = conv_taps.shape[0]
    half_width = span_width // 2
    length = signal.shape[0]
    padded = jnp.pad(signal, ((half_width, half_width), (0, 0)))
    running = jnp.zeros_like(signal)
    for offset in range(span_width):
        running = running + padded[offset:offset + length] * conv_taps[offset]
    return running

def duality_mix(gate_flat, value_flat, write_flat, read_flat, step_raw, step_bias, decay_log, skip_gain, conv_value, conv_write, conv_read):
    groups, per_group = skip_gain.shape
    length = gate_flat.shape[0]
    head_size = value_flat.shape[1] // (groups * per_group)
    state_size = write_flat.shape[1] // groups
    taps_count = conv_value.shape[0]
    value_act = jax.nn.silu(centred_conv(value_flat.astype(jnp.float32), conv_value.reshape(taps_count, -1))).astype(jnp.bfloat16)
    write_act = jax.nn.silu(centred_conv(write_flat.astype(jnp.float32), conv_write.reshape(taps_count, -1))).astype(jnp.bfloat16)
    read_act = jax.nn.silu(centred_conv(read_flat.astype(jnp.float32), conv_read.reshape(taps_count, -1))).astype(jnp.bfloat16)
    step_size = jax.nn.softplus(step_raw.reshape(length, 2, groups, per_group) + step_bias[None])
    log_decay = step_size * (-jnp.exp(decay_log))[None]
    fwd_cum = jnp.cumsum(log_decay[:, 0], axis=0)
    bwd_cum = jnp.flip(jnp.cumsum(jnp.flip(log_decay[:, 1], 0), axis=0), 0)
    positions = jnp.arange(length)
    lower_mask = (positions[:, None] >= positions[None, :])[:, :, None, None]
    upper_mask = (positions[:, None] <= positions[None, :])[:, :, None, None]
    fwd_weight = jnp.exp(jnp.where(lower_mask, fwd_cum[:, None] - fwd_cum[None, :], -jnp.inf)) * step_size[None, :, 0]
    bwd_weight = jnp.exp(jnp.where(upper_mask, bwd_cum[:, None] - bwd_cum[None, :], -jnp.inf)) * step_size[None, :, 1]
    scores = jnp.einsum('tgn,sgn->tsg', read_act.reshape(length, groups, state_size).astype(jnp.float32), write_act.reshape(length, groups, state_size).astype(jnp.float32), precision=lax.Precision.HIGHEST)
    combined = scores[:, :, :, None] * (fwd_weight + bwd_weight)
    value_heads = value_act.reshape(length, groups, per_group, head_size).astype(jnp.float32)
    mixed_heads = jnp.einsum('tsgh,sghp->tghp', combined, value_heads, precision=lax.Precision.HIGHEST)
    mixed_heads = mixed_heads + skip_gain[None, :, :, None] * value_heads
    return (mixed_heads.reshape(length, -1) * jax.nn.silu(gate_flat.astype(jnp.float32))).astype(jnp.bfloat16)

def section_apply(tokens, norm_gain, proj_gate, proj_value, proj_write, proj_read, proj_step, step_bias, decay_log, skip_gain, conv_value, conv_write, conv_read, proj_out):
    width_model = tokens.shape[1]
    as_float = tokens.astype(jnp.float32)
    scale_rms = lax.rsqrt(lax.optimization_barrier(jnp.mean(as_float * as_float, axis=1, keepdims=True)) + epsilon)
    normed = (as_float * scale_rms * norm_gain[None, :]).astype(jnp.bfloat16)
    gate_flat = jnp.dot(normed, proj_gate.reshape(width_model, -1), preferred_element_type=jnp.float32).astype(jnp.bfloat16)
    value_flat = jnp.dot(normed, proj_value.reshape(width_model, -1), preferred_element_type=jnp.float32).astype(jnp.bfloat16)
    write_flat = jnp.dot(normed, proj_write.reshape(width_model, -1), preferred_element_type=jnp.float32).astype(jnp.bfloat16)
    read_flat = jnp.dot(normed, proj_read.reshape(width_model, -1), preferred_element_type=jnp.float32).astype(jnp.bfloat16)
    step_raw = jnp.dot(normed, proj_step.reshape(width_model, -1), preferred_element_type=jnp.float32)
    gated_out = duality_mix(gate_flat, value_flat, write_flat, read_flat, step_raw, step_bias, decay_log, skip_gain, conv_value, conv_write, conv_read)
    branch = jnp.dot(gated_out, proj_out.reshape(-1, width_model), preferred_element_type=jnp.float32).astype(jnp.bfloat16)
    branch = lax.optimization_barrier(branch)
    return (as_float + 0.5 * branch.astype(jnp.float32)).astype(jnp.bfloat16)

def reference(micro_in, norm_gain, proj_gate, proj_value, proj_write, proj_read, proj_step, step_bias, decay_log, skip_gain, conv_value, conv_write, conv_read, proj_out):
    weights = (norm_gain, proj_gate, proj_value, proj_write, proj_read, proj_step, step_bias, decay_log, skip_gain, conv_value, conv_write, conv_read, proj_out)

    def run_section(current, section_weights):
        return (section_apply(current, *section_weights), None)

    def one_micro(tokens):
        final_section, unused = lax.scan(run_section, tokens, weights)
        as_float = final_section.astype(jnp.float32)
        scale_rms = lax.rsqrt(lax.optimization_barrier(jnp.mean(as_float * as_float, axis=1, keepdims=True)) + epsilon)
        return (as_float * scale_rms).astype(jnp.bfloat16)
    return lax.map(one_micro, micro_in)
```

```python
import jax
import jax.numpy as jnp
from jax import lax
from jax.experimental import pallas as pl
from jax.experimental.pallas import tpu as pltpu
from jax.sharding import Mesh
from jax.sharding import PartitionSpec as P

FS = ("yh", "ym")
TP = ("tz", "tc")
ALL = ("pp", "tz", "tc", "yh", "ym")
EPS = 1e-06
T = 96
D = 1024
F32 = jnp.float32
BF16 = jnp.bfloat16
ROWS = 176
VMEM = pltpu.VMEM


def lanes(shape):
    return lax.broadcasted_iota(jnp.int32, shape, len(shape) - 1)


def split3(v):
    hi = v.astype(BF16).astype(F32)
    mid = (v - hi).astype(BF16).astype(F32)
    low = v - hi - mid
    return hi, mid, low


def pack_kernel(
    where_ref, micro_ref, gate_ref, value_ref, step_ref, out_ref, small_ref, send_ref, same_ref, other_ref
):
    core = where_ref[1]
    half = where_ref[0]
    zero = jnp.zeros((2, 128), F32)
    for m in range(2):
        micro = micro_ref[m].astype(F32)
        rows = jnp.concatenate([micro[k * 6 : (k + 1) * 6] for k in range(4)], axis=1)
        rows = jnp.concatenate([rows, zero], axis=0).astype(BF16)
        for dest in range(64):
            send_ref[2 * dest + m] = rows
    gate = gate_ref[...]
    value = value_ref[...]
    step = step_ref[...].astype(F32)
    small = split3(small_ref[...])
    misc = jnp.concatenate(
        [step, *[s[0:1] for s in small], *[s[1:2] for s in small], jnp.zeros((8, D), F32)], axis=0
    ).astype(BF16)
    out = out_ref[...].astype(F32)
    low = lanes((64, 128)) < 64
    halves = []
    for h in range(2):
        by_core = []
        for c in range(2):
            for p in range(2):
                first = out[:, (4 * p + c) * 128 : (4 * p + c + 1) * 128]
                second = out[:, (4 * p + 2 + c) * 128 : (4 * p + 3 + c) * 128]
                if h == 0:
                    block = jnp.where(low, first, pltpu.roll(second, 64, 1))
                else:
                    block = jnp.where(low, pltpu.roll(first, 64, 1), second)
                by_core.append(block)
        own = [jnp.where(core == 0, by_core[i], by_core[2 + i]) for i in range(2)]
        far = [jnp.where(core == 0, by_core[2 + i], by_core[i]) for i in range(2)]
        halves.append(jnp.concatenate(own + far, axis=1))
    for ref, pick in ((same_ref, 0), (other_ref, 1)):
        part = jnp.where(half == pick, halves[0], halves[1])
        ref[0:64] = gate
        ref[64:128] = value
        ref[128:160] = jnp.concatenate([part[0:32], part[32:64]], axis=1).astype(BF16)
        ref[160:176] = misc


def nt_dot(a, b):
    return lax.dot_general(a, b, (((1,), (1,)), ((), ())), preferred_element_type=F32)


def nn_dot(a, b):
    return lax.dot_general(a, b, (((1,), (0,)), ((), ())), preferred_element_type=F32)


def silu(v):
    return v * jax.nn.sigmoid(v)


def entry_quarter(recv_ref, quarter_ref, h, c, index):
    lane = lanes((8, 128)) // 32
    for x in range(4):
        for p in range(2):
            blocks = []
            for zz in range(2):
                for m in range(2):
                    src = (((x * 4 + 2 * p + zz) * 2 + c) * 2 + h) * 2 + m
                    blocks.append(recv_ref[src].astype(F32))
            for k in range(4):
                row = None
                for g in range(4):
                    moved = blocks[g] if g == k else pltpu.roll(blocks[g], ((g - k) % 4) * 32, 1)
                    row = moved if row is None else jnp.where(lane == g, moved, row)
                quarter_ref[index, x * 24 + k * 6 : x * 24 + k * 6 + 6, p * 128 : (p + 1) * 128] = row[:6]


def section_body(
    where_ref, quarters, weight_refs, write_ref, read_ref, gain_ref, taps_ref, own_ref, far_ref, pad_ref
):
    low = lanes((T, 128)) < 64
    total = None
    for pair in quarters:
        for q in pair:
            sq = q * q
            sq = sq[:, :128] + sq[:, 128:]
            total = sq if total is None else total + sq
    scale = lax.rsqrt(jnp.sum(total, axis=1, keepdims=True) * (1.0 / D) + EPS)
    blocks = []
    for z in range(4):
        for c in range(2):
            span = slice((z // 2) * 128, (z // 2 + 1) * 128)
            q0 = quarters[0][c][:, span]
            q1 = quarters[1][c][:, span]
            if z % 2 == 0:
                block = jnp.where(low, q0, pltpu.roll(q1, 64, 1))
            else:
                block = jnp.where(low, pltpu.roll(q0, 64, 1), q1)
            n = 2 * z + c
            blocks.append((block * scale * gain_ref[:, n * 128 : (n + 1) * 128]).astype(BF16))
    normed = jnp.concatenate(blocks, axis=1)

    step_rows = jnp.concatenate([w[160:176].astype(F32)[0:2] for w in weight_refs], axis=0)
    step_raw = nt_dot(step_rows.astype(BF16), normed)
    small = []
    for w in weight_refs:
        misc = w[160:176].astype(F32)
        small.append((misc[2:3] + misc[3:4] + misc[4:5], misc[5:6] + misc[6:7] + misc[7:8]))
    bias = jnp.concatenate([s[0][:, 640 + 128 * d : 640 + 128 * d + T] for s in small for d in range(2)], axis=0)
    decay = jnp.concatenate([s[1][:, 128 * d : 128 * d + T] for s in small for d in range(2)], axis=0)
    raw = step_raw + bias
    dt = jnp.maximum(raw, 0.0) + jnp.log1p(jnp.exp(-jnp.abs(raw)))
    log_decay = dt * (-jnp.exp(decay))
    parts = [s.astype(BF16) for s in split3(log_decay)]
    row_id = lax.broadcasted_iota(jnp.int32, (T, T), 0)
    col_id = lax.broadcasted_iota(jnp.int32, (T, T), 1)
    upto = (row_id <= col_id).astype(F32).astype(BF16)
    since = (row_id >= col_id).astype(F32).astype(BF16)
    fwd_all = (nn_dot(parts[0], upto) + nn_dot(parts[1], upto)) + nn_dot(parts[2], upto)
    bwd_all = (nn_dot(parts[0], since) + nn_dot(parts[1], since)) + nn_dot(parts[2], since)
    odd = lax.broadcasted_iota(jnp.int32, (8, T), 0) % 2 == 1
    cum = jnp.where(odd, bwd_all, fwd_all)
    cum_pad = jnp.concatenate([cum, jnp.zeros((8, 128 - T), F32)], axis=1)
    cum_cols = cum_pad.T[:T]

    gv01 = nt_dot(normed, jnp.concatenate([weight_refs[0][0:128], weight_refs[1][0:128]], axis=0))
    gv23 = nt_dot(normed, jnp.concatenate([weight_refs[2][0:128], weight_refs[3][0:128]], axis=0))
    wr = nn_dot(normed, jnp.concatenate([write_ref[...], read_ref[...]], axis=1))
    pad_ref[0:8] = jnp.zeros((8, 768), F32)
    pad_ref[8 + T : 16 + T] = jnp.zeros((8, 768), F32)
    pad_ref[8 : 8 + T, 0:256] = gv01.astype(BF16).astype(F32)
    pad_ref[8 : 8 + T, 256:512] = gv23.astype(BF16).astype(F32)
    pad_ref[8 : 8 + T, 512:768] = wr.astype(BF16).astype(F32)
    acts = []
    for g in range(6):
        span = slice(g * 128, (g + 1) * 128)
        acc = None
        for k in range(5):
            tap = small[g][0][:, k * 128 : (k + 1) * 128] if g < 4 else taps_ref[k : k + 1, (g - 4) * 128 : (g - 3) * 128]
            term = pad_ref[6 + k : 6 + k + T, span] * tap
            acc = term if acc is None else acc + term
        acts.append(silu(acc).astype(BF16))
    scores = nt_dot(acts[5], acts[4])
    lower = row_id >= col_id
    diagonal = row_id == col_id
    gated = []
    for j in range(4):
        fc = cum_cols[:, 2 * j : 2 * j + 1]
        bc = cum_cols[:, 2 * j + 1 : 2 * j + 2]
        fr = cum[2 * j : 2 * j + 1]
        br = cum[2 * j + 1 : 2 * j + 2]
        d0 = dt[2 * j : 2 * j + 1]
        d1 = dt[2 * j + 1 : 2 * j + 2]
        mix = jnp.exp(jnp.where(lower, fc - fr, bc - br)) * jnp.where(lower, d0, d1)
        mix = mix + jnp.where(diagonal, d1, 0.0)
        combined = scores * mix
        high = combined.astype(BF16)
        rest = (combined - high.astype(F32)).astype(BF16)
        y = nn_dot(high, acts[j]) + nn_dot(rest, acts[j])
        y = y + small[j][1][:, 256:384] * acts[j].astype(F32)
        gate = pltpu.roll(pad_ref[8 : 8 + T, j * 128 : (j + 1) * 128], 64, 1)
        gated.append(y * silu(gate))
    pairs = [jnp.where(low, pltpu.roll(gated[2 * i], 64, 1), gated[2 * i + 1]).astype(BF16) for i in range(2)]
    gated_all = jnp.concatenate(pairs, axis=1)
    for side, ref in ((0, own_ref), (1, far_ref)):
        weight = jnp.concatenate(
            [
                w[128:160, 512 * r + 256 * side : 512 * r + 256 * side + 256]
                for w in weight_refs
                for r in range(2)
            ],
            axis=0,
        )
        ref[...] = nn_dot(gated_all, weight).astype(ref.dtype)


def entry_section_kernel(where_ref, recv_ref, *refs):
    *rest, quarter_out, own_ref, far_ref, pad_ref, quarter_ref = refs
    for h in range(2):
        for c in range(2):
            entry_quarter(recv_ref, quarter_ref, h, c, 2 * h + c)
    quarters = [[quarter_ref[2 * h + c] for c in range(2)] for h in range(2)]
    mine = quarter_ref[2 * where_ref[0] + where_ref[1]]
    quarter_out[...] = mine.astype(BF16)
    section_body(where_ref, quarters, rest[0:4], *rest[4:], own_ref, far_ref, pad_ref)


def relay_section_kernel(where_ref, a_ref, b_ref, c_ref, d_ref, *refs):
    *rest, own_ref, far_ref, pad_ref = refs
    half = where_ref[0] == 0
    core = where_ref[1] == 0
    a, b, c, d = [r[...].astype(F32) for r in (a_ref, b_ref, c_ref, d_ref)]
    own0, own1 = jnp.where(half, a, c), jnp.where(half, c, a)
    far0, far1 = jnp.where(half, b, d), jnp.where(half, d, b)
    quarters = [
        [jnp.where(core, own0, far0), jnp.where(core, far0, own0)],
        [jnp.where(core, own1, far1), jnp.where(core, far1, own1)],
    ]
    section_body(where_ref, quarters, rest[0:4], *rest[4:], own_ref, far_ref, pad_ref)


SMEM_SPEC = pl.BlockSpec(memory_space=pltpu.SMEM)
VMEM_SPEC = pl.BlockSpec(memory_space=pltpu.VMEM)


def call_kernel(kernel, out_shape, count, scratch=()):
    return pl.pallas_call(
        kernel,
        out_shape=out_shape,
        in_specs=[SMEM_SPEC] + [VMEM_SPEC] * count,
        out_specs=[VMEM_SPEC] * len(out_shape),
        scratch_shapes=scratch,
        compiler_params=pltpu.CompilerParams(vmem_limit_bytes=24 * 1024 * 1024),
    )


def flip(v, axes, bits):
    size = lax.axis_size(axes)
    return lax.ppermute(v, axes, [(i, i ^ bits) for i in range(size)])


def per_device(
    micro_in,
    norm_gain,
    proj_gate,
    proj_value,
    proj_write,
    proj_read,
    proj_step,
    step_bias,
    decay_log,
    skip_gain,
    conv_value,
    conv_write,
    conv_read,
    proj_out,
):
    sections = lax.axis_size("pp")
    stage = lax.axis_index("pp")
    half = lax.axis_index("yh")
    micro = lax.axis_index("ym")
    core = lax.axis_index("tc")
    zpos = lax.axis_index("tz")
    where = jnp.stack([half, core]).astype(jnp.int32)

    gate_rows = proj_gate[0, :, 0, 0, :].T
    value_rows = proj_value[0, :, 0, 0, :].T
    step_rows = proj_step[0, :, :, 0, 0].T
    taps = jnp.pad(conv_value[0, :, 0, 0, :], ((0, 0), (64, 0))).reshape(1, 640)
    wide = lambda v: jnp.broadcast_to(v, (128,))
    row_a = jnp.concatenate(
        [taps[0], wide(step_bias[0, 0, 0]), wide(step_bias[0, 1, 0]), jnp.zeros((128,), F32)]
    )
    row_b = jnp.concatenate(
        [wide(decay_log[0, 0, 0]), wide(decay_log[0, 1, 0]), wide(skip_gain[0, 0]), jnp.zeros((640,), F32)]
    )
    small = jnp.stack([row_a, row_b])
    shape = jax.ShapeDtypeStruct
    send, same, other = call_kernel(
        pack_kernel,
        [shape((128, 8, 128), BF16), shape((ROWS, D), BF16), shape((ROWS, D), BF16)],
        6,
    )(where, micro_in, gate_rows, value_rows, step_rows, proj_out[0, 0, 0], small)
    w1 = flip(same, FS, 1)
    w2 = flip(other, FS, 2)
    w3 = flip(other, FS, 3)
    recv = lax.all_to_all(send, ALL, 0, 0)

    taps_wr = jnp.concatenate([conv_write[0, :, 0, :], conv_read[0, :, 0, :]], axis=1)
    params = (same, w1, w2, w3, proj_write[0, :, 0, :], proj_read[0, :, 0, :], norm_gain, taps_wr)
    quarter = shape((T, 256), BF16)
    outs = [shape((T, 256), F32), quarter]
    pad = pltpu.VMEM((T + 16, 768), F32)
    mine, own, far = call_kernel(
        entry_section_kernel, [quarter, *outs], 9, [pad, pltpu.VMEM((4, T, 256), F32)]
    )(where, recv, *params)
    hop = [(i, i + 1) for i in range(sections - 1)]
    hop_flip = [(2 * i + h, 2 * (i + 1) + 1 - h) for i in range(sections - 1) for h in range(2)]
    for s in range(sections):
        got = flip(far, "tc", 1)
        mixed = (own + got.astype(F32)).astype(BF16)
        r1, r2, r3 = [flip(mixed, "tz", d).astype(F32) for d in (1, 2, 3)]
        branch = ((mixed.astype(F32) + r1) + (r2 + r3)).astype(BF16).astype(F32)
        produced = (mine.astype(F32) + 0.5 * branch).astype(BF16)
        if s + 1 == sections:
            break
        a = lax.ppermute(produced, "pp", hop)
        c = lax.ppermute(produced, ("pp", "yh"), hop_flip)
        b = flip(a, "tc", 1)
        d = flip(c, "tc", 1)
        mine = a
        own, far = call_kernel(relay_section_kernel, outs, 12, [pad])(where, a, b, c, d, *params)

    final = produced.astype(F32)
    squares = jnp.sum(final * final, axis=1)
    squares = squares + flip(squares, "tc", 1)
    pair = lax.dynamic_slice_in_dim(final, zpos * 64, 64, 1).reshape(T, 2, 32)
    keep = lax.dynamic_index_in_dim(pair, micro, 1, keepdims=False)
    give = lax.dynamic_index_in_dim(pair, 1 - micro, 1, keepdims=False)
    message = jnp.concatenate([give, jnp.broadcast_to(squares[:, None], (T, 96))], axis=1)
    g1 = flip(message, FS, 1)
    s2 = flip(squares, FS, 2)
    s3 = flip(squares, FS, 3)
    keep = keep * lax.rsqrt((squares + s2) / D + EPS)[:, None]
    taken = g1[:, :32] * lax.rsqrt((g1[:, 32] + s3) / D + EPS)[:, None]
    both = jnp.where(micro == 0, jnp.stack([keep, taken]), jnp.stack([taken, keep])).astype(BF16)
    share = T // sections
    result = both[:, (sections - 1) * share :]
    for x in range(sections - 1):
        moved = lax.ppermute(both[:, x * share : (x + 1) * share], "pp", [(sections - 1, x)])
        result = jnp.where(stage == x, moved, result)
    return result


def solution(mesh):
    split = Mesh(
        mesh.devices.reshape(mesh.shape["pp"], 2, 2, 4, 2), ("pp", "yh", "ym", "tz", "tc")
    )
    in_specs = (
        P(None, "pp", TP + FS),
        P("pp", None),
        P("pp", None, TP, FS, None),
        P("pp", None, TP, FS, None),
        P("pp", None, TP, None),
        P("pp", None, TP, None),
        P("pp", None, None, TP, FS),
        P("pp", None, TP, FS),
        P("pp", None, TP, FS),
        P("pp", TP, FS),
        P("pp", None, TP, FS, None),
        P("pp", None, TP, None),
        P("pp", None, TP, None),
        P("pp", TP, FS, None, None),
    )
    out_specs = P(None, "pp", TP + FS)
    return jax.shard_map(
        per_device, mesh=split, in_specs=in_specs, out_specs=out_specs, check_vma=False
    )
```

```python
import jax
import jax.numpy as jnp
from jax import lax
from jax.experimental import pallas as pl
from jax.experimental.pallas import tpu as pltpu
from jax.sharding import Mesh
from jax.sharding import PartitionSpec as P

FS = ("ym", "yh")
TP = ("tz", "tc")
ALL = ("pp", "tz", "tc", "ym", "yh")
EPS = 1e-06
T = 96
D = 1024
F32 = jnp.float32
BF16 = jnp.bfloat16
ROWS = 168
VMEM = pltpu.VMEM


def lanes(shape):
    return lax.broadcasted_iota(jnp.int32, shape, len(shape) - 1)


def split3(v):
    hi = v.astype(BF16).astype(F32)
    mid = (v - hi).astype(BF16).astype(F32)
    low = v - hi - mid
    return hi, mid, low


def permuted(v):
    group = lanes((v.shape[0], 128)) // 32
    out = []
    for h in range(2):
        for c in range(2):
            for p in range(2):
                block = None
                for g in range(4):
                    zz, m = g // 2, g % 2
                    n = (2 * p + zz) * 2 + c
                    moved = v[:, n * 128 : (n + 1) * 128]
                    turn = (64 * zz - 32 * m - 32 * h) % 128
                    if turn:
                        moved = pltpu.roll(moved, turn, 1)
                    block = moved if block is None else jnp.where(group == g, moved, block)
                out.append(block)
    return out


def pack_kernel(
    where_ref,
    micro_hbm,
    gate_hbm,
    value_hbm,
    step_hbm,
    out_hbm,
    taps_hbm,
    bias_hbm,
    decay_hbm,
    skip_hbm,
    gain_hbm,
    send_ref,
    same_ref,
    other_ref,
    gain_out,
    *scratch,
):
    sources = (
        gate_hbm,
        value_hbm,
        out_hbm,
        step_hbm,
        taps_hbm,
        bias_hbm,
        decay_hbm,
        skip_hbm,
        gain_hbm,
        micro_hbm,
    )
    buffers, sems = scratch[:-1], scratch[-1]
    copies = [pltpu.make_async_copy(s, b, sems.at[i]) for i, (s, b) in enumerate(zip(sources, buffers))]
    for copy in copies:
        copy.start()
    for copy in copies:
        copy.wait()
    gate_ref, value_ref, out_ref, step_ref, taps_ref, bias_ref, decay_ref, skip_ref, gain_ref, micro_ref = buffers
    core = where_ref[1] == 0
    half = where_ref[0] == 0
    gate = jnp.concatenate(permuted(gate_ref[...].astype(F32)), axis=1).astype(BF16)
    value = jnp.concatenate(permuted(value_ref[...].astype(F32)), axis=1).astype(BF16)
    step = jnp.concatenate(permuted(step_ref[...].astype(F32)), axis=1)
    gain_out[...] = jnp.concatenate(permuted(gain_ref[...]), axis=1)
    blank = jnp.zeros((1, 64), F32)
    wide = lambda ref, k: jnp.broadcast_to(ref[:, k : k + 1], (1, 128))
    row_a = [piece for k in range(5) for piece in (blank, taps_ref[k])]
    row_a = jnp.concatenate(row_a + [wide(bias_ref, 0), wide(bias_ref, 1), blank, blank], axis=1)
    row_b = [wide(decay_ref, 0), wide(decay_ref, 1), wide(skip_ref, 0)] + [blank] * 10
    row_b = jnp.concatenate(row_b, axis=1)
    misc = jnp.concatenate([step, *split3(row_a), *split3(row_b)], axis=0).astype(BF16)
    out = permuted(out_ref[...].astype(F32))
    halves = []
    for h in range(2):
        first, second = out[4 * h : 4 * h + 2], out[4 * h + 2 : 4 * h + 4]
        own = [jnp.where(core, a, b) for a, b in zip(first, second)]
        far = [jnp.where(core, b, a) for a, b in zip(first, second)]
        halves.append(jnp.concatenate(own + far, axis=1))
    for ref, pick in ((same_ref, half), (other_ref, jnp.logical_not(half))):
        part = jnp.where(pick, halves[0], halves[1])
        ref[0:64] = gate
        ref[64:128] = value
        ref[128:160] = jnp.concatenate([part[0:32], part[32:64]], axis=1).astype(BF16)
        ref[160:168] = misc
    zero = jnp.zeros((2, 128), F32)
    for m in range(2):
        micro = micro_ref[m].astype(F32)
        rows = jnp.concatenate([micro[k * 6 : (k + 1) * 6] for k in range(4)], axis=1)
        rows = jnp.concatenate([rows, zero], axis=0).astype(BF16)
        for dest in range(64):
            send_ref[dest // 2 * 4 + 2 * m + dest % 2] = rows


def nt_dot(a, b):
    return lax.dot_general(a, b, (((1,), (1,)), ((), ())), preferred_element_type=F32)


def nn_dot(a, b):
    return lax.dot_general(a, b, (((1,), (0,)), ((), ())), preferred_element_type=F32)


def silu(v):
    return v * jax.nn.sigmoid(v)


def entry_quarter(recv_ref, quarter_ref, h, c, index):
    lane = lanes((8, 128)) // 32
    for x in range(4):
        for p in range(2):
            blocks = []
            for zz in range(2):
                for m in range(2):
                    src = (((x * 4 + 2 * p + zz) * 2 + c) * 2 + m) * 2 + h
                    blocks.append(recv_ref[src].astype(F32))
            for k in range(4):
                row = None
                for g in range(4):
                    moved = blocks[g] if g == k else pltpu.roll(blocks[g], ((g - k) % 4) * 32, 1)
                    row = moved if row is None else jnp.where(lane == g, moved, row)
                quarter_ref[index, x * 24 + k * 6 : x * 24 + k * 6 + 6, p * 128 : (p + 1) * 128] = row[:6]


def section_body(quarters, weight_refs, write_ref, read_ref, gain_ref, taps_refs, own_ref, far_ref, pad_ref):
    low = lanes((T, 128)) < 64
    total = None
    for pair in quarters:
        for q in pair:
            sq = q * q
            sq = sq[:, :128] + sq[:, 128:]
            total = sq if total is None else total + sq
    scale = lax.rsqrt(jnp.sum(total, axis=1, keepdims=True) * (1.0 / D) + EPS)
    blocks = []
    for h in range(2):
        for c in range(2):
            n = (2 * h + c) * 256
            blocks.append((quarters[h][c] * scale * gain_ref[:, n : n + 256]).astype(BF16))
    normed = jnp.concatenate(blocks, axis=1)

    step_rows = jnp.concatenate([w[160:168].astype(F32)[0:2] for w in weight_refs], axis=0)
    step_raw = nt_dot(step_rows.astype(BF16), normed)
    small = []
    for w in weight_refs:
        misc = w[160:168].astype(F32)
        small.append((misc[2:3] + misc[3:4] + misc[4:5], misc[5:6] + misc[6:7] + misc[7:8]))
    bias = jnp.concatenate([s[0][:, 640 + 128 * d : 640 + 128 * d + T] for s in small for d in range(2)], axis=0)
    decay = jnp.concatenate([s[1][:, 128 * d : 128 * d + T] for s in small for d in range(2)], axis=0)
    raw = step_raw + bias
    dt = jnp.maximum(raw, 0.0) + jnp.log1p(jnp.exp(-jnp.abs(raw)))
    log_decay = dt * (-jnp.exp(decay))
    parts = [s.astype(BF16) for s in split3(log_decay)]
    row_id = lax.broadcasted_iota(jnp.int32, (T, T), 0)
    col_id = lax.broadcasted_iota(jnp.int32, (T, T), 1)
    upto = (row_id <= col_id).astype(F32).astype(BF16)
    since = (row_id >= col_id).astype(F32).astype(BF16)
    fwd_all = (nn_dot(parts[0], upto) + nn_dot(parts[1], upto)) + nn_dot(parts[2], upto)
    bwd_all = (nn_dot(parts[0], since) + nn_dot(parts[1], since)) + nn_dot(parts[2], since)
    odd = lax.broadcasted_iota(jnp.int32, (8, T), 0) % 2 == 1
    cum = jnp.where(odd, bwd_all, fwd_all)
    cum_pad = jnp.concatenate([cum, jnp.zeros((8, 128 - T), F32)], axis=1)
    cum_cols = cum_pad.T[:T]

    gv01 = nt_dot(normed, jnp.concatenate([weight_refs[0][0:128], weight_refs[1][0:128]], axis=0))
    gv23 = nt_dot(normed, jnp.concatenate([weight_refs[2][0:128], weight_refs[3][0:128]], axis=0))
    wr_rows = [
        jnp.concatenate([r[n * 128 + y * 32 : n * 128 + y * 32 + 32] for r in (write_ref, read_ref)], axis=1)
        for h in range(2)
        for c in range(2)
        for n in (c, 2 + c, 4 + c, 6 + c)
        for y in (h, 2 + h)
    ]
    wr = nn_dot(normed, jnp.concatenate(wr_rows, axis=0))
    pad_ref[0:8] = jnp.zeros((8, 768), F32)
    pad_ref[8 + T : 16 + T] = jnp.zeros((8, 768), F32)
    pad_ref[8 : 8 + T, 0:256] = gv01.astype(BF16).astype(F32)
    pad_ref[8 : 8 + T, 256:512] = gv23.astype(BF16).astype(F32)
    pad_ref[8 : 8 + T, 512:768] = wr.astype(BF16).astype(F32)
    acts = []
    for g in range(6):
        span = slice(g * 128, (g + 1) * 128)
        acc = None
        for k in range(5):
            tap = small[g][0][:, k * 128 : (k + 1) * 128] if g < 4 else taps_refs[g - 4][k]
            term = pad_ref[6 + k : 6 + k + T, span] * tap
            acc = term if acc is None else acc + term
        acts.append(silu(acc).astype(BF16))
    scores = nt_dot(acts[5], acts[4])
    lower = row_id >= col_id
    diagonal = row_id == col_id
    gated = []
    for j in range(4):
        fc = cum_cols[:, 2 * j : 2 * j + 1]
        bc = cum_cols[:, 2 * j + 1 : 2 * j + 2]
        fr = cum[2 * j : 2 * j + 1]
        br = cum[2 * j + 1 : 2 * j + 2]
        d0 = dt[2 * j : 2 * j + 1]
        d1 = dt[2 * j + 1 : 2 * j + 2]
        mix = jnp.exp(jnp.where(lower, fc - fr, bc - br)) * jnp.where(lower, d0, d1)
        mix = mix + jnp.where(diagonal, d1, 0.0)
        combined = scores * mix
        high = combined.astype(BF16)
        rest = (combined - high.astype(F32)).astype(BF16)
        y = nn_dot(high, acts[j]) + nn_dot(rest, acts[j])
        y = y + small[j][1][:, 256:384] * acts[j].astype(F32)
        gate = pltpu.roll(pad_ref[8 : 8 + T, j * 128 : (j + 1) * 128], 64, 1)
        gated.append(y * silu(gate))
    pairs = [jnp.where(low, pltpu.roll(gated[2 * i], 64, 1), gated[2 * i + 1]).astype(BF16) for i in range(2)]
    gated_all = jnp.concatenate(pairs, axis=1)
    for side, ref in ((0, own_ref), (1, far_ref)):
        weight = jnp.concatenate(
            [
                w[128:160, 512 * r + 256 * side : 512 * r + 256 * side + 256]
                for w in weight_refs
                for r in range(2)
            ],
            axis=0,
        )
        ref[...] = nn_dot(gated_all, weight).astype(ref.dtype)


def entry_section_kernel(where_ref, recv_ref, *refs):
    *rest, quarter_out, own_ref, far_ref, pad_ref, quarter_ref = refs
    for h in range(2):
        for c in range(2):
            entry_quarter(recv_ref, quarter_ref, h, c, 2 * h + c)
    quarters = [[quarter_ref[2 * h + c] for c in range(2)] for h in range(2)]
    mine = quarter_ref[2 * where_ref[0] + where_ref[1]]
    quarter_out[...] = mine.astype(BF16)
    section_body(quarters, rest[0:4], *rest[4:7], rest[7:9], own_ref, far_ref, pad_ref)


def relay_section_kernel(where_ref, a_ref, b_ref, c_ref, d_ref, *refs):
    *rest, own_ref, far_ref, pad_ref = refs
    half = where_ref[0] == 0
    core = where_ref[1] == 0
    a, b, c, d = [r[...].astype(F32) for r in (a_ref, b_ref, c_ref, d_ref)]
    own0, own1 = jnp.where(half, a, c), jnp.where(half, c, a)
    far0, far1 = jnp.where(half, b, d), jnp.where(half, d, b)
    quarters = [
        [jnp.where(core, own0, far0), jnp.where(core, far0, own0)],
        [jnp.where(core, own1, far1), jnp.where(core, far1, own1)],
    ]
    section_body(quarters, rest[0:4], *rest[4:7], rest[7:9], own_ref, far_ref, pad_ref)


SMEM_SPEC = pl.BlockSpec(memory_space=pltpu.SMEM)
VMEM_SPEC = pl.BlockSpec(memory_space=pltpu.VMEM)


def call_kernel(kernel, out_shape, count, scratch=()):
    return pl.pallas_call(
        kernel,
        out_shape=out_shape,
        in_specs=[SMEM_SPEC] + [VMEM_SPEC] * count,
        out_specs=[VMEM_SPEC] * len(out_shape),
        scratch_shapes=scratch,
        compiler_params=pltpu.CompilerParams(vmem_limit_bytes=24 * 1024 * 1024),
    )


def flip(v, axes, bits):
    size = lax.axis_size(axes)
    return lax.ppermute(v, axes, [(i, i ^ bits) for i in range(size)])


def per_device(
    micro_in,
    norm_gain,
    proj_gate,
    proj_value,
    proj_write,
    proj_read,
    proj_step,
    step_bias,
    decay_log,
    skip_gain,
    conv_value,
    conv_write,
    conv_read,
    proj_out,
):
    sections = lax.axis_size("pp")
    stage = lax.axis_index("pp")
    half = lax.axis_index("yh")
    micro = lax.axis_index("ym")
    core = lax.axis_index("tc")
    zpos = lax.axis_index("tz")
    where = jnp.stack([half, core]).astype(jnp.int32)

    shape = jax.ShapeDtypeStruct
    raw = (
        micro_in,
        proj_gate[0, :, 0, 0, :].T,
        proj_value[0, :, 0, 0, :].T,
        proj_step[0, :, :, 0, 0].T,
        proj_out[0, 0, 0],
        conv_value.reshape(5, 1, 64),
        step_bias.reshape(1, 2),
        decay_log.reshape(1, 2),
        skip_gain.reshape(1, 1),
        norm_gain,
    )
    order = (1, 2, 4, 3, 5, 6, 7, 8, 9, 0)
    send, same, other, gain = pl.pallas_call(
        pack_kernel,
        out_shape=[
            shape((128, 8, 128), BF16),
            shape((ROWS, D), BF16),
            shape((ROWS, D), BF16),
            shape((1, D), F32),
        ],
        in_specs=[SMEM_SPEC] + [pl.BlockSpec(memory_space=pl.ANY)] * len(raw),
        out_specs=[VMEM_SPEC] * 4,
        scratch_shapes=[pltpu.VMEM(raw[i].shape, raw[i].dtype) for i in order]
        + [pltpu.SemaphoreType.DMA((len(raw),))],
        compiler_params=pltpu.CompilerParams(vmem_limit_bytes=24 * 1024 * 1024),
    )(where, *raw)
    w1 = flip(other, FS, 1)
    w2 = flip(same, FS, 2)
    w3 = flip(other, FS, 3)
    recv = lax.all_to_all(send, ALL, 0, 0)

    taps_w = conv_write.reshape(5, 1, 128)
    taps_r = conv_read.reshape(5, 1, 128)
    params = (same, w1, w2, w3, proj_write[0, :, 0, :], proj_read[0, :, 0, :], gain, taps_w, taps_r)
    quarter = shape((T, 256), BF16)
    outs = [shape((T, 256), F32), quarter]
    pad = pltpu.VMEM((T + 16, 768), F32)
    mine, own, far = call_kernel(
        entry_section_kernel, [quarter, *outs], 10, [pad, pltpu.VMEM((4, T, 256), F32)]
    )(where, recv, *params)
    hop = [(i, (i + 1) % sections) for i in range(sections)]
    hop_flip = [(2 * i + h, 2 * j + 1 - h) for i, j in hop for h in range(2)]
    for s in range(sections):
        got = flip(far, "tc", 1)
        mixed = (own + got.astype(F32)).astype(BF16)
        r1, r2, r3 = [flip(mixed, "tz", d).astype(F32) for d in (1, 2, 3)]
        branch = ((mixed.astype(F32) + r1) + (r2 + r3)).astype(BF16).astype(F32)
        produced = (mine.astype(F32) + 0.5 * branch).astype(BF16)
        if s + 1 == sections:
            break
        a = lax.ppermute(produced, "pp", hop)
        c = lax.ppermute(produced, ("pp", "yh"), hop_flip)
        b = flip(a, "tc", 1)
        d = flip(c, "tc", 1)
        mine = a
        own, far = call_kernel(relay_section_kernel, outs, 13, [pad])(where, a, b, c, d, *params)

    final = produced.astype(F32)
    squares = jnp.sum(final * final, axis=1)
    squares = squares + flip(squares, "tc", 1)
    pair = lax.dynamic_slice_in_dim(final, zpos * 64, 64, 1).reshape(T, 2, 32)
    keep = lax.dynamic_index_in_dim(pair, micro, 1, keepdims=False)
    give = lax.dynamic_index_in_dim(pair, 1 - micro, 1, keepdims=False)
    message = jnp.concatenate([give, jnp.broadcast_to(squares[:, None], (T, 96))], axis=1)
    g1 = flip(message, FS, 2)
    s2 = flip(squares, FS, 1)
    s3 = flip(squares, FS, 3)
    keep = keep * lax.rsqrt((squares + s2) / D + EPS)[:, None]
    taken = g1[:, :32] * lax.rsqrt((g1[:, 32] + s3) / D + EPS)[:, None]
    both = jnp.where(micro == 0, jnp.stack([keep, taken]), jnp.stack([taken, keep])).astype(BF16)
    share = T // sections
    result = both[:, (sections - 1) * share :]
    for x in range(sections - 1):
        moved = lax.ppermute(both[:, x * share : (x + 1) * share], "pp", [(sections - 1, x)])
        result = jnp.where(stage == x, moved, result)
    return result


def solution(mesh):
    split = Mesh(
        mesh.devices.reshape(mesh.shape["pp"], 2, 2, 4, 2), ("pp", "ym", "yh", "tz", "tc")
    )
    in_specs = (
        P(None, "pp", TP + FS),
        P("pp", None),
        P("pp", None, TP, FS, None),
        P("pp", None, TP, FS, None),
        P("pp", None, TP, None),
        P("pp", None, TP, None),
        P("pp", None, None, TP, FS),
        P("pp", None, TP, FS),
        P("pp", None, TP, FS),
        P("pp", TP, FS),
        P("pp", None, TP, FS, None),
        P("pp", None, TP, None),
        P("pp", None, TP, None),
        P("pp", TP, FS, None, None),
    )
    out_specs = P(None, "pp", TP + FS)
    return jax.shard_map(
        per_device, mesh=split, in_specs=in_specs, out_specs=out_specs, check_vma=False
    )
```

```python
import jax
import jax.numpy as jnp
from jax import lax
from jax.experimental import pallas as pl
from jax.experimental.pallas import tpu as pltpu
from jax.sharding import Mesh
from jax.sharding import PartitionSpec as P

FS = ("ym", "yh")
TP = ("tz", "tc")
ALL = ("pp", "tz", "tc", "ym", "yh")
EPS = 1e-06
T = 96
D = 1024
F32 = jnp.float32
BF16 = jnp.bfloat16
ROWS = 168
VMEM = pltpu.VMEM


def lanes(shape):
    return lax.broadcasted_iota(jnp.int32, shape, len(shape) - 1)


def split3(v):
    hi = v.astype(BF16).astype(F32)
    mid = (v - hi).astype(BF16).astype(F32)
    low = v - hi - mid
    return hi, mid, low


def permuted(v):
    group = lanes((v.shape[0], 128)) // 32
    out = []
    for h in range(2):
        for c in range(2):
            for p in range(2):
                block = None
                for g in range(4):
                    zz, m = g // 2, g % 2
                    n = (2 * p + zz) * 2 + c
                    moved = v[:, n * 128 : (n + 1) * 128]
                    turn = (64 * zz - 32 * m - 32 * h) % 128
                    if turn:
                        moved = pltpu.roll(moved, turn, 1)
                    block = moved if block is None else jnp.where(group == g, moved, block)
                out.append(block)
    return out


def pack_kernel(
    where_ref,
    micro_hbm,
    gate_hbm,
    value_hbm,
    step_hbm,
    out_hbm,
    taps_hbm,
    bias_hbm,
    decay_hbm,
    skip_hbm,
    gain_hbm,
    send_ref,
    same_ref,
    other_ref,
    gain_out,
    *scratch,
):
    sources = (
        gate_hbm,
        value_hbm,
        out_hbm,
        step_hbm,
        taps_hbm,
        bias_hbm,
        decay_hbm,
        skip_hbm,
        gain_hbm,
        micro_hbm,
    )
    buffers, sems = scratch[:-1], scratch[-1]
    copies = [pltpu.make_async_copy(s, b, sems.at[i]) for i, (s, b) in enumerate(zip(sources, buffers))]
    for copy in copies:
        copy.start()
    for copy in copies:
        copy.wait()
    gate_ref, value_ref, out_ref, step_ref, taps_ref, bias_ref, decay_ref, skip_ref, gain_ref, micro_ref = buffers
    core = where_ref[1] == 0
    half = where_ref[0] == 0
    gate = jnp.concatenate(permuted(gate_ref[...].astype(F32)), axis=1).astype(BF16)
    value = jnp.concatenate(permuted(value_ref[...].astype(F32)), axis=1).astype(BF16)
    step = jnp.concatenate(permuted(step_ref[...].astype(F32)), axis=1)
    gain_out[...] = jnp.concatenate(permuted(gain_ref[...]), axis=1)
    blank = jnp.zeros((1, 64), F32)
    wide = lambda ref, k: jnp.broadcast_to(ref[:, k : k + 1], (1, 128))
    row_a = [piece for k in range(5) for piece in (blank, taps_ref[k])]
    row_a = jnp.concatenate(row_a + [wide(bias_ref, 0), wide(bias_ref, 1), blank, blank], axis=1)
    row_b = [wide(decay_ref, 0), wide(decay_ref, 1), wide(skip_ref, 0)] + [blank] * 10
    row_b = jnp.concatenate(row_b, axis=1)
    misc = jnp.concatenate([step, *split3(row_a), *split3(row_b)], axis=0).astype(BF16)
    out = permuted(out_ref[...].astype(F32))
    halves = []
    for h in range(2):
        first, second = out[4 * h : 4 * h + 2], out[4 * h + 2 : 4 * h + 4]
        own = [jnp.where(core, a, b) for a, b in zip(first, second)]
        far = [jnp.where(core, b, a) for a, b in zip(first, second)]
        halves.append(jnp.concatenate(own + far, axis=1))
    for ref, pick in ((same_ref, half), (other_ref, jnp.logical_not(half))):
        part = jnp.where(pick, halves[0], halves[1])
        ref[0:64] = gate
        ref[64:128] = value
        ref[128:160] = jnp.concatenate([part[0:32], part[32:64]], axis=1).astype(BF16)
        ref[160:168] = misc
    zero = jnp.zeros((2, 128), F32)
    for m in range(2):
        micro = micro_ref[m].astype(F32)
        rows = jnp.concatenate([micro[k * 6 : (k + 1) * 6] for k in range(4)], axis=1)
        rows = jnp.concatenate([rows, zero], axis=0).astype(BF16)
        for dest in range(64):
            send_ref[dest // 2 * 4 + 2 * m + dest % 2] = rows


def nt_dot(a, b):
    return lax.dot_general(a, b, (((1,), (1,)), ((), ())), preferred_element_type=F32)


def nn_dot(a, b):
    return lax.dot_general(a, b, (((1,), (0,)), ((), ())), preferred_element_type=F32)


def silu(v):
    return v * jax.nn.sigmoid(v)


def entry_quarter(recv_ref, quarter_ref, h, c, index):
    lane = lanes((8, 128)) // 32
    for x in range(4):
        for p in range(2):
            blocks = []
            for zz in range(2):
                for m in range(2):
                    src = (((x * 4 + 2 * p + zz) * 2 + c) * 2 + m) * 2 + h
                    blocks.append(recv_ref[src].astype(F32))
            for k in range(4):
                row = None
                for g in range(4):
                    moved = blocks[g] if g == k else pltpu.roll(blocks[g], ((g - k) % 4) * 32, 1)
                    row = moved if row is None else jnp.where(lane == g, moved, row)
                quarter_ref[index, x * 24 + k * 6 : x * 24 + k * 6 + 6, p * 128 : (p + 1) * 128] = row[:6]


def section_body(quarters, weight_refs, write_ref, read_ref, gain_ref, taps_refs, own_ref, far_ref, pad_ref):
    low = lanes((T, 128)) < 64
    total = None
    for pair in quarters:
        for q in pair:
            sq = q * q
            sq = sq[:, :128] + sq[:, 128:]
            total = sq if total is None else total + sq
    scale = lax.rsqrt(jnp.sum(total, axis=1, keepdims=True) * (1.0 / D) + EPS)
    blocks = []
    for h in range(2):
        for c in range(2):
            n = (2 * h + c) * 256
            blocks.append((quarters[h][c] * scale * gain_ref[:, n : n + 256]).astype(BF16))
    normed = jnp.concatenate(blocks, axis=1)

    step_rows = jnp.concatenate([w[160:168].astype(F32)[0:2] for w in weight_refs], axis=0)
    step_raw = nt_dot(step_rows.astype(BF16), normed)
    small = []
    for w in weight_refs:
        misc = w[160:168].astype(F32)
        small.append((misc[2:3] + misc[3:4] + misc[4:5], misc[5:6] + misc[6:7] + misc[7:8]))
    bias = jnp.concatenate([s[0][:, 640 + 128 * d : 640 + 128 * d + T] for s in small for d in range(2)], axis=0)
    decay = jnp.concatenate([s[1][:, 128 * d : 128 * d + T] for s in small for d in range(2)], axis=0)
    raw = step_raw + bias
    dt = jnp.maximum(raw, 0.0) + jnp.log1p(jnp.exp(-jnp.abs(raw)))
    log_decay = dt * (-jnp.exp(decay))
    parts = [s.astype(BF16) for s in split3(log_decay)]
    row_id = lax.broadcasted_iota(jnp.int32, (T, T), 0)
    col_id = lax.broadcasted_iota(jnp.int32, (T, T), 1)
    upto = (row_id <= col_id).astype(F32).astype(BF16)
    since = (row_id >= col_id).astype(F32).astype(BF16)
    fwd_all = (nn_dot(parts[0], upto) + nn_dot(parts[1], upto)) + nn_dot(parts[2], upto)
    bwd_all = (nn_dot(parts[0], since) + nn_dot(parts[1], since)) + nn_dot(parts[2], since)
    odd = lax.broadcasted_iota(jnp.int32, (8, T), 0) % 2 == 1
    cum = jnp.where(odd, bwd_all, fwd_all)
    cum_pad = jnp.concatenate([cum, jnp.zeros((8, 128 - T), F32)], axis=1)
    cum_cols = cum_pad.T[:T]

    gv01 = nt_dot(normed, jnp.concatenate([weight_refs[0][0:128], weight_refs[1][0:128]], axis=0))
    gv23 = nt_dot(normed, jnp.concatenate([weight_refs[2][0:128], weight_refs[3][0:128]], axis=0))
    wr_rows = [
        jnp.concatenate([r[n * 128 + y * 32 : n * 128 + y * 32 + 32] for r in (write_ref, read_ref)], axis=1)
        for h in range(2)
        for c in range(2)
        for n in (c, 2 + c, 4 + c, 6 + c)
        for y in (h, 2 + h)
    ]
    wr = nn_dot(normed, jnp.concatenate(wr_rows, axis=0))
    pad_ref[0:8] = jnp.zeros((8, 768), F32)
    pad_ref[8 + T : 16 + T] = jnp.zeros((8, 768), F32)
    pad_ref[8 : 8 + T, 0:256] = gv01.astype(BF16).astype(F32)
    pad_ref[8 : 8 + T, 256:512] = gv23.astype(BF16).astype(F32)
    pad_ref[8 : 8 + T, 512:768] = wr.astype(BF16).astype(F32)
    acts = []
    for g in range(6):
        span = slice(g * 128, (g + 1) * 128)
        acc = None
        for k in range(5):
            tap = small[g][0][:, k * 128 : (k + 1) * 128] if g < 4 else taps_refs[g - 4][k]
            term = pad_ref[6 + k : 6 + k + T, span] * tap
            acc = term if acc is None else acc + term
        acts.append(silu(acc).astype(BF16))
    scores = nt_dot(acts[5], acts[4])
    lower = row_id >= col_id
    diagonal = row_id == col_id
    gated = []
    for j in range(4):
        fc = cum_cols[:, 2 * j : 2 * j + 1]
        bc = cum_cols[:, 2 * j + 1 : 2 * j + 2]
        fr = cum[2 * j : 2 * j + 1]
        br = cum[2 * j + 1 : 2 * j + 2]
        d0 = dt[2 * j : 2 * j + 1]
        d1 = dt[2 * j + 1 : 2 * j + 2]
        mix = jnp.exp(jnp.where(lower, fc - fr, bc - br)) * jnp.where(lower, d0, d1)
        mix = mix + jnp.where(diagonal, d1, 0.0)
        combined = scores * mix
        high = combined.astype(BF16)
        rest = (combined - high.astype(F32)).astype(BF16)
        y = nn_dot(high, acts[j]) + nn_dot(rest, acts[j])
        y = y + small[j][1][:, 256:384] * acts[j].astype(F32)
        gate = pltpu.roll(pad_ref[8 : 8 + T, j * 128 : (j + 1) * 128], 64, 1)
        gated.append(y * silu(gate))
    pairs = [jnp.where(low, pltpu.roll(gated[2 * i], 64, 1), gated[2 * i + 1]).astype(BF16) for i in range(2)]
    gated_all = jnp.concatenate(pairs, axis=1)
    for side, ref in ((0, own_ref), (1, far_ref)):
        weight = jnp.concatenate(
            [
                w[128:160, 512 * r + 256 * side : 512 * r + 256 * side + 256]
                for w in weight_refs
                for r in range(2)
            ],
            axis=0,
        )
        ref[...] = nn_dot(gated_all, weight).astype(ref.dtype)


def entry_section_kernel(where_ref, recv_ref, *refs):
    *rest, quarter_out, own_ref, far_ref, pad_ref, quarter_ref = refs
    for h in range(2):
        for c in range(2):
            entry_quarter(recv_ref, quarter_ref, h, c, 2 * h + c)
    quarters = [[quarter_ref[2 * h + c] for c in range(2)] for h in range(2)]
    mine = quarter_ref[2 * where_ref[0] + where_ref[1]]
    quarter_out[...] = mine.astype(BF16)
    section_body(quarters, rest[0:4], *rest[4:7], rest[7:9], own_ref, far_ref, pad_ref)


def relay_section_kernel(where_ref, a_ref, b_ref, c_ref, d_ref, *refs):
    *rest, own_ref, far_ref, pad_ref = refs
    half = where_ref[0] == 0
    core = where_ref[1] == 0
    a, b, c, d = [r[...].astype(F32) for r in (a_ref, b_ref, c_ref, d_ref)]
    own0, own1 = jnp.where(half, a, c), jnp.where(half, c, a)
    far0, far1 = jnp.where(half, b, d), jnp.where(half, d, b)
    quarters = [
        [jnp.where(core, own0, far0), jnp.where(core, far0, own0)],
        [jnp.where(core, own1, far1), jnp.where(core, far1, own1)],
    ]
    section_body(quarters, rest[0:4], *rest[4:7], rest[7:9], own_ref, far_ref, pad_ref)


def exit_pack_kernel(where_ref, mine_ref, m0_ref, m1_ref, m2_ref, m3_ref, send_ref):
    branch = (m0_ref[...].astype(F32) + m1_ref[...].astype(F32)) + (m2_ref[...].astype(F32) + m3_ref[...].astype(F32))
    branch = branch.astype(BF16).astype(F32)
    final = (mine_ref[...].astype(F32) + 0.5 * branch).astype(BF16).astype(F32)
    squares = final * final
    squares = jnp.sum(squares[:, :128] + squares[:, 128:], axis=1, keepdims=True)
    squares = jnp.broadcast_to(squares, (T, 128))
    zpos = where_ref[2]
    own = jnp.where(zpos < 2, final[:, :128], final[:, 128:])
    own = jnp.where(zpos % 2 == 0, own, pltpu.roll(own, 64, 1))
    turned = {d: own if d == 0 else pltpu.roll(own, (32 * d) % 128, 1) for d in (-1, 0, 1, 2, 3)}
    group = lanes((6, 128)) // 32
    zero = jnp.zeros((2, 128), F32)
    for x in range(4):
        rows = [slice(x * 24 + k * 6, x * 24 + k * 6 + 6) for k in range(4)]
        total = squares[rows[0]]
        for k in range(1, 4):
            total = jnp.where(group == k, squares[rows[k]], total)
        for m in range(2):
            block = turned[-m][rows[0]]
            for k in range(1, 4):
                block = jnp.where(group == k, turned[k - m][rows[k]], block)
            message = jnp.concatenate([block, zero, total, zero], axis=0)
            for peer in range(4):
                send_ref[(x * 2 + m) * 4 + peer] = message


def exit_unpack_kernel(where_ref, recv_ref, out_ref):
    for m in range(2):
        first = (6 + m) * 4
        total = (recv_ref[first][8:16] + recv_ref[first + 1][8:16]) + (recv_ref[first + 2][8:16] + recv_ref[first + 3][8:16])
        block = recv_ref[first + 2 * where_ref[0] + where_ref[1]][0:8]
        block = block * lax.rsqrt(total * (1.0 / D) + EPS)
        rows = [block if k == 0 else pltpu.roll(block, 128 - 32 * k, 1) for k in range(4)]
        out_ref[m] = jnp.concatenate([r[:6, :32] for r in rows], axis=0).astype(BF16)


SMEM_SPEC = pl.BlockSpec(memory_space=pltpu.SMEM)
VMEM_SPEC = pl.BlockSpec(memory_space=pltpu.VMEM)


def call_kernel(kernel, out_shape, count, scratch=()):
    return pl.pallas_call(
        kernel,
        out_shape=out_shape,
        in_specs=[SMEM_SPEC] + [VMEM_SPEC] * count,
        out_specs=[VMEM_SPEC] * len(out_shape),
        scratch_shapes=scratch,
        compiler_params=pltpu.CompilerParams(vmem_limit_bytes=24 * 1024 * 1024),
    )


def flip(v, axes, bits):
    size = lax.axis_size(axes)
    return lax.ppermute(v, axes, [(i, i ^ bits) for i in range(size)])


def swap_pairs(first, size):
    other = {}
    for low in range(first % 2, size - 1, 2):
        other[low], other[low + 1] = low + 1, low
    return [(i, other.get(i, i)) for i in range(size)]


def per_device(
    micro_in,
    norm_gain,
    proj_gate,
    proj_value,
    proj_write,
    proj_read,
    proj_step,
    step_bias,
    decay_log,
    skip_gain,
    conv_value,
    conv_write,
    conv_read,
    proj_out,
):
    sections = lax.axis_size("pp")
    half = lax.axis_index("yh")
    core = lax.axis_index("tc")
    zpos = lax.axis_index("tz")
    where = jnp.stack([half, core, zpos]).astype(jnp.int32)

    shape = jax.ShapeDtypeStruct
    raw = (
        micro_in,
        proj_gate[0, :, 0, 0, :].T,
        proj_value[0, :, 0, 0, :].T,
        proj_step[0, :, :, 0, 0].T,
        proj_out[0, 0, 0],
        conv_value.reshape(5, 1, 64),
        step_bias.reshape(1, 2),
        decay_log.reshape(1, 2),
        skip_gain.reshape(1, 1),
        norm_gain,
    )
    order = (1, 2, 4, 3, 5, 6, 7, 8, 9, 0)
    send, same, other, gain = pl.pallas_call(
        pack_kernel,
        out_shape=[
            shape((128, 8, 128), BF16),
            shape((ROWS, D), BF16),
            shape((ROWS, D), BF16),
            shape((1, D), F32),
        ],
        in_specs=[SMEM_SPEC] + [pl.BlockSpec(memory_space=pltpu.HBM)] * len(raw),
        out_specs=[VMEM_SPEC] * 4,
        scratch_shapes=[pltpu.VMEM(raw[i].shape, raw[i].dtype) for i in order]
        + [pltpu.SemaphoreType.DMA((len(raw),))],
        compiler_params=pltpu.CompilerParams(vmem_limit_bytes=24 * 1024 * 1024),
    )(where, *[pltpu.with_memory_space_constraint(v, pltpu.HBM) if i in (0, 1, 2, 3, 4, 5, 9) else v for i, v in enumerate(raw)])
    w1 = flip(other, FS, 1)
    w2 = flip(same, FS, 2)
    w3 = flip(other, FS, 3)
    recv = lax.all_to_all(send, ALL, 0, 0)

    taps_w = conv_write.reshape(5, 1, 128)
    taps_r = conv_read.reshape(5, 1, 128)
    params = (same, w1, w2, w3, proj_write[0, :, 0, :], proj_read[0, :, 0, :], gain, taps_w, taps_r)
    quarter = shape((T, 256), BF16)
    outs = [shape((T, 256), F32), quarter]
    pad = pltpu.VMEM((T + 16, 768), F32)
    mine, own, far = call_kernel(
        entry_section_kernel, [quarter, *outs], 10, [pad, pltpu.VMEM((4, T, 256), F32)]
    )(where, recv, *params)
    for s in range(sections):
        got = flip(far, "tc", 1)
        mixed = (own + got.astype(F32)).astype(BF16)
        others = [flip(mixed, "tz", d) for d in (1, 2, 3)]
        if s + 1 == sections:
            break
        r1, r2, r3 = [v.astype(F32) for v in others]
        branch = ((mixed.astype(F32) + r1) + (r2 + r3)).astype(BF16).astype(F32)
        produced = (mine.astype(F32) + 0.5 * branch).astype(BF16)
        hop = swap_pairs(s, sections)
        hop_flip = [(2 * i + h, 2 * j + 1 - h) for i, j in hop for h in range(2)]
        a = lax.ppermute(produced, "pp", hop)
        c = lax.ppermute(produced, ("pp", "yh"), hop_flip)
        b = flip(a, "tc", 1)
        d = flip(c, "tc", 1)
        mine = a
        own, far = call_kernel(relay_section_kernel, outs, 13, [pad])(where, a, b, c, d, *params)

    (send,) = call_kernel(exit_pack_kernel, [shape((32, 16, 128), F32)], 5)(where, mine, mixed, *others)
    recv = lax.all_to_all(send, ("pp", "ym", "yh", "tc"), 0, 0)
    (result,) = call_kernel(exit_unpack_kernel, [shape((2, T // sections, 32), BF16)], 1)(where, recv)
    return result


def solution(mesh):
    split = Mesh(
        mesh.devices.reshape(mesh.shape["pp"], 2, 2, 4, 2), ("pp", "ym", "yh", "tz", "tc")
    )
    in_specs = (
        P(None, "pp", TP + FS),
        P("pp", None),
        P("pp", None, TP, FS, None),
        P("pp", None, TP, FS, None),
        P("pp", None, TP, None),
        P("pp", None, TP, None),
        P("pp", None, None, TP, FS),
        P("pp", None, TP, FS),
        P("pp", None, TP, FS),
        P("pp", TP, FS),
        P("pp", None, TP, FS, None),
        P("pp", None, TP, None),
        P("pp", None, TP, None),
        P("pp", TP, FS, None, None),
    )
    out_specs = P(None, "pp", TP + FS)
    return jax.shard_map(
        per_device, mesh=split, in_specs=in_specs, out_specs=out_specs, check_vma=False
    )
```

```python
import jax
import jax.numpy as jnp
from jax import lax
from jax.experimental import pallas as pl
from jax.experimental.pallas import tpu as pltpu
from jax.sharding import Mesh
from jax.sharding import PartitionSpec as P


FS = ("ym", "yh")
TP = ("tz", "tc")
BLOCKS = ("pp", "tz", "tc")
EPS = 1e-06
T = 96
D = 1024
F32 = jnp.float32
BF16 = jnp.bfloat16
ROWS = 168


def lanes(shape):
    return lax.broadcasted_iota(jnp.int32, shape, len(shape) - 1)


def split3(v):
    hi = v.astype(BF16).astype(F32)
    mid = (v - hi).astype(BF16).astype(F32)
    low = v - hi - mid
    return hi, mid, low


def permuted(v):
    group = lanes((v.shape[0], 128)) // 32
    out = []
    for h in range(2):
        for c in range(2):
            for p in range(2):
                block = None
                for g in range(4):
                    zz, m = g // 2, g % 2
                    n = (2 * p + zz) * 2 + c
                    moved = v[:, n * 128 : (n + 1) * 128]
                    turn = (64 * zz - 32 * m - 32 * h) % 128
                    if turn:
                        moved = pltpu.roll(moved, turn, 1)
                    block = moved if block is None else jnp.where(group == g, moved, block)
                out.append(block)
    return out


def pack_kernel(
    where_ref,
    micro_hbm,
    gate_hbm,
    value_hbm,
    step_hbm,
    out_hbm,
    taps_hbm,
    bias_hbm,
    decay_hbm,
    skip_hbm,
    gain_hbm,
    near_ref,
    away_ref,
    same_ref,
    other_ref,
    gain_out,
    *scratch,
):
    sources = (
        gate_hbm,
        value_hbm,
        out_hbm,
        step_hbm,
        taps_hbm,
        bias_hbm,
        decay_hbm,
        skip_hbm,
        gain_hbm,
        micro_hbm,
    )
    buffers, sems = scratch[:-1], scratch[-1]
    copies = [pltpu.make_async_copy(s, b, sems.at[i]) for i, (s, b) in enumerate(zip(sources, buffers))]
    for copy in copies:
        copy.start()
    for copy in copies:
        copy.wait()
    gate_ref, value_ref, out_ref, step_ref, taps_ref, bias_ref, decay_ref, skip_ref, gain_ref, micro_ref = buffers
    core = where_ref[1] == 0
    half = where_ref[0] == 0
    gate = jnp.concatenate(permuted(gate_ref[...].astype(F32)), axis=1).astype(BF16)
    value = jnp.concatenate(permuted(value_ref[...].astype(F32)), axis=1).astype(BF16)
    step = jnp.concatenate(permuted(step_ref[...].astype(F32)), axis=1)
    gain_out[...] = jnp.concatenate(permuted(gain_ref[...]), axis=1)
    blank = jnp.zeros((1, 64), F32)
    wide = lambda ref, k: jnp.broadcast_to(ref[:, k : k + 1], (1, 128))
    row_a = [piece for k in range(5) for piece in (blank, taps_ref[k])]
    row_a = jnp.concatenate(row_a + [wide(bias_ref, 0), wide(bias_ref, 1), blank, blank], axis=1)
    row_b = [wide(decay_ref, 0), wide(decay_ref, 1), wide(skip_ref, 0)] + [blank] * 10
    row_b = jnp.concatenate(row_b, axis=1)
    misc = jnp.concatenate([step, *split3(row_a), *split3(row_b)], axis=0).astype(BF16)
    out = permuted(out_ref[...].astype(F32))
    halves = []
    for h in range(2):
        first, second = out[4 * h : 4 * h + 2], out[4 * h + 2 : 4 * h + 4]
        own = [jnp.where(core, a, b) for a, b in zip(first, second)]
        far = [jnp.where(core, b, a) for a, b in zip(first, second)]
        halves.append(jnp.concatenate(own + far, axis=1))
    for ref, pick in ((same_ref, half), (other_ref, jnp.logical_not(half))):
        part = jnp.where(pick, halves[0], halves[1])
        ref[0:64] = gate
        ref[64:128] = value
        ref[128:160] = jnp.concatenate([part[0:32], part[32:64]], axis=1).astype(BF16)
        ref[160:168] = misc
    first = where_ref[3] == 0
    near_ref[...] = jnp.where(first, micro_ref[0], micro_ref[1])
    away_ref[...] = jnp.where(first, micro_ref[1], micro_ref[0])


def block_kernel(where_ref, r0_ref, r1_ref, r2_ref, r3_ref, send_ref):
    y = 2 * where_ref[3] + where_ref[0]
    group = lanes((24, 128)) // 32
    blank = jnp.zeros((24, 96), F32)
    block = jnp.zeros((24, 128), F32)
    for bits, ref in enumerate((r0_ref, r1_ref, r2_ref, r3_ref)):
        wide = jnp.concatenate([ref[...].astype(F32), blank], axis=1)
        for k in range(4):
            moved = wide if k == 0 else pltpu.roll(wide, 32 * k, 1)
            block = jnp.where((group == k) & ((y ^ bits) == k), moved, block)
    block = block.astype(BF16)
    for peer in range(32):
        send_ref[peer] = block


def nt_dot(a, b):
    return lax.dot_general(a, b, (((1,), (1,)), ((), ())), preferred_element_type=F32)


def nn_dot(a, b):
    return lax.dot_general(a, b, (((1,), (0,)), ((), ())), preferred_element_type=F32)


def silu(v):
    return v * jax.nn.sigmoid(v)


def section_body(quarters, weight_refs, write_ref, read_ref, gain_ref, taps_refs, own_ref, far_ref, pad_ref):
    low = lanes((T, 128)) < 64
    total = None
    for pair in quarters:
        for q in pair:
            sq = q * q
            sq = sq[:, :128] + sq[:, 128:]
            total = sq if total is None else total + sq
    scale = lax.rsqrt(jnp.sum(total, axis=1, keepdims=True) * (1.0 / D) + EPS)
    blocks = []
    for h in range(2):
        for c in range(2):
            n = (2 * h + c) * 256
            blocks.append((quarters[h][c] * scale * gain_ref[:, n : n + 256]).astype(BF16))
    normed = jnp.concatenate(blocks, axis=1)

    step_rows = jnp.concatenate([w[160:168].astype(F32)[0:2] for w in weight_refs], axis=0)
    step_raw = nt_dot(step_rows.astype(BF16), normed)
    small = []
    for w in weight_refs:
        misc = w[160:168].astype(F32)
        small.append((misc[2:3] + misc[3:4] + misc[4:5], misc[5:6] + misc[6:7] + misc[7:8]))
    bias = jnp.concatenate([s[0][:, 640 + 128 * d : 640 + 128 * d + T] for s in small for d in range(2)], axis=0)
    decay = jnp.concatenate([s[1][:, 128 * d : 128 * d + T] for s in small for d in range(2)], axis=0)
    raw = step_raw + bias
    dt = jnp.maximum(raw, 0.0) + jnp.log1p(jnp.exp(-jnp.abs(raw)))
    log_decay = dt * (-jnp.exp(decay))
    parts = [s.astype(BF16) for s in split3(log_decay)]
    row_id = lax.broadcasted_iota(jnp.int32, (T, T), 0)
    col_id = lax.broadcasted_iota(jnp.int32, (T, T), 1)
    upto = (row_id <= col_id).astype(F32).astype(BF16)
    since = (row_id >= col_id).astype(F32).astype(BF16)
    fwd_all = (nn_dot(parts[0], upto) + nn_dot(parts[1], upto)) + nn_dot(parts[2], upto)
    bwd_all = (nn_dot(parts[0], since) + nn_dot(parts[1], since)) + nn_dot(parts[2], since)
    odd = lax.broadcasted_iota(jnp.int32, (8, T), 0) % 2 == 1
    cum = jnp.where(odd, bwd_all, fwd_all)
    cum_pad = jnp.concatenate([cum, jnp.zeros((8, 128 - T), F32)], axis=1)
    cum_cols = cum_pad.T[:T]

    gv01 = nt_dot(normed, jnp.concatenate([weight_refs[0][0:128], weight_refs[1][0:128]], axis=0))
    gv23 = nt_dot(normed, jnp.concatenate([weight_refs[2][0:128], weight_refs[3][0:128]], axis=0))
    wr_rows = [
        jnp.concatenate([r[n * 128 + y * 32 : n * 128 + y * 32 + 32] for r in (write_ref, read_ref)], axis=1)
        for h in range(2)
        for c in range(2)
        for n in (c, 2 + c, 4 + c, 6 + c)
        for y in (h, 2 + h)
    ]
    wr = nn_dot(normed, jnp.concatenate(wr_rows, axis=0))
    pad_ref[0:8] = jnp.zeros((8, 768), F32)
    pad_ref[8 + T : 16 + T] = jnp.zeros((8, 768), F32)
    pad_ref[8 : 8 + T, 0:256] = gv01.astype(BF16).astype(F32)
    pad_ref[8 : 8 + T, 256:512] = gv23.astype(BF16).astype(F32)
    pad_ref[8 : 8 + T, 512:768] = wr.astype(BF16).astype(F32)
    acts = []
    for g in range(6):
        span = slice(g * 128, (g + 1) * 128)
        acc = None
        for k in range(5):
            tap = small[g][0][:, k * 128 : (k + 1) * 128] if g < 4 else taps_refs[g - 4][k]
            term = pad_ref[6 + k : 6 + k + T, span] * tap
            acc = term if acc is None else acc + term
        acts.append(silu(acc).astype(BF16))
    scores = nt_dot(acts[5], acts[4])
    lower = row_id >= col_id
    diagonal = row_id == col_id
    gated = []
    for j in range(4):
        fc = cum_cols[:, 2 * j : 2 * j + 1]
        bc = cum_cols[:, 2 * j + 1 : 2 * j + 2]
        fr = cum[2 * j : 2 * j + 1]
        br = cum[2 * j + 1 : 2 * j + 2]
        d0 = dt[2 * j : 2 * j + 1]
        d1 = dt[2 * j + 1 : 2 * j + 2]
        mix = jnp.exp(jnp.where(lower, fc - fr, bc - br)) * jnp.where(lower, d0, d1)
        mix = mix + jnp.where(diagonal, d1, 0.0)
        combined = scores * mix
        high = combined.astype(BF16)
        rest = (combined - high.astype(F32)).astype(BF16)
        y = nn_dot(high, acts[j]) + nn_dot(rest, acts[j])
        y = y + small[j][1][:, 256:384] * acts[j].astype(F32)
        gate = pltpu.roll(pad_ref[8 : 8 + T, j * 128 : (j + 1) * 128], 64, 1)
        gated.append(y * silu(gate))
    pairs = [jnp.where(low, pltpu.roll(gated[2 * i], 64, 1), gated[2 * i + 1]).astype(BF16) for i in range(2)]
    gated_all = jnp.concatenate(pairs, axis=1)
    for side, ref in ((0, own_ref), (1, far_ref)):
        weight = jnp.concatenate(
            [
                w[128:160, 512 * r + 256 * side : 512 * r + 256 * side + 256]
                for w in weight_refs
                for r in range(2)
            ],
            axis=0,
        )
        ref[...] = nn_dot(gated_all, weight).astype(ref.dtype)


def entry_section_kernel(where_ref, recv_ref, *refs):
    *rest, quarter_out, own_ref, far_ref, pad_ref, quarter_ref = refs
    tokens = [
        jnp.concatenate([recv_ref[x * 8 + n].astype(F32) for x in range(4)], axis=0) for n in range(8)
    ]
    blocks = permuted(jnp.concatenate(tokens, axis=1))
    for q in range(4):
        quarter_ref[q] = jnp.concatenate(blocks[2 * q : 2 * q + 2], axis=1)
    quarters = [[quarter_ref[2 * h + c] for c in range(2)] for h in range(2)]
    mine = quarter_ref[2 * where_ref[0] + where_ref[1]]
    quarter_out[...] = mine.astype(BF16)
    section_body(quarters, rest[0:4], *rest[4:7], rest[7:9], own_ref, far_ref, pad_ref)


def relay_section_kernel(where_ref, a_ref, b_ref, c_ref, d_ref, *refs):
    *rest, own_ref, far_ref, pad_ref = refs
    half = where_ref[0] == 0
    core = where_ref[1] == 0
    a, b, c, d = [r[...].astype(F32) for r in (a_ref, b_ref, c_ref, d_ref)]
    own0, own1 = jnp.where(half, a, c), jnp.where(half, c, a)
    far0, far1 = jnp.where(half, b, d), jnp.where(half, d, b)
    quarters = [
        [jnp.where(core, own0, far0), jnp.where(core, far0, own0)],
        [jnp.where(core, own1, far1), jnp.where(core, far1, own1)],
    ]
    section_body(quarters, rest[0:4], *rest[4:7], rest[7:9], own_ref, far_ref, pad_ref)


def exit_pack_kernel(where_ref, mine_ref, m0_ref, m1_ref, m2_ref, m3_ref, send_ref):
    branch = (m0_ref[...].astype(F32) + m1_ref[...].astype(F32)) + (m2_ref[...].astype(F32) + m3_ref[...].astype(F32))
    branch = branch.astype(BF16).astype(F32)
    final = (mine_ref[...].astype(F32) + 0.5 * branch).astype(BF16).astype(F32)
    squares = final * final
    squares = jnp.sum(squares[:, :128] + squares[:, 128:], axis=1, keepdims=True)
    squares = jnp.broadcast_to(squares, (T, 128))
    zpos = where_ref[2]
    own = jnp.where(zpos < 2, final[:, :128], final[:, 128:])
    own = jnp.where(zpos % 2 == 0, own, pltpu.roll(own, 64, 1))
    turned = {d: own if d == 0 else pltpu.roll(own, (32 * d) % 128, 1) for d in (-1, 0, 1, 2, 3)}
    lane = lanes((6, 128))
    group = lane // 32
    spot = lane % 32 == lax.broadcasted_iota(jnp.int32, (6, 128), 0)
    for x in range(4):
        rows = [slice(x * 24 + k * 6, x * 24 + k * 6 + 6) for k in range(4)]
        total = squares[rows[0]]
        for k in range(1, 4):
            total = jnp.where(group == k, squares[rows[k]], total)
        total = jnp.sum(jnp.where(spot, total, 0.0), axis=0, keepdims=True)
        parts = split3(total)
        for m in range(2):
            block = turned[-m][rows[0]]
            for k in range(1, 4):
                block = jnp.where(group == k, turned[k - m][rows[k]], block)
            message = jnp.concatenate([block, parts[0], parts[1]], axis=0).astype(BF16)
            for peer in range(4):
                send_ref[(x * 2 + m) * 4 + peer] = message


def exit_unpack_kernel(where_ref, recv_ref, out_ref):
    lane = lanes((8, 128))
    spot = lane % 32 == lax.broadcasted_iota(jnp.int32, (8, 128), 0)
    same_group = (
        lax.broadcasted_iota(jnp.int32, (128, 128), 0) // 32 == lanes((128, 128)) // 32
    ).astype(F32).astype(BF16)
    for m in range(2):
        first = (6 + m) * 4
        sums = [recv_ref[first + i].astype(F32) for i in range(4)]
        total = (sums[0][6:7] + sums[0][7:8]) + (sums[1][6:7] + sums[1][7:8])
        total = total + ((sums[2][6:7] + sums[2][7:8]) + (sums[3][6:7] + sums[3][7:8]))
        spread = jnp.where(spot, jnp.broadcast_to(total, (8, 128)), 0.0)
        parts = [p.astype(BF16) for p in split3(spread)]
        total = (nn_dot(parts[0], same_group) + nn_dot(parts[1], same_group)) + nn_dot(parts[2], same_group)
        block = recv_ref[first + 2 * where_ref[0] + where_ref[1]].astype(F32)
        block = block * lax.rsqrt(total * (1.0 / D) + EPS)
        rows = [block if k == 0 else pltpu.roll(block, 128 - 32 * k, 1) for k in range(4)]
        out_ref[m] = jnp.concatenate([r[:6, :32] for r in rows], axis=0).astype(BF16)


SMEM_SPEC = pl.BlockSpec(memory_space=pltpu.SMEM)
VMEM_SPEC = pl.BlockSpec(memory_space=pltpu.VMEM)


def call_kernel(kernel, out_shape, count, scratch=()):
    return pl.pallas_call(
        kernel,
        out_shape=out_shape,
        in_specs=[SMEM_SPEC] + [VMEM_SPEC] * count,
        out_specs=[VMEM_SPEC] * len(out_shape),
        scratch_shapes=scratch,
        compiler_params=pltpu.CompilerParams(vmem_limit_bytes=24 * 1024 * 1024),
    )


def flip(v, axes, bits):
    size = lax.axis_size(axes)
    return lax.ppermute(v, axes, [(i, i ^ bits) for i in range(size)])


def swap_pairs(first, size):
    pairs = []
    for low in range(first % 2, size, 2):
        high = (low + 1) % size
        pairs += [(low, high), (high, low)]
    return pairs


def per_device(
    micro_in,
    norm_gain,
    proj_gate,
    proj_value,
    proj_write,
    proj_read,
    proj_step,
    step_bias,
    decay_log,
    skip_gain,
    conv_value,
    conv_write,
    conv_read,
    proj_out,
):
    sections = lax.axis_size("pp")
    half = lax.axis_index("yh")
    core = lax.axis_index("tc")
    zpos = lax.axis_index("tz")
    where = jnp.stack([half, core, zpos, lax.axis_index("ym")]).astype(jnp.int32)

    shape = jax.ShapeDtypeStruct
    raw = (
        micro_in,
        proj_gate[0, :, 0, 0, :].T,
        proj_value[0, :, 0, 0, :].T,
        proj_step[0, :, :, 0, 0].T,
        proj_out[0, 0, 0],
        conv_value.reshape(5, 1, 64),
        step_bias.reshape(1, 2),
        decay_log.reshape(1, 2),
        skip_gain.reshape(1, 1),
        norm_gain,
    )
    order = (1, 2, 4, 3, 5, 6, 7, 8, 9, 0)
    near, away, same, other, gain = pl.pallas_call(
        pack_kernel,
        out_shape=[
            shape((T // 4, 32), BF16),
            shape((T // 4, 32), BF16),
            shape((ROWS, D), BF16),
            shape((ROWS, D), BF16),
            shape((1, D), F32),
        ],
        in_specs=[SMEM_SPEC] + [pl.BlockSpec(memory_space=pltpu.HBM)] * len(raw),
        out_specs=[VMEM_SPEC] * 5,
        scratch_shapes=[pltpu.VMEM(raw[i].shape, raw[i].dtype) for i in order]
        + [pltpu.SemaphoreType.DMA((len(raw),))],
        compiler_params=pltpu.CompilerParams(vmem_limit_bytes=24 * 1024 * 1024),
    )(where, *[pltpu.with_memory_space_constraint(v, pltpu.HBM) if i in (0, 1, 2, 3, 4, 5, 9) else v for i, v in enumerate(raw)])
    r1 = flip(near, FS, 1)
    r2 = flip(away, FS, 2)
    r3 = flip(away, FS, 3)
    w1 = flip(other, FS, 1)
    w2 = flip(same, FS, 2)
    w3 = flip(other, FS, 3)
    (send,) = call_kernel(block_kernel, [shape((32, T // 4, 128), BF16)], 4)(where, near, r1, r2, r3)
    recv = lax.all_to_all(send, BLOCKS, 0, 0)

    taps_w = conv_write.reshape(5, 1, 128)
    taps_r = conv_read.reshape(5, 1, 128)
    params = (same, w1, w2, w3, proj_write[0, :, 0, :], proj_read[0, :, 0, :], gain, taps_w, taps_r)
    quarter = shape((T, 256), BF16)
    outs = [shape((T, 256), F32), quarter]
    pad = pltpu.VMEM((T + 16, 768), F32)
    mine, own, far = call_kernel(
        entry_section_kernel, [quarter, *outs], 10, [pad, pltpu.VMEM((4, T, 256), F32)]
    )(where, recv, *params)
    for s in range(sections):
        got = flip(far, "tc", 1)
        mixed = (own + got.astype(F32)).astype(BF16)
        others = [flip(mixed, "tz", d) for d in (1, 2, 3)]
        if s + 1 == sections:
            break
        r1, r2, r3 = [v.astype(F32) for v in others]
        branch = ((mixed.astype(F32) + r1) + (r2 + r3)).astype(BF16).astype(F32)
        produced = (mine.astype(F32) + 0.5 * branch).astype(BF16)
        hop = swap_pairs(s, sections)
        hop_flip = [(2 * i + h, 2 * j + 1 - h) for i, j in hop for h in range(2)]
        a = lax.ppermute(produced, "pp", hop)
        c = lax.ppermute(produced, ("pp", "yh"), hop_flip)
        b = flip(a, "tc", 1)
        d = flip(c, "tc", 1)
        mine = a
        own, far = call_kernel(relay_section_kernel, outs, 13, [pad])(where, a, b, c, d, *params)

    (send,) = call_kernel(exit_pack_kernel, [shape((32, 8, 128), BF16)], 5)(where, mine, mixed, *others)
    recv = lax.all_to_all(send, ("pp", "ym", "yh", "tc"), 0, 0)
    (result,) = call_kernel(exit_unpack_kernel, [shape((2, T // sections, 32), BF16)], 1)(where, recv)
    return result


def solution(mesh):
    split = Mesh(
        mesh.devices.reshape(mesh.shape["pp"], 2, 2, 4, 2), ("pp", "ym", "yh", "tz", "tc")
    )
    in_specs = (
        P(None, "pp", TP + FS),
        P("pp", None),
        P("pp", None, TP, FS, None),
        P("pp", None, TP, FS, None),
        P("pp", None, TP, None),
        P("pp", None, TP, None),
        P("pp", None, None, TP, FS),
        P("pp", None, TP, FS),
        P("pp", None, TP, FS),
        P("pp", TP, FS),
        P("pp", None, TP, FS, None),
        P("pp", None, TP, None),
        P("pp", None, TP, None),
        P("pp", TP, FS, None, None),
    )
    out_specs = P(None, "pp", TP + FS)
    return jax.shard_map(
        per_device, mesh=split, in_specs=in_specs, out_specs=out_specs, check_vma=False
    )
```

```python
import jax
import jax.numpy as jnp
from jax import lax
from jax.experimental import pallas as pl
from jax.experimental.pallas import tpu as pltpu
from jax.sharding import Mesh
from jax.sharding import PartitionSpec as P


FS = ("ym", "yh")
TP = ("tz", "tc")
BLOCKS = ("pp", "tz", "tc")
EPS = 1e-06
T = 96
D = 1024
F32 = jnp.float32
BF16 = jnp.bfloat16
ROWS = 168


def lanes(shape):
    return lax.broadcasted_iota(jnp.int32, shape, len(shape) - 1)


def split3(v):
    hi = v.astype(BF16).astype(F32)
    mid = (v - hi).astype(BF16).astype(F32)
    low = v - hi - mid
    return hi, mid, low


def permuted(v):
    group = lanes((v.shape[0], 128)) // 32
    out = []
    for h in range(2):
        for c in range(2):
            for p in range(2):
                block = None
                for g in range(4):
                    zz, m = g // 2, g % 2
                    n = (2 * p + zz) * 2 + c
                    moved = v[:, n * 128 : (n + 1) * 128]
                    turn = (64 * zz - 32 * m - 32 * h) % 128
                    if turn:
                        moved = pltpu.roll(moved, turn, 1)
                    block = moved if block is None else jnp.where(group == g, moved, block)
                out.append(block)
    return out


def pack_kernel(
    where_ref,
    micro_hbm,
    gate_hbm,
    value_hbm,
    step_hbm,
    out_hbm,
    taps_hbm,
    bias_hbm,
    decay_hbm,
    skip_hbm,
    gain_hbm,
    taps_w_hbm,
    taps_r_hbm,
    near_ref,
    away_ref,
    same_ref,
    other_ref,
    gain_out,
    taps_w_out,
    taps_r_out,
    *scratch,
):
    sources = (
        gate_hbm,
        value_hbm,
        out_hbm,
        step_hbm,
        taps_hbm,
        bias_hbm,
        decay_hbm,
        skip_hbm,
        gain_hbm,
        micro_hbm,
        taps_w_hbm,
        taps_r_hbm,
    )
    buffers, sems = (*scratch[:-1], taps_w_out, taps_r_out), scratch[-1]
    copies = [pltpu.make_async_copy(s, b, sems.at[i]) for i, (s, b) in enumerate(zip(sources, buffers))]
    for copy in copies:
        copy.start()
    for copy in copies:
        copy.wait()
    gate_ref, value_ref, out_ref, step_ref, taps_ref, bias_ref, decay_ref, skip_ref, gain_ref, micro_ref = buffers[:10]
    core = where_ref[1] == 0
    half = where_ref[0] == 0
    gate = jnp.concatenate(permuted(gate_ref[...].astype(F32)), axis=1).astype(BF16)
    value = jnp.concatenate(permuted(value_ref[...].astype(F32)), axis=1).astype(BF16)
    step = jnp.concatenate(permuted(step_ref[...].astype(F32)), axis=1)
    gain_out[...] = jnp.concatenate(permuted(gain_ref[...]), axis=1)
    blank = jnp.zeros((1, 64), F32)
    wide = lambda ref, k: jnp.broadcast_to(ref[:, k : k + 1], (1, 128))
    row_a = [piece for k in range(5) for piece in (blank, taps_ref[k])]
    row_a = jnp.concatenate(row_a + [wide(bias_ref, 0), wide(bias_ref, 1), blank, blank], axis=1)
    row_b = [wide(decay_ref, 0), wide(decay_ref, 1), wide(skip_ref, 0)] + [blank] * 10
    row_b = jnp.concatenate(row_b, axis=1)
    misc = jnp.concatenate([step, *split3(row_a), *split3(row_b)], axis=0).astype(BF16)
    out = permuted(out_ref[...].astype(F32))
    halves = []
    for h in range(2):
        first, second = out[4 * h : 4 * h + 2], out[4 * h + 2 : 4 * h + 4]
        own = [jnp.where(core, a, b) for a, b in zip(first, second)]
        far = [jnp.where(core, b, a) for a, b in zip(first, second)]
        halves.append(jnp.concatenate(own + far, axis=1))
    for ref, pick in ((same_ref, half), (other_ref, jnp.logical_not(half))):
        part = jnp.where(pick, halves[0], halves[1])
        ref[0:64] = gate
        ref[64:128] = value
        ref[128:160] = jnp.concatenate([part[0:32], part[32:64]], axis=1).astype(BF16)
        ref[160:168] = misc
    first = where_ref[3] == 0
    near_ref[...] = jnp.where(first, micro_ref[0], micro_ref[1])
    away_ref[...] = jnp.where(first, micro_ref[1], micro_ref[0])


def block_kernel(where_ref, r0_ref, r1_ref, r2_ref, r3_ref, send_ref):
    y = 2 * where_ref[3] + where_ref[0]
    group = lanes((24, 128)) // 32
    blank = jnp.zeros((24, 96), F32)
    block = jnp.zeros((24, 128), F32)
    for bits, ref in enumerate((r0_ref, r1_ref, r2_ref, r3_ref)):
        wide = jnp.concatenate([ref[...].astype(F32), blank], axis=1)
        for k in range(4):
            moved = wide if k == 0 else pltpu.roll(wide, 32 * k, 1)
            block = jnp.where((group == k) & ((y ^ bits) == k), moved, block)
    block = block.astype(BF16)
    for peer in range(32):
        send_ref[peer] = block


def nt_dot(a, b):
    return lax.dot_general(a, b, (((1,), (1,)), ((), ())), preferred_element_type=F32)


def nn_dot(a, b):
    return lax.dot_general(a, b, (((1,), (0,)), ((), ())), preferred_element_type=F32)


def silu(v):
    return v * jax.nn.sigmoid(v)


def section_body(quarters, weight_refs, write_ref, read_ref, gain_ref, taps_refs, own_ref, far_ref, pad_ref):
    low = lanes((T, 128)) < 64
    total = None
    for pair in quarters:
        for q in pair:
            sq = q * q
            sq = sq[:, :128] + sq[:, 128:]
            total = sq if total is None else total + sq
    scale = lax.rsqrt(jnp.sum(total, axis=1, keepdims=True) * (1.0 / D) + EPS)
    blocks = []
    for h in range(2):
        for c in range(2):
            n = (2 * h + c) * 256
            blocks.append((quarters[h][c] * scale * gain_ref[:, n : n + 256]).astype(BF16))
    normed = jnp.concatenate(blocks, axis=1)

    step_rows = jnp.concatenate([w[160:168].astype(F32)[0:2] for w in weight_refs], axis=0)
    step_raw = nt_dot(step_rows.astype(BF16), normed)
    small = []
    for w in weight_refs:
        misc = w[160:168].astype(F32)
        small.append((misc[2:3] + misc[3:4] + misc[4:5], misc[5:6] + misc[6:7] + misc[7:8]))
    bias = jnp.concatenate([s[0][:, 640 + 128 * d : 640 + 128 * d + T] for s in small for d in range(2)], axis=0)
    decay = jnp.concatenate([s[1][:, 128 * d : 128 * d + T] for s in small for d in range(2)], axis=0)
    raw = step_raw + bias
    dt = jnp.maximum(raw, 0.0) + jnp.log1p(jnp.exp(-jnp.abs(raw)))
    log_decay = dt * (-jnp.exp(decay))
    parts = [s.astype(BF16) for s in split3(log_decay)]
    row_id = lax.broadcasted_iota(jnp.int32, (T, T), 0)
    col_id = lax.broadcasted_iota(jnp.int32, (T, T), 1)
    upto = (row_id <= col_id).astype(F32).astype(BF16)
    since = (row_id >= col_id).astype(F32).astype(BF16)
    fwd_all = (nn_dot(parts[0], upto) + nn_dot(parts[1], upto)) + nn_dot(parts[2], upto)
    bwd_all = (nn_dot(parts[0], since) + nn_dot(parts[1], since)) + nn_dot(parts[2], since)
    odd = lax.broadcasted_iota(jnp.int32, (8, T), 0) % 2 == 1
    cum = jnp.where(odd, bwd_all, fwd_all)
    cum_pad = jnp.concatenate([cum, jnp.zeros((8, 128 - T), F32)], axis=1)
    cum_cols = cum_pad.T[:T]

    gv01 = nt_dot(normed, jnp.concatenate([weight_refs[0][0:128], weight_refs[1][0:128]], axis=0))
    gv23 = nt_dot(normed, jnp.concatenate([weight_refs[2][0:128], weight_refs[3][0:128]], axis=0))
    wr_rows = [
        jnp.concatenate([r[n * 128 + y * 32 : n * 128 + y * 32 + 32] for r in (write_ref, read_ref)], axis=1)
        for h in range(2)
        for c in range(2)
        for n in (c, 2 + c, 4 + c, 6 + c)
        for y in (h, 2 + h)
    ]
    wr = nn_dot(normed, jnp.concatenate(wr_rows, axis=0))
    pad_ref[0:8] = jnp.zeros((8, 768), F32)
    pad_ref[8 + T : 16 + T] = jnp.zeros((8, 768), F32)
    pad_ref[8 : 8 + T, 0:256] = gv01.astype(BF16).astype(F32)
    pad_ref[8 : 8 + T, 256:512] = gv23.astype(BF16).astype(F32)
    pad_ref[8 : 8 + T, 512:768] = wr.astype(BF16).astype(F32)
    acts = []
    for g in range(6):
        span = slice(g * 128, (g + 1) * 128)
        acc = None
        for k in range(5):
            tap = small[g][0][:, k * 128 : (k + 1) * 128] if g < 4 else taps_refs[g - 4][k]
            term = pad_ref[6 + k : 6 + k + T, span] * tap
            acc = term if acc is None else acc + term
        acts.append(silu(acc).astype(BF16))
    scores = nt_dot(acts[5], acts[4])
    lower = row_id >= col_id
    diagonal = row_id == col_id
    gated = []
    for j in range(4):
        fc = cum_cols[:, 2 * j : 2 * j + 1]
        bc = cum_cols[:, 2 * j + 1 : 2 * j + 2]
        fr = cum[2 * j : 2 * j + 1]
        br = cum[2 * j + 1 : 2 * j + 2]
        d0 = dt[2 * j : 2 * j + 1]
        d1 = dt[2 * j + 1 : 2 * j + 2]
        mix = jnp.exp(jnp.where(lower, fc - fr, bc - br)) * jnp.where(lower, d0, d1)
        mix = mix + jnp.where(diagonal, d1, 0.0)
        combined = scores * mix
        high = combined.astype(BF16)
        rest = (combined - high.astype(F32)).astype(BF16)
        y = nn_dot(high, acts[j]) + nn_dot(rest, acts[j])
        y = y + small[j][1][:, 256:384] * acts[j].astype(F32)
        gate = pltpu.roll(pad_ref[8 : 8 + T, j * 128 : (j + 1) * 128], 64, 1)
        gated.append(y * silu(gate))
    pairs = [jnp.where(low, pltpu.roll(gated[2 * i], 64, 1), gated[2 * i + 1]).astype(BF16) for i in range(2)]
    gated_all = jnp.concatenate(pairs, axis=1)
    for side, ref in ((0, own_ref), (1, far_ref)):
        weight = jnp.concatenate(
            [
                w[128:160, 512 * r + 256 * side : 512 * r + 256 * side + 256]
                for w in weight_refs
                for r in range(2)
            ],
            axis=0,
        )
        ref[...] = nn_dot(gated_all, weight).astype(ref.dtype)


def entry_section_kernel(where_ref, recv_ref, *refs):
    *rest, quarter_out, own_ref, far_ref, pad_ref, quarter_ref = refs
    tokens = [
        jnp.concatenate([recv_ref[x * 8 + n].astype(F32) for x in range(4)], axis=0) for n in range(8)
    ]
    blocks = permuted(jnp.concatenate(tokens, axis=1))
    for q in range(4):
        quarter_ref[q] = jnp.concatenate(blocks[2 * q : 2 * q + 2], axis=1)
    quarters = [[quarter_ref[2 * h + c] for c in range(2)] for h in range(2)]
    mine = quarter_ref[2 * where_ref[0] + where_ref[1]]
    quarter_out[...] = mine.astype(BF16)
    section_body(quarters, rest[0:4], *rest[4:7], rest[7:9], own_ref, far_ref, pad_ref)


def relay_section_kernel(where_ref, a_ref, b_ref, c_ref, d_ref, *refs):
    *rest, own_ref, far_ref, pad_ref = refs
    half = where_ref[0] == 0
    core = where_ref[1] == 0
    a, b, c, d = [r[...].astype(F32) for r in (a_ref, b_ref, c_ref, d_ref)]
    own0, own1 = jnp.where(half, a, c), jnp.where(half, c, a)
    far0, far1 = jnp.where(half, b, d), jnp.where(half, d, b)
    quarters = [
        [jnp.where(core, own0, far0), jnp.where(core, far0, own0)],
        [jnp.where(core, own1, far1), jnp.where(core, far1, own1)],
    ]
    section_body(quarters, rest[0:4], *rest[4:7], rest[7:9], own_ref, far_ref, pad_ref)


def exit_pack_kernel(where_ref, mine_ref, m0_ref, m1_ref, m2_ref, m3_ref, send_ref):
    branch = (m0_ref[...].astype(F32) + m1_ref[...].astype(F32)) + (m2_ref[...].astype(F32) + m3_ref[...].astype(F32))
    branch = branch.astype(BF16).astype(F32)
    final = (mine_ref[...].astype(F32) + 0.5 * branch).astype(BF16).astype(F32)
    squares = final * final
    squares = jnp.sum(squares[:, :128] + squares[:, 128:], axis=1, keepdims=True)
    squares = jnp.broadcast_to(squares, (T, 128))
    zpos = where_ref[2]
    own = jnp.where(zpos < 2, final[:, :128], final[:, 128:])
    own = jnp.where(zpos % 2 == 0, own, pltpu.roll(own, 64, 1))
    turned = {d: own if d == 0 else pltpu.roll(own, (32 * d) % 128, 1) for d in (-1, 0, 1, 2, 3)}
    lane = lanes((6, 128))
    group = lane // 32
    spot = lane % 32 == lax.broadcasted_iota(jnp.int32, (6, 128), 0)
    for x in range(4):
        rows = [slice(x * 24 + k * 6, x * 24 + k * 6 + 6) for k in range(4)]
        total = squares[rows[0]]
        for k in range(1, 4):
            total = jnp.where(group == k, squares[rows[k]], total)
        total = jnp.sum(jnp.where(spot, total, 0.0), axis=0, keepdims=True)
        parts = split3(total)
        for m in range(2):
            block = turned[-m][rows[0]]
            for k in range(1, 4):
                block = jnp.where(group == k, turned[k - m][rows[k]], block)
            message = jnp.concatenate([block, parts[0], parts[1]], axis=0).astype(BF16)
            for peer in range(4):
                send_ref[(x * 2 + m) * 4 + peer] = message


def exit_unpack_kernel(where_ref, recv_ref, out_ref):
    lane = lanes((8, 128))
    spot = lane % 32 == lax.broadcasted_iota(jnp.int32, (8, 128), 0)
    same_group = (
        lax.broadcasted_iota(jnp.int32, (128, 128), 0) // 32 == lanes((128, 128)) // 32
    ).astype(F32).astype(BF16)
    parts = []
    for m in range(2):
        first = (6 + m) * 4
        sums = [recv_ref[first + i].astype(F32) for i in range(4)]
        total = (sums[0][6:7] + sums[0][7:8]) + (sums[1][6:7] + sums[1][7:8])
        total = total + ((sums[2][6:7] + sums[2][7:8]) + (sums[3][6:7] + sums[3][7:8]))
        parts += split3(jnp.where(spot, jnp.broadcast_to(total, (8, 128)), 0.0))
    spread = nn_dot(jnp.concatenate(parts, axis=0).astype(BF16), same_group)
    for m in range(2):
        total = (spread[24 * m : 24 * m + 8] + spread[24 * m + 8 : 24 * m + 16]) + spread[24 * m + 16 : 24 * m + 24]
        block = recv_ref[(6 + m) * 4 + 2 * where_ref[0] + where_ref[1]].astype(F32)
        block = block * lax.rsqrt(total * (1.0 / D) + EPS)
        rows = [block if k == 0 else pltpu.roll(block, 128 - 32 * k, 1) for k in range(4)]
        out_ref[m] = jnp.concatenate([r[:6, :32] for r in rows], axis=0).astype(BF16)


SMEM_SPEC = pl.BlockSpec(memory_space=pltpu.SMEM)
VMEM_SPEC = pl.BlockSpec(memory_space=pltpu.VMEM)


def call_kernel(kernel, out_shape, count, scratch=()):
    return pl.pallas_call(
        kernel,
        out_shape=out_shape,
        in_specs=[SMEM_SPEC] + [VMEM_SPEC] * count,
        out_specs=[VMEM_SPEC] * len(out_shape),
        scratch_shapes=scratch,
        compiler_params=pltpu.CompilerParams(vmem_limit_bytes=24 * 1024 * 1024),
    )


def flip(v, axes, bits):
    size = lax.axis_size(axes)
    return lax.ppermute(v, axes, [(i, i ^ bits) for i in range(size)])


def hop_pairs(first, size, flip_half):
    pairs = []
    for i in range(size):
        j = i + 1 if (i - first) % 2 == 0 else i - 1
        for h in range(2):
            for c in range(2):
                if 0 <= j < size:
                    target = (j, 1 - h if flip_half else h, c)
                else:
                    target = (i, h, 1 - c)
                pairs.append((4 * i + 2 * h + c, 4 * target[0] + 2 * target[1] + target[2]))
    return pairs


def per_device(
    micro_in,
    norm_gain,
    proj_gate,
    proj_value,
    proj_write,
    proj_read,
    proj_step,
    step_bias,
    decay_log,
    skip_gain,
    conv_value,
    conv_write,
    conv_read,
    proj_out,
):
    sections = lax.axis_size("pp")
    half = lax.axis_index("yh")
    core = lax.axis_index("tc")
    zpos = lax.axis_index("tz")
    where = jnp.stack([half, core, zpos, lax.axis_index("ym")]).astype(jnp.int32)

    shape = jax.ShapeDtypeStruct
    raw = (
        micro_in,
        proj_gate[0, :, 0, 0, :].T,
        proj_value[0, :, 0, 0, :].T,
        proj_step[0, :, :, 0, 0].T,
        proj_out[0, 0, 0],
        conv_value.reshape(5, 1, 64),
        step_bias.reshape(1, 2),
        decay_log.reshape(1, 2),
        skip_gain.reshape(1, 1),
        norm_gain,
        conv_write.reshape(5, 1, 128),
        conv_read.reshape(5, 1, 128),
    )
    order = (1, 2, 4, 3, 5, 6, 7, 8, 9, 0)
    near, away, same, other, gain, taps_w, taps_r = pl.pallas_call(
        pack_kernel,
        out_shape=[
            shape((T // 4, 32), BF16),
            shape((T // 4, 32), BF16),
            shape((ROWS, D), BF16),
            shape((ROWS, D), BF16),
            shape((1, D), F32),
            shape((5, 1, 128), F32),
            shape((5, 1, 128), F32),
        ],
        in_specs=[SMEM_SPEC] + [pl.BlockSpec(memory_space=pltpu.HBM)] * len(raw),
        out_specs=[VMEM_SPEC] * 7,
        scratch_shapes=[pltpu.VMEM(raw[i].shape, raw[i].dtype) for i in order]
        + [pltpu.SemaphoreType.DMA((len(raw),))],
        compiler_params=pltpu.CompilerParams(vmem_limit_bytes=24 * 1024 * 1024),
    )(where, *[pltpu.with_memory_space_constraint(v, pltpu.HBM) if i != 8 else v for i, v in enumerate(raw)])
    r1 = flip(near, FS, 1)
    r2 = flip(away, FS, 2)
    r3 = flip(away, FS, 3)
    w1 = flip(other, FS, 1)
    w2 = flip(same, FS, 2)
    w3 = flip(other, FS, 3)
    (send,) = call_kernel(block_kernel, [shape((32, T // 4, 128), BF16)], 4)(where, near, r1, r2, r3)
    recv = lax.all_to_all(send, BLOCKS, 0, 0)

    params = (same, w1, w2, w3, proj_write[0, :, 0, :], proj_read[0, :, 0, :], gain, taps_w, taps_r)
    quarter = shape((T, 256), BF16)
    outs = [shape((T, 256), F32), quarter]
    pad = pltpu.VMEM((T + 16, 768), F32)
    mine, own, far = call_kernel(
        entry_section_kernel, [quarter, *outs], 10, [pad, pltpu.VMEM((4, T, 256), F32)]
    )(where, recv, *params)
    for s in range(sections):
        got = flip(far, "tc", 1)
        mixed = (own + got.astype(F32)).astype(BF16)
        others = [flip(mixed, "tz", d) for d in (1, 2, 3)]
        if s + 1 == sections:
            break
        r1, r2, r3 = [v.astype(F32) for v in others]
        branch = ((mixed.astype(F32) + r1) + (r2 + r3)).astype(BF16).astype(F32)
        produced = (mine.astype(F32) + 0.5 * branch).astype(BF16)
        a, c = [lax.ppermute(produced, ("pp", "yh", "tc"), hop_pairs(s, sections, f)) for f in (False, True)]
        b = flip(a, "tc", 1)
        d = flip(c, "tc", 1)
        mine = a
        own, far = call_kernel(relay_section_kernel, outs, 13, [pad])(where, a, b, c, d, *params)

    (send,) = call_kernel(exit_pack_kernel, [shape((32, 8, 128), BF16)], 5)(where, mine, mixed, *others)
    recv = lax.all_to_all(send, ("pp", "ym", "yh", "tc"), 0, 0)
    (result,) = call_kernel(exit_unpack_kernel, [shape((2, T // sections, 32), BF16)], 1)(where, recv)
    return result


def solution(mesh):
    split = Mesh(
        mesh.devices.reshape(mesh.shape["pp"], 2, 2, 4, 2), ("pp", "ym", "yh", "tz", "tc")
    )
    in_specs = (
        P(None, "pp", TP + FS),
        P("pp", None),
        P("pp", None, TP, FS, None),
        P("pp", None, TP, FS, None),
        P("pp", None, TP, None),
        P("pp", None, TP, None),
        P("pp", None, None, TP, FS),
        P("pp", None, TP, FS),
        P("pp", None, TP, FS),
        P("pp", TP, FS),
        P("pp", None, TP, FS, None),
        P("pp", None, TP, None),
        P("pp", None, TP, None),
        P("pp", TP, FS, None, None),
    )
    out_specs = P(None, "pp", TP + FS)
    return jax.shard_map(
        per_device, mesh=split, in_specs=in_specs, out_specs=out_specs, check_vma=False
    )
```

```python
import jax
import jax.numpy as jnp
from jax import lax
from jax.experimental import pallas as pl
from jax.experimental.pallas import tpu as pltpu
from jax.sharding import Mesh
from jax.sharding import PartitionSpec as P


FS = ("ym", "yh")
TP = ("tz", "tc")
BLOCKS = ("pp", "tz", "tc")
EPS = 1e-06
T = 96
D = 1024
F32 = jnp.float32
BF16 = jnp.bfloat16
ROWS = 168


def lanes(shape):
    return lax.broadcasted_iota(jnp.int32, shape, len(shape) - 1)


def split3(v):
    hi = v.astype(BF16).astype(F32)
    mid = (v - hi).astype(BF16).astype(F32)
    low = v - hi - mid
    return hi, mid, low


def flag(where_ref, row, width=256):
    return where_ref[row : row + 1, :width] == 0


def permuted(v):
    group = lanes((v.shape[0], 128)) // 32
    out = []
    for h in range(2):
        for c in range(2):
            for p in range(2):
                block = None
                for g in range(4):
                    zz, m = g // 2, g % 2
                    n = (2 * p + zz) * 2 + c
                    moved = v[:, n * 128 : (n + 1) * 128]
                    turn = (64 * zz - 32 * m - 32 * h) % 128
                    if turn:
                        moved = pltpu.roll(moved, turn, 1)
                    block = moved if block is None else jnp.where(group == g, moved, block)
                out.append(block)
    return out


def pack_kernel(
    where_ref,
    micro_hbm,
    gate_hbm,
    value_hbm,
    step_hbm,
    out_hbm,
    taps_hbm,
    bias_hbm,
    decay_hbm,
    skip_hbm,
    gain_hbm,
    taps_w_hbm,
    taps_r_hbm,
    near_ref,
    away_ref,
    same_ref,
    other_ref,
    gain_out,
    taps_w_out,
    taps_r_out,
    *scratch,
):
    sources = (
        gate_hbm,
        value_hbm,
        out_hbm,
        step_hbm,
        taps_hbm,
        bias_hbm,
        decay_hbm,
        skip_hbm,
        gain_hbm,
        micro_hbm,
        taps_w_hbm,
        taps_r_hbm,
    )
    buffers, sems = (*scratch[:-1], taps_w_out, taps_r_out), scratch[-1]
    copies = [pltpu.make_async_copy(s, b, sems.at[i]) for i, (s, b) in enumerate(zip(sources, buffers))]
    for copy in copies:
        copy.start()
    for copy in copies:
        copy.wait()
    gate_ref, value_ref, out_ref, step_ref, taps_ref, bias_ref, decay_ref, skip_ref, gain_ref, micro_ref = buffers[:10]
    core = flag(where_ref, 1, 128)
    half = flag(where_ref, 0, 128)
    gate = jnp.concatenate(permuted(gate_ref[...].astype(F32)), axis=1).astype(BF16)
    value = jnp.concatenate(permuted(value_ref[...].astype(F32)), axis=1).astype(BF16)
    step = jnp.concatenate(permuted(step_ref[...].astype(F32)), axis=1)
    gain_out[...] = jnp.concatenate(permuted(gain_ref[...]), axis=1)
    blank = jnp.zeros((1, 64), F32)
    wide = lambda ref, k: jnp.broadcast_to(ref[:, k : k + 1], (1, 128))
    row_a = [piece for k in range(5) for piece in (blank, taps_ref[k])]
    row_a = jnp.concatenate(row_a + [wide(bias_ref, 0), wide(bias_ref, 1), blank, blank], axis=1)
    row_b = [wide(decay_ref, 0), wide(decay_ref, 1), wide(skip_ref, 0)] + [blank] * 10
    row_b = jnp.concatenate(row_b, axis=1)
    misc = jnp.concatenate([step, *split3(row_a), *split3(row_b)], axis=0).astype(BF16)
    out = permuted(out_ref[...].astype(F32))
    halves = []
    for h in range(2):
        first, second = out[4 * h : 4 * h + 2], out[4 * h + 2 : 4 * h + 4]
        own = [jnp.where(core, a, b) for a, b in zip(first, second)]
        far = [jnp.where(core, b, a) for a, b in zip(first, second)]
        halves.append(own + far)
    for ref, pair in ((same_ref, zip(*halves)), (other_ref, zip(*halves[::-1]))):
        part = jnp.concatenate([jnp.where(half, a, b) for a, b in pair], axis=1)
        ref[0:64] = gate
        ref[64:128] = value
        ref[128:160] = jnp.concatenate([part[0:32], part[32:64]], axis=1).astype(BF16)
        ref[160:168] = misc
    first = flag(where_ref, 4, 32)
    micro = [micro_ref[m].astype(F32) for m in range(2)]
    near_ref[...] = jnp.where(first, micro[0], micro[1]).astype(BF16)
    away_ref[...] = jnp.where(first, micro[1], micro[0]).astype(BF16)


def block_kernel(where_ref, r0_ref, r1_ref, r2_ref, r3_ref, send_ref):
    y = 2 * where_ref[4:5, :128] + where_ref[0:1, :128]
    group = lanes((24, 128)) // 32
    blank = jnp.zeros((24, 96), F32)
    block = jnp.zeros((24, 128), F32)
    for bits, ref in enumerate((r0_ref, r1_ref, r2_ref, r3_ref)):
        wide = jnp.concatenate([ref[...].astype(F32), blank], axis=1)
        for k in range(4):
            moved = wide if k == 0 else pltpu.roll(wide, 32 * k, 1)
            block = jnp.where((group == k) & ((y ^ bits) == group), moved, block)
    block = block.astype(BF16)
    for peer in range(32):
        send_ref[peer] = block


def nt_dot(a, b):
    return lax.dot_general(a, b, (((1,), (1,)), ((), ())), preferred_element_type=F32)


def nn_dot(a, b):
    return lax.dot_general(a, b, (((1,), (0,)), ((), ())), preferred_element_type=F32)


def silu(v):
    return v * jax.nn.sigmoid(v)


def section_body(quarters, weight_refs, write_ref, read_ref, gain_ref, taps_refs, own_ref, far_ref, pad_ref):
    low = lanes((T, 128)) < 64
    total = None
    for pair in quarters:
        for q in pair:
            sq = q * q
            sq = sq[:, :128] + sq[:, 128:]
            total = sq if total is None else total + sq
    scale = lax.rsqrt(jnp.sum(total, axis=1, keepdims=True) * (1.0 / D) + EPS)
    blocks = []
    for h in range(2):
        for c in range(2):
            n = (2 * h + c) * 256
            blocks.append((quarters[h][c] * scale * gain_ref[:, n : n + 256]).astype(BF16))
    normed = jnp.concatenate(blocks, axis=1)

    step_rows = jnp.concatenate([w[160:168].astype(F32)[0:2] for w in weight_refs], axis=0)
    step_raw = nt_dot(step_rows.astype(BF16), normed)
    small = []
    for w in weight_refs:
        misc = w[160:168].astype(F32)
        small.append((misc[2:3] + misc[3:4] + misc[4:5], misc[5:6] + misc[6:7] + misc[7:8]))
    bias = jnp.concatenate([s[0][:, 640 + 128 * d : 640 + 128 * d + T] for s in small for d in range(2)], axis=0)
    decay = jnp.concatenate([s[1][:, 128 * d : 128 * d + T] for s in small for d in range(2)], axis=0)
    raw = step_raw + bias
    dt = jnp.maximum(raw, 0.0) + jnp.log1p(jnp.exp(-jnp.abs(raw)))
    log_decay = dt * (-jnp.exp(decay))
    parts = [s.astype(BF16) for s in split3(log_decay)]
    row_id = lax.broadcasted_iota(jnp.int32, (T, T), 0)
    col_id = lax.broadcasted_iota(jnp.int32, (T, T), 1)
    upto = (row_id <= col_id).astype(F32).astype(BF16)
    since = (row_id >= col_id).astype(F32).astype(BF16)
    fwd_all = (nn_dot(parts[0], upto) + nn_dot(parts[1], upto)) + nn_dot(parts[2], upto)
    bwd_all = (nn_dot(parts[0], since) + nn_dot(parts[1], since)) + nn_dot(parts[2], since)
    odd = lax.broadcasted_iota(jnp.int32, (8, T), 0) % 2 == 1
    cum = jnp.where(odd, bwd_all, fwd_all)
    cum_pad = jnp.concatenate([cum, jnp.zeros((8, 128 - T), F32)], axis=1)
    cum_cols = cum_pad.T[:T]

    gv01 = nt_dot(normed, jnp.concatenate([weight_refs[0][0:128], weight_refs[1][0:128]], axis=0))
    gv23 = nt_dot(normed, jnp.concatenate([weight_refs[2][0:128], weight_refs[3][0:128]], axis=0))
    wr_rows = [
        jnp.concatenate([r[n * 128 + y * 32 : n * 128 + y * 32 + 32] for r in (write_ref, read_ref)], axis=1)
        for h in range(2)
        for c in range(2)
        for n in (c, 2 + c, 4 + c, 6 + c)
        for y in (h, 2 + h)
    ]
    wr = nn_dot(normed, jnp.concatenate(wr_rows, axis=0))
    pad_ref[0:8] = jnp.zeros((8, 768), F32)
    pad_ref[8 + T : 16 + T] = jnp.zeros((8, 768), F32)
    pad_ref[8 : 8 + T, 0:256] = gv01.astype(BF16).astype(F32)
    pad_ref[8 : 8 + T, 256:512] = gv23.astype(BF16).astype(F32)
    pad_ref[8 : 8 + T, 512:768] = wr.astype(BF16).astype(F32)
    acts = []
    for g in range(6):
        span = slice(g * 128, (g + 1) * 128)
        acc = None
        for k in range(5):
            tap = small[g][0][:, k * 128 : (k + 1) * 128] if g < 4 else taps_refs[g - 4][k]
            term = pad_ref[6 + k : 6 + k + T, span] * tap
            acc = term if acc is None else acc + term
        acts.append(silu(acc).astype(BF16))
    scores = nt_dot(acts[5], acts[4])
    lower = row_id >= col_id
    diagonal = row_id == col_id
    gated = []
    for j in range(4):
        fc = cum_cols[:, 2 * j : 2 * j + 1]
        bc = cum_cols[:, 2 * j + 1 : 2 * j + 2]
        fr = cum[2 * j : 2 * j + 1]
        br = cum[2 * j + 1 : 2 * j + 2]
        d0 = dt[2 * j : 2 * j + 1]
        d1 = dt[2 * j + 1 : 2 * j + 2]
        mix = jnp.exp(jnp.where(lower, fc - fr, bc - br)) * jnp.where(lower, d0, d1)
        mix = mix + jnp.where(diagonal, d1, 0.0)
        combined = scores * mix
        high = combined.astype(BF16)
        rest = (combined - high.astype(F32)).astype(BF16)
        y = nn_dot(high, acts[j]) + nn_dot(rest, acts[j])
        y = y + small[j][1][:, 256:384] * acts[j].astype(F32)
        gate = pltpu.roll(pad_ref[8 : 8 + T, j * 128 : (j + 1) * 128], 64, 1)
        gated.append(y * silu(gate))
    pairs = [jnp.where(low, pltpu.roll(gated[2 * i], 64, 1), gated[2 * i + 1]).astype(BF16) for i in range(2)]
    gated_all = jnp.concatenate(pairs, axis=1)
    for side, ref in ((0, own_ref), (1, far_ref)):
        weight = jnp.concatenate(
            [
                w[128:160, 512 * r + 256 * side : 512 * r + 256 * side + 256]
                for w in weight_refs
                for r in range(2)
            ],
            axis=0,
        )
        ref[...] = nn_dot(gated_all, weight).astype(ref.dtype)


def entry_section_kernel(where_ref, recv_ref, *refs):
    *rest, quarter_out, own_ref, far_ref, pad_ref, quarter_ref = refs
    tokens = [
        jnp.concatenate([recv_ref[x * 8 + n].astype(F32) for x in range(4)], axis=0) for n in range(8)
    ]
    blocks = permuted(jnp.concatenate(tokens, axis=1))
    for q in range(4):
        quarter_ref[q] = jnp.concatenate(blocks[2 * q : 2 * q + 2], axis=1)
    quarters = [[quarter_ref[2 * h + c] for c in range(2)] for h in range(2)]
    half, core = flag(where_ref, 0), flag(where_ref, 1)
    mine = jnp.where(half, jnp.where(core, *quarters[0]), jnp.where(core, *quarters[1]))
    quarter_out[...] = mine.astype(BF16)
    section_body(quarters, rest[0:4], *rest[4:7], rest[7:9], own_ref, far_ref, pad_ref)


def relay_section_kernel(where_ref, a_ref, b_ref, c_ref, d_ref, *refs):
    *rest, own_ref, far_ref, pad_ref = refs
    half, core = flag(where_ref, 0), flag(where_ref, 1)
    a, b, c, d = [r[...].astype(F32) for r in (a_ref, b_ref, c_ref, d_ref)]
    own0, own1 = jnp.where(half, a, c), jnp.where(half, c, a)
    far0, far1 = jnp.where(half, b, d), jnp.where(half, d, b)
    quarters = [
        [jnp.where(core, own0, far0), jnp.where(core, far0, own0)],
        [jnp.where(core, own1, far1), jnp.where(core, far1, own1)],
    ]
    section_body(quarters, rest[0:4], *rest[4:7], rest[7:9], own_ref, far_ref, pad_ref)


def exit_pack_kernel(where_ref, mine_ref, m0_ref, m1_ref, m2_ref, m3_ref, send_ref):
    branch = (m0_ref[...].astype(F32) + m1_ref[...].astype(F32)) + (m2_ref[...].astype(F32) + m3_ref[...].astype(F32))
    branch = branch.astype(BF16).astype(F32)
    final = (mine_ref[...].astype(F32) + 0.5 * branch).astype(BF16).astype(F32)
    squares = final * final
    squares = jnp.sum(squares[:, :128] + squares[:, 128:], axis=1, keepdims=True)
    squares = jnp.broadcast_to(squares, (T, 128))
    own = jnp.where(flag(where_ref, 2, 128), final[:, :128], final[:, 128:])
    own = jnp.where(flag(where_ref, 3, 128), own, pltpu.roll(own, 64, 1))
    turned = {d: own if d == 0 else pltpu.roll(own, (32 * d) % 128, 1) for d in (-1, 0, 1, 2, 3)}
    lane = lanes((6, 128))
    group = lane // 32
    spot = lane % 32 == lax.broadcasted_iota(jnp.int32, (6, 128), 0)
    for x in range(4):
        rows = [slice(x * 24 + k * 6, x * 24 + k * 6 + 6) for k in range(4)]
        total = squares[rows[0]]
        for k in range(1, 4):
            total = jnp.where(group == k, squares[rows[k]], total)
        total = jnp.sum(jnp.where(spot, total, 0.0), axis=0, keepdims=True)
        parts = split3(total)
        for m in range(2):
            block = turned[-m][rows[0]]
            for k in range(1, 4):
                block = jnp.where(group == k, turned[k - m][rows[k]], block)
            message = jnp.concatenate([block, parts[0], parts[1]], axis=0).astype(BF16)
            for peer in range(4):
                send_ref[(x * 2 + m) * 4 + peer] = message


def exit_unpack_kernel(where_ref, recv_ref, out_ref):
    half, core = flag(where_ref, 0, 128), flag(where_ref, 1, 128)
    lane = lanes((8, 128))
    spot = lane % 32 == lax.broadcasted_iota(jnp.int32, (8, 128), 0)
    same_group = (
        lax.broadcasted_iota(jnp.int32, (128, 128), 0) // 32 == lanes((128, 128)) // 32
    ).astype(F32).astype(BF16)
    parts = []
    for m in range(2):
        first = (6 + m) * 4
        sums = [recv_ref[first + i].astype(F32) for i in range(4)]
        total = (sums[0][6:7] + sums[0][7:8]) + (sums[1][6:7] + sums[1][7:8])
        total = total + ((sums[2][6:7] + sums[2][7:8]) + (sums[3][6:7] + sums[3][7:8]))
        parts += split3(jnp.where(spot, jnp.broadcast_to(total, (8, 128)), 0.0))
    spread = nn_dot(jnp.concatenate(parts, axis=0).astype(BF16), same_group)
    for m in range(2):
        total = (spread[24 * m : 24 * m + 8] + spread[24 * m + 8 : 24 * m + 16]) + spread[24 * m + 16 : 24 * m + 24]
        blocks = [recv_ref[(6 + m) * 4 + i].astype(F32) for i in range(4)]
        block = jnp.where(half, jnp.where(core, *blocks[:2]), jnp.where(core, *blocks[2:]))
        block = block * lax.rsqrt(total * (1.0 / D) + EPS)
        rows = [block if k == 0 else pltpu.roll(block, 128 - 32 * k, 1) for k in range(4)]
        out_ref[m] = jnp.concatenate([r[:6, :32] for r in rows], axis=0).astype(BF16)


VMEM_SPEC = pl.BlockSpec(memory_space=pltpu.VMEM)


def call_kernel(kernel, out_shape, count, scratch=()):
    return pl.pallas_call(
        kernel,
        out_shape=out_shape,
        in_specs=[VMEM_SPEC] + [VMEM_SPEC] * count,
        out_specs=[VMEM_SPEC] * len(out_shape),
        scratch_shapes=scratch,
        compiler_params=pltpu.CompilerParams(vmem_limit_bytes=24 * 1024 * 1024),
    )


def flip(v, axes, bits):
    size = lax.axis_size(axes)
    return lax.ppermute(v, axes, [(i, i ^ bits) for i in range(size)])


def hop_pairs(first, size, flip_half):
    pairs = []
    for i in range(size):
        j = i + 1 if (i - first) % 2 == 0 else i - 1
        for h in range(2):
            for c in range(2):
                if 0 <= j < size:
                    target = (j, 1 - h if flip_half else h, c)
                else:
                    target = (i, h, 1 - c)
                pairs.append((4 * i + 2 * h + c, 4 * target[0] + 2 * target[1] + target[2]))
    return pairs


def per_device(
    micro_in,
    norm_gain,
    proj_gate,
    proj_value,
    proj_write,
    proj_read,
    proj_step,
    step_bias,
    decay_log,
    skip_gain,
    conv_value,
    conv_write,
    conv_read,
    proj_out,
):
    sections = lax.axis_size("pp")
    half = lax.axis_index("yh")
    micro = lax.axis_index("ym")
    core = lax.axis_index("tc")
    zpos = lax.axis_index("tz")
    where = jnp.stack([half, core, zpos // 2, zpos % 2, micro]).astype(jnp.int32)
    where = jnp.broadcast_to(where[:, None], (5, 256))

    shape = jax.ShapeDtypeStruct
    raw = (
        micro_in,
        proj_gate[0, :, 0, 0, :].T,
        proj_value[0, :, 0, 0, :].T,
        proj_step[0, :, :, 0, 0].T,
        proj_out[0, 0, 0],
        conv_value.reshape(5, 1, 64),
        step_bias.reshape(1, 2),
        decay_log.reshape(1, 2),
        skip_gain.reshape(1, 1),
        norm_gain,
        conv_write.reshape(5, 1, 128),
        conv_read.reshape(5, 1, 128),
    )
    order = (1, 2, 4, 3, 5, 6, 7, 8, 9, 0)
    near, away, same, other, gain, taps_w, taps_r = pl.pallas_call(
        pack_kernel,
        out_shape=[
            shape((T // 4, 32), BF16),
            shape((T // 4, 32), BF16),
            shape((ROWS, D), BF16),
            shape((ROWS, D), BF16),
            shape((1, D), F32),
            shape((5, 1, 128), F32),
            shape((5, 1, 128), F32),
        ],
        in_specs=[VMEM_SPEC] + [pl.BlockSpec(memory_space=pltpu.HBM)] * len(raw),
        out_specs=[VMEM_SPEC] * 7,
        scratch_shapes=[pltpu.VMEM(raw[i].shape, raw[i].dtype) for i in order]
        + [pltpu.SemaphoreType.DMA((len(raw),))],
        compiler_params=pltpu.CompilerParams(vmem_limit_bytes=24 * 1024 * 1024),
    )(where, *[pltpu.with_memory_space_constraint(v, pltpu.HBM) if i != 8 else v for i, v in enumerate(raw)])
    r1 = flip(near, FS, 1)
    r2 = flip(away, FS, 2)
    r3 = flip(away, FS, 3)
    w1 = flip(other, FS, 1)
    w2 = flip(same, FS, 2)
    w3 = flip(other, FS, 3)
    (send,) = call_kernel(block_kernel, [shape((32, T // 4, 128), BF16)], 4)(where, near, r1, r2, r3)
    recv = lax.all_to_all(send, BLOCKS, 0, 0)

    params = (same, w1, w2, w3, proj_write[0, :, 0, :], proj_read[0, :, 0, :], gain, taps_w, taps_r)
    quarter = shape((T, 256), BF16)
    outs = [shape((T, 256), F32), quarter]
    pad = pltpu.VMEM((T + 16, 768), F32)
    mine, own, far = call_kernel(
        entry_section_kernel, [quarter, *outs], 10, [pad, pltpu.VMEM((4, T, 256), F32)]
    )(where, recv, *params)
    for s in range(sections):
        got = flip(far, "tc", 1)
        mixed = (own + got.astype(F32)).astype(BF16)
        others = [flip(mixed, "tz", d) for d in (1, 2, 3)]
        if s + 1 == sections:
            break
        r1, r2, r3 = [v.astype(F32) for v in others]
        branch = ((mixed.astype(F32) + r1) + (r2 + r3)).astype(BF16).astype(F32)
        produced = (mine.astype(F32) + 0.5 * branch).astype(BF16)
        a, c = [lax.ppermute(produced, ("pp", "yh", "tc"), hop_pairs(s, sections, f)) for f in (False, True)]
        b = flip(a, "tc", 1)
        d = flip(c, "tc", 1)
        mine = a
        own, far = call_kernel(relay_section_kernel, outs, 13, [pad])(where, a, b, c, d, *params)

    (send,) = call_kernel(exit_pack_kernel, [shape((32, 8, 128), BF16)], 5)(where, mine, mixed, *others)
    recv = lax.all_to_all(send, ("pp", "ym", "yh", "tc"), 0, 0)
    (result,) = call_kernel(exit_unpack_kernel, [shape((2, T // sections, 32), BF16)], 1)(where, recv)
    return result


def solution(mesh):
    split = Mesh(
        mesh.devices.reshape(mesh.shape["pp"], 2, 2, 4, 2), ("pp", "ym", "yh", "tz", "tc")
    )
    in_specs = (
        P(None, "pp", TP + FS),
        P("pp", None),
        P("pp", None, TP, FS, None),
        P("pp", None, TP, FS, None),
        P("pp", None, TP, None),
        P("pp", None, TP, None),
        P("pp", None, None, TP, FS),
        P("pp", None, TP, FS),
        P("pp", None, TP, FS),
        P("pp", TP, FS),
        P("pp", None, TP, FS, None),
        P("pp", None, TP, None),
        P("pp", None, TP, None),
        P("pp", TP, FS, None, None),
    )
    out_specs = P(None, "pp", TP + FS)
    return jax.shard_map(
        per_device, mesh=split, in_specs=in_specs, out_specs=out_specs, check_vma=False
    )
```

```python
import jax
import jax.numpy as jnp
from jax import lax
from jax.experimental import pallas as pl
from jax.experimental.pallas import tpu as pltpu
from jax.sharding import Mesh
from jax.sharding import PartitionSpec as P


FS = ("ym", "yh")
TP = ("tz", "tc")
BLOCKS = ("pp", "tz", "tc")
EPS = 1e-06
T = 96
D = 1024
F32 = jnp.float32
BF16 = jnp.bfloat16
ROWS = 168


def lanes(shape):
    return lax.broadcasted_iota(jnp.int32, shape, len(shape) - 1)


def split3(v):
    hi = v.astype(BF16).astype(F32)
    mid = (v - hi).astype(BF16).astype(F32)
    low = v - hi - mid
    return hi, mid, low


def flag(where_ref, row, width=256):
    return where_ref[row : row + 1, :width] == 0


def permuted(v):
    group = lanes((v.shape[0], 128)) // 32
    out = []
    for h in range(2):
        for c in range(2):
            for p in range(2):
                block = None
                for g in range(4):
                    zz, m = g // 2, g % 2
                    n = (2 * p + zz) * 2 + c
                    moved = v[:, n * 128 : (n + 1) * 128]
                    turn = (64 * zz - 32 * m - 32 * h) % 128
                    if turn:
                        moved = pltpu.roll(moved, turn, 1)
                    block = moved if block is None else jnp.where(group == g, moved, block)
                out.append(block)
    return out


def pack_kernel(
    where_ref,
    micro_hbm,
    gate_hbm,
    value_hbm,
    step_hbm,
    out_hbm,
    taps_hbm,
    bias_hbm,
    decay_hbm,
    skip_hbm,
    gain_hbm,
    taps_w_hbm,
    taps_r_hbm,
    near_ref,
    away_ref,
    same_ref,
    other_ref,
    gain_out,
    taps_w_out,
    taps_r_out,
    *scratch,
):
    sources = (
        gate_hbm,
        value_hbm,
        out_hbm,
        step_hbm,
        taps_hbm,
        bias_hbm,
        decay_hbm,
        skip_hbm,
        gain_hbm,
        micro_hbm,
        taps_w_hbm,
        taps_r_hbm,
    )
    buffers, sems = (*scratch[:-1], taps_w_out, taps_r_out), scratch[-1]
    copies = [pltpu.make_async_copy(s, b, sems.at[i]) for i, (s, b) in enumerate(zip(sources, buffers))]
    for copy in copies:
        copy.start()
    for copy in copies:
        copy.wait()
    gate_ref, value_ref, out_ref, step_ref, taps_ref, bias_ref, decay_ref, skip_ref, gain_ref, micro_ref = buffers[:10]
    core = flag(where_ref, 1, 128)
    half = flag(where_ref, 0, 128)
    gate = jnp.concatenate(permuted(gate_ref[...].astype(F32)), axis=1).astype(BF16)
    value = jnp.concatenate(permuted(value_ref[...].astype(F32)), axis=1).astype(BF16)
    step = jnp.concatenate(permuted(step_ref[...].astype(F32)), axis=1)
    gain_out[...] = jnp.concatenate(permuted(gain_ref[...]), axis=1)
    blank = jnp.zeros((1, 64), F32)
    wide = lambda ref, k: jnp.broadcast_to(ref[:, k : k + 1], (1, 128))
    row_a = [piece for k in range(5) for piece in (blank, taps_ref[k])]
    row_a = jnp.concatenate(row_a + [wide(bias_ref, 0), wide(bias_ref, 1), blank, blank], axis=1)
    row_b = [wide(decay_ref, 0), wide(decay_ref, 1), wide(skip_ref, 0)] + [blank] * 10
    row_b = jnp.concatenate(row_b, axis=1)
    misc = jnp.concatenate([step, *split3(row_a), *split3(row_b)], axis=0).astype(BF16)
    out = permuted(out_ref[...].astype(F32))
    halves = []
    for h in range(2):
        first, second = out[4 * h : 4 * h + 2], out[4 * h + 2 : 4 * h + 4]
        own = [jnp.where(core, a, b) for a, b in zip(first, second)]
        far = [jnp.where(core, b, a) for a, b in zip(first, second)]
        halves.append(own + far)
    for ref, pair in ((same_ref, zip(*halves)), (other_ref, zip(*halves[::-1]))):
        part = jnp.concatenate([jnp.where(half, a, b) for a, b in pair], axis=1)
        ref[0:64] = gate
        ref[64:128] = value
        ref[128:160] = jnp.concatenate([part[0:32], part[32:64]], axis=1).astype(BF16)
        ref[160:168] = misc
    first = flag(where_ref, 4, 32)
    micro = [micro_ref[m].astype(F32) for m in range(2)]
    near_ref[...] = jnp.where(first, micro[0], micro[1]).astype(BF16)
    away_ref[...] = jnp.where(first, micro[1], micro[0]).astype(BF16)


def block_kernel(where_ref, r0_ref, r1_ref, r2_ref, r3_ref, send_ref):
    y = 2 * where_ref[4:5, :128] + where_ref[0:1, :128]
    group = lanes((24, 128)) // 32
    blank = jnp.zeros((24, 96), F32)
    block = jnp.zeros((24, 128), F32)
    for bits, ref in enumerate((r0_ref, r1_ref, r2_ref, r3_ref)):
        wide = jnp.concatenate([ref[...].astype(F32), blank], axis=1)
        for k in range(4):
            moved = wide if k == 0 else pltpu.roll(wide, 32 * k, 1)
            block = jnp.where((group == k) & ((y ^ bits) == group), moved, block)
    block = block.astype(BF16)
    for peer in range(32):
        send_ref[peer] = block


def nt_dot(a, b):
    return lax.dot_general(a, b, (((1,), (1,)), ((), ())), preferred_element_type=F32)


def nn_dot(a, b):
    return lax.dot_general(a, b, (((1,), (0,)), ((), ())), preferred_element_type=F32)


def silu(v):
    return v * jax.nn.sigmoid(v)


def section_body(quarters, weight_refs, write_ref, read_ref, gain_ref, taps_refs, own_ref, far_ref, pad_ref):
    low = lanes((T, 128)) < 64
    total = None
    for pair in quarters:
        for q in pair:
            sq = q * q
            sq = sq[:, :128] + sq[:, 128:]
            total = sq if total is None else total + sq
    scale = lax.rsqrt(jnp.sum(total, axis=1, keepdims=True) * (1.0 / D) + EPS)
    blocks = []
    for h in range(2):
        for c in range(2):
            n = (2 * h + c) * 256
            blocks.append((quarters[h][c] * scale * gain_ref[:, n : n + 256]).astype(BF16))
    normed = jnp.concatenate(blocks, axis=1)

    step_rows = jnp.concatenate([w[160:168].astype(F32)[0:2] for w in weight_refs], axis=0)
    step_raw = nt_dot(step_rows.astype(BF16), normed)
    small = []
    for w in weight_refs:
        misc = w[160:168].astype(F32)
        small.append((misc[2:3] + misc[3:4] + misc[4:5], misc[5:6] + misc[6:7] + misc[7:8]))
    bias = jnp.concatenate([s[0][:, 640 + 128 * d : 640 + 128 * d + T] for s in small for d in range(2)], axis=0)
    decay = jnp.concatenate([s[1][:, 128 * d : 128 * d + T] for s in small for d in range(2)], axis=0)
    raw = step_raw + bias
    dt = jnp.maximum(raw, 0.0) + jnp.log1p(jnp.exp(-jnp.abs(raw)))
    log_decay = dt * (-jnp.exp(decay))
    parts = [s.astype(BF16) for s in split3(log_decay)]
    row_id = lax.broadcasted_iota(jnp.int32, (T, T), 0)
    col_id = lax.broadcasted_iota(jnp.int32, (T, T), 1)
    upto = (row_id <= col_id).astype(F32).astype(BF16)
    since = (row_id >= col_id).astype(F32).astype(BF16)
    fwd_all = (nn_dot(parts[0], upto) + nn_dot(parts[1], upto)) + nn_dot(parts[2], upto)
    bwd_all = (nn_dot(parts[0], since) + nn_dot(parts[1], since)) + nn_dot(parts[2], since)
    odd = lax.broadcasted_iota(jnp.int32, (8, T), 0) % 2 == 1
    cum = jnp.where(odd, bwd_all, fwd_all)
    cum_pad = jnp.concatenate([cum, jnp.zeros((8, 128 - T), F32)], axis=1)
    cum_cols = cum_pad.T[:T]

    gv01 = nt_dot(normed, jnp.concatenate([weight_refs[0][0:128], weight_refs[1][0:128]], axis=0))
    gv23 = nt_dot(normed, jnp.concatenate([weight_refs[2][0:128], weight_refs[3][0:128]], axis=0))
    wr_rows = [
        jnp.concatenate([r[n * 128 + y * 32 : n * 128 + y * 32 + 32] for r in (write_ref, read_ref)], axis=1)
        for h in range(2)
        for c in range(2)
        for n in (c, 2 + c, 4 + c, 6 + c)
        for y in (h, 2 + h)
    ]
    wr = nn_dot(normed, jnp.concatenate(wr_rows, axis=0))
    pad_ref[0:8] = jnp.zeros((8, 768), F32)
    pad_ref[8 + T : 16 + T] = jnp.zeros((8, 768), F32)
    pad_ref[8 : 8 + T, 0:256] = gv01.astype(BF16).astype(F32)
    pad_ref[8 : 8 + T, 256:512] = gv23.astype(BF16).astype(F32)
    pad_ref[8 : 8 + T, 512:768] = wr.astype(BF16).astype(F32)
    acts = []
    for g in range(6):
        span = slice(g * 128, (g + 1) * 128)
        acc = None
        for k in range(5):
            tap = small[g][0][:, k * 128 : (k + 1) * 128] if g < 4 else taps_refs[g - 4][k]
            term = pad_ref[6 + k : 6 + k + T, span] * tap
            acc = term if acc is None else acc + term
        acts.append(silu(acc).astype(BF16))
    scores = nt_dot(acts[5], acts[4])
    lower = row_id >= col_id
    diagonal = row_id == col_id
    gated = []
    for j in range(4):
        fc = cum_cols[:, 2 * j : 2 * j + 1]
        bc = cum_cols[:, 2 * j + 1 : 2 * j + 2]
        fr = cum[2 * j : 2 * j + 1]
        br = cum[2 * j + 1 : 2 * j + 2]
        d0 = dt[2 * j : 2 * j + 1]
        d1 = dt[2 * j + 1 : 2 * j + 2]
        mix = jnp.exp(jnp.where(lower, fc - fr, bc - br)) * jnp.where(lower, d0, d1)
        mix = mix + jnp.where(diagonal, d1, 0.0)
        combined = scores * mix
        high = combined.astype(BF16)
        rest = (combined - high.astype(F32)).astype(BF16)
        y = nn_dot(high, acts[j]) + nn_dot(rest, acts[j])
        y = y + small[j][1][:, 256:384] * acts[j].astype(F32)
        gate = pltpu.roll(pad_ref[8 : 8 + T, j * 128 : (j + 1) * 128], 64, 1)
        gated.append(y * silu(gate))
    pairs = [jnp.where(low, pltpu.roll(gated[2 * i], 64, 1), gated[2 * i + 1]).astype(BF16) for i in range(2)]
    gated_all = jnp.concatenate(pairs, axis=1)
    for side, ref in ((0, own_ref), (1, far_ref)):
        weight = jnp.concatenate(
            [
                w[128:160, 512 * r + 256 * side : 512 * r + 256 * side + 256]
                for w in weight_refs
                for r in range(2)
            ],
            axis=0,
        )
        ref[...] = nn_dot(gated_all, weight).astype(ref.dtype)


def entry_section_kernel(where_ref, recv_ref, *refs):
    *rest, quarter_out, own_ref, far_ref, pad_ref, quarter_ref = refs
    tokens = [
        jnp.concatenate([recv_ref[x * 8 + n].astype(F32) for x in range(4)], axis=0) for n in range(8)
    ]
    blocks = permuted(jnp.concatenate(tokens, axis=1))
    for q in range(4):
        quarter_ref[q] = jnp.concatenate(blocks[2 * q : 2 * q + 2], axis=1)
    quarters = [[quarter_ref[2 * h + c] for c in range(2)] for h in range(2)]
    half, core = flag(where_ref, 0), flag(where_ref, 1)
    mine = jnp.where(half, jnp.where(core, *quarters[0]), jnp.where(core, *quarters[1]))
    quarter_out[...] = mine.astype(BF16)
    section_body(quarters, rest[0:4], *rest[4:7], rest[7:9], own_ref, far_ref, pad_ref)


def relay_section_kernel(where_ref, a_ref, b_ref, c_ref, d_ref, *refs):
    *rest, own_ref, far_ref, pad_ref = refs
    half, core = flag(where_ref, 0), flag(where_ref, 1)
    a, b, c, d = [r[...].astype(F32) for r in (a_ref, b_ref, c_ref, d_ref)]
    own0, own1 = jnp.where(half, a, c), jnp.where(half, c, a)
    far0, far1 = jnp.where(half, b, d), jnp.where(half, d, b)
    quarters = [
        [jnp.where(core, own0, far0), jnp.where(core, far0, own0)],
        [jnp.where(core, own1, far1), jnp.where(core, far1, own1)],
    ]
    section_body(quarters, rest[0:4], *rest[4:7], rest[7:9], own_ref, far_ref, pad_ref)


def exit_pack_kernel(where_ref, mine_ref, m0_ref, m1_ref, m2_ref, m3_ref, send_ref):
    branch = (m0_ref[...].astype(F32) + m1_ref[...].astype(F32)) + (m2_ref[...].astype(F32) + m3_ref[...].astype(F32))
    branch = branch.astype(BF16).astype(F32)
    final = (mine_ref[...].astype(F32) + 0.5 * branch).astype(BF16).astype(F32)
    squares = final * final
    squares = jnp.sum(squares[:, :128] + squares[:, 128:], axis=1, keepdims=True)
    squares = jnp.broadcast_to(squares, (T, 128))
    own = jnp.where(flag(where_ref, 2, 128), final[:, :128], final[:, 128:])
    own = jnp.where(flag(where_ref, 3, 128), own, pltpu.roll(own, 64, 1))
    turned = {d: own if d == 0 else pltpu.roll(own, (32 * d) % 128, 1) for d in (-1, 0, 1, 2, 3)}
    lane = lanes((6, 128))
    group = lane // 32
    spot = lane % 32 == lax.broadcasted_iota(jnp.int32, (6, 128), 0)
    for x in range(4):
        rows = [slice(x * 24 + k * 6, x * 24 + k * 6 + 6) for k in range(4)]
        total = squares[rows[0]]
        for k in range(1, 4):
            total = jnp.where(group == k, squares[rows[k]], total)
        total = jnp.sum(jnp.where(spot, total, 0.0), axis=0, keepdims=True)
        parts = split3(total)
        for m in range(2):
            block = turned[-m][rows[0]]
            for k in range(1, 4):
                block = jnp.where(group == k, turned[k - m][rows[k]], block)
            message = jnp.concatenate([block, parts[0], parts[1]], axis=0).astype(BF16)
            for peer in range(4):
                send_ref[(x * 2 + m) * 4 + peer] = message


def exit_unpack_kernel(where_ref, recv_ref, out_ref):
    half, core = flag(where_ref, 0, 128), flag(where_ref, 1, 128)
    lane = lanes((8, 128))
    spot = lane % 32 == lax.broadcasted_iota(jnp.int32, (8, 128), 0)
    same_group = (
        lax.broadcasted_iota(jnp.int32, (128, 128), 0) // 32 == lanes((128, 128)) // 32
    ).astype(F32).astype(BF16)
    parts = []
    for m in range(2):
        first = (6 + m) * 4
        sums = [recv_ref[first + i].astype(F32) for i in range(4)]
        total = (sums[0][6:7] + sums[0][7:8]) + (sums[1][6:7] + sums[1][7:8])
        total = total + ((sums[2][6:7] + sums[2][7:8]) + (sums[3][6:7] + sums[3][7:8]))
        parts += split3(jnp.where(spot, jnp.broadcast_to(total, (8, 128)), 0.0))
    spread = nn_dot(jnp.concatenate(parts, axis=0).astype(BF16), same_group)
    for m in range(2):
        total = (spread[24 * m : 24 * m + 8] + spread[24 * m + 8 : 24 * m + 16]) + spread[24 * m + 16 : 24 * m + 24]
        blocks = [recv_ref[(6 + m) * 4 + i].astype(F32) for i in range(4)]
        block = jnp.where(half, jnp.where(core, *blocks[:2]), jnp.where(core, *blocks[2:]))
        block = block * lax.rsqrt(total * (1.0 / D) + EPS)
        rows = [block if k == 0 else pltpu.roll(block, 128 - 32 * k, 1) for k in range(4)]
        out_ref[m] = jnp.concatenate([r[:6, :32] for r in rows], axis=0).astype(BF16)


VMEM_SPEC = pl.BlockSpec(memory_space=pltpu.VMEM)


def call_kernel(kernel, out_shape, count, scratch=()):
    return pl.pallas_call(
        kernel,
        out_shape=out_shape,
        in_specs=[VMEM_SPEC] + [VMEM_SPEC] * count,
        out_specs=[VMEM_SPEC] * len(out_shape),
        scratch_shapes=scratch,
        compiler_params=pltpu.CompilerParams(vmem_limit_bytes=24 * 1024 * 1024),
    )


def flip(v, axes, bits):
    size = lax.axis_size(axes)
    return lax.ppermute(v, axes, [(i, i ^ bits) for i in range(size)])


def hop_pairs(first, size, flip_half):
    pairs = []
    for i in range(size):
        j = i + 1 if (i - first) % 2 == 0 else i - 1
        for h in range(2):
            for c in range(2):
                if 0 <= j < size:
                    target = (j, 1 - h if flip_half else h, c)
                else:
                    target = (i, h, 1 - c)
                pairs.append((4 * i + 2 * h + c, 4 * target[0] + 2 * target[1] + target[2]))
    return pairs


def per_device(
    micro_in,
    norm_gain,
    proj_gate,
    proj_value,
    proj_write,
    proj_read,
    proj_step,
    step_bias,
    decay_log,
    skip_gain,
    conv_value,
    conv_write,
    conv_read,
    proj_out,
):
    sections = lax.axis_size("pp")
    half = lax.axis_index("yh")
    micro = lax.axis_index("ym")
    core = lax.axis_index("tc")
    zpos = lax.axis_index("tz")
    where = jnp.stack([half, core, zpos // 2, zpos % 2, micro]).astype(jnp.int32)
    where = jnp.broadcast_to(where[:, None], (5, 256))

    shape = jax.ShapeDtypeStruct
    raw = (
        micro_in,
        proj_gate[0, :, 0, 0, :].T,
        proj_value[0, :, 0, 0, :].T,
        proj_step[0, :, :, 0, 0].T,
        proj_out[0, 0, 0],
        conv_value.reshape(5, 1, 64),
        step_bias.reshape(1, 2),
        decay_log.reshape(1, 2),
        skip_gain.reshape(1, 1),
        norm_gain,
        conv_write.reshape(5, 1, 128),
        conv_read.reshape(5, 1, 128),
    )
    order = (1, 2, 4, 3, 5, 6, 7, 8, 9, 0)
    near, away, same, other, gain, taps_w, taps_r = pl.pallas_call(
        pack_kernel,
        out_shape=[
            shape((T // 4, 32), BF16),
            shape((T // 4, 32), BF16),
            shape((ROWS, D), BF16),
            shape((ROWS, D), BF16),
            shape((1, D), F32),
            shape((5, 1, 128), F32),
            shape((5, 1, 128), F32),
        ],
        in_specs=[VMEM_SPEC] + [pl.BlockSpec(memory_space=pltpu.HBM)] * len(raw),
        out_specs=[VMEM_SPEC] * 7,
        scratch_shapes=[pltpu.VMEM(raw[i].shape, raw[i].dtype) for i in order]
        + [pltpu.SemaphoreType.DMA((len(raw),))],
        compiler_params=pltpu.CompilerParams(vmem_limit_bytes=24 * 1024 * 1024),
    )(where, *[pltpu.with_memory_space_constraint(v, pltpu.HBM) if i != 8 else v for i, v in enumerate(raw)])
    r1 = flip(near, FS, 1)
    r2 = flip(away, FS, 2)
    r3 = flip(away, FS, 3)
    w1 = flip(other, FS, 1)
    w2 = flip(same, FS, 2)
    w3 = flip(other, FS, 3)
    (send,) = call_kernel(block_kernel, [shape((32, T // 4, 128), BF16)], 4)(where, near, r1, r2, r3)
    recv = lax.all_to_all(send, BLOCKS, 0, 0)

    params = (same, w1, w2, w3, proj_write[0, :, 0, :], proj_read[0, :, 0, :], gain, taps_w, taps_r)
    quarter = shape((T, 256), BF16)
    outs = [shape((T, 256), F32), quarter]
    pad = pltpu.VMEM((T + 16, 768), F32)
    mine, own, far = call_kernel(
        entry_section_kernel, [quarter, *outs], 10, [pad, pltpu.VMEM((4, T, 256), F32)]
    )(where, recv, *params)
    for s in range(sections):
        got = flip(far, "tc", 1)
        mixed = (own + got.astype(F32)).astype(BF16)
        others = []
        for d in (1, 2, 3):
            others.append(flip(mixed, "tz", d))
        if s + 1 == sections:
            break
        r1, r2, r3 = [v.astype(F32) for v in others]
        branch = ((mixed.astype(F32) + r1) + (r2 + r3)).astype(BF16).astype(F32)
        produced = (mine.astype(F32) + 0.5 * branch).astype(BF16)
        a = lax.ppermute(produced, ("pp", "yh", "tc"), hop_pairs(s, sections, False))
        c = lax.ppermute(produced, ("pp", "yh", "tc"), hop_pairs(s, sections, True))
        b = flip(a, "tc", 1)
        d = flip(c, "tc", 1)
        mine = a
        own, far = call_kernel(relay_section_kernel, outs, 13, [pad])(where, a, b, c, d, *params)

    (send,) = call_kernel(exit_pack_kernel, [shape((32, 8, 128), BF16)], 5)(where, mine, mixed, *others)
    recv = lax.all_to_all(send, ("pp", "ym", "yh", "tc"), 0, 0)
    (result,) = call_kernel(exit_unpack_kernel, [shape((2, T // sections, 32), BF16)], 1)(where, recv)
    return result


def solution(mesh):
    split = Mesh(
        mesh.devices.reshape(mesh.shape["pp"], 2, 2, 4, 2), ("pp", "ym", "yh", "tz", "tc")
    )
    in_specs = (
        P(None, "pp", TP + FS),
        P("pp", None),
        P("pp", None, TP, FS, None),
        P("pp", None, TP, FS, None),
        P("pp", None, TP, None),
        P("pp", None, TP, None),
        P("pp", None, None, TP, FS),
        P("pp", None, TP, FS),
        P("pp", None, TP, FS),
        P("pp", TP, FS),
        P("pp", None, TP, FS, None),
        P("pp", None, TP, None),
        P("pp", None, TP, None),
        P("pp", TP, FS, None, None),
    )
    out_specs = P(None, "pp", TP + FS)
    return jax.shard_map(
        per_device, mesh=split, in_specs=in_specs, out_specs=out_specs, check_vma=False
    )
```

```python
import jax
import jax.numpy as jnp
from jax import lax
from jax.experimental import pallas as pl
from jax.experimental.pallas import tpu as pltpu
from jax.sharding import Mesh
from jax.sharding import PartitionSpec as P


FS = ("ym", "yh")
TP = ("tz", "tc")
BLOCKS = ("pp", "tz", "tc")
EPS = 1e-06
T = 96
D = 1024
F32 = jnp.float32
BF16 = jnp.bfloat16
ROWS = 168


def lanes(shape):
    return lax.broadcasted_iota(jnp.int32, shape, len(shape) - 1)


def split3(v):
    hi = v.astype(BF16).astype(F32)
    mid = (v - hi).astype(BF16).astype(F32)
    low = v - hi - mid
    return hi, mid, low


def flag(where_ref, row, width=256):
    return where_ref[row : row + 1, :width] == 0


def permuted(v):
    group = lanes((v.shape[0], 128)) // 32
    out = []
    for h in range(2):
        for c in range(2):
            for p in range(2):
                block = None
                for g in range(4):
                    zz, m = g // 2, g % 2
                    n = (2 * p + zz) * 2 + c
                    moved = v[:, n * 128 : (n + 1) * 128]
                    turn = (64 * zz - 32 * m - 32 * h) % 128
                    if turn:
                        moved = pltpu.roll(moved, turn, 1)
                    block = moved if block is None else jnp.where(group == g, moved, block)
                out.append(block)
    return out


def pack_kernel(
    where_ref,
    micro_hbm,
    gate_hbm,
    value_hbm,
    step_hbm,
    out_hbm,
    taps_hbm,
    bias_hbm,
    decay_hbm,
    skip_hbm,
    gain_hbm,
    taps_w_hbm,
    taps_r_hbm,
    near_ref,
    away_ref,
    same_ref,
    other_ref,
    gain_out,
    taps_w_out,
    taps_r_out,
    *scratch,
):
    sources = (
        gate_hbm,
        value_hbm,
        out_hbm,
        step_hbm,
        taps_hbm,
        bias_hbm,
        decay_hbm,
        skip_hbm,
        gain_hbm,
        micro_hbm,
        taps_w_hbm,
        taps_r_hbm,
    )
    buffers, sems = (*scratch[:-1], taps_w_out, taps_r_out), scratch[-1]
    copies = [pltpu.make_async_copy(s, b, sems.at[i]) for i, (s, b) in enumerate(zip(sources, buffers))]
    for copy in copies:
        copy.start()
    for copy in copies:
        copy.wait()
    gate_ref, value_ref, out_ref, step_ref, taps_ref, bias_ref, decay_ref, skip_ref, gain_ref, micro_ref = buffers[:10]
    core = flag(where_ref, 1, 128)
    half = flag(where_ref, 0, 128)
    gate = jnp.concatenate(permuted(gate_ref[...].astype(F32)), axis=1).astype(BF16)
    value = jnp.concatenate(permuted(value_ref[...].astype(F32)), axis=1).astype(BF16)
    step = jnp.concatenate(permuted(step_ref[...].astype(F32)), axis=1)
    gain_out[...] = jnp.concatenate(permuted(gain_ref[...]), axis=1)
    blank = jnp.zeros((1, 64), F32)
    wide = lambda ref, k: jnp.broadcast_to(ref[:, k : k + 1], (1, 128))
    row_a = [piece for k in range(5) for piece in (blank, taps_ref[k])]
    row_a = jnp.concatenate(row_a + [wide(bias_ref, 0), wide(bias_ref, 1), blank, blank], axis=1)
    row_b = [wide(decay_ref, 0), wide(decay_ref, 1), wide(skip_ref, 0)] + [blank] * 10
    row_b = jnp.concatenate(row_b, axis=1)
    misc = jnp.concatenate([step, *split3(row_a), *split3(row_b)], axis=0).astype(BF16)
    out = permuted(out_ref[...].astype(F32))
    halves = []
    for h in range(2):
        first, second = out[4 * h : 4 * h + 2], out[4 * h + 2 : 4 * h + 4]
        own = [jnp.where(core, a, b) for a, b in zip(first, second)]
        far = [jnp.where(core, b, a) for a, b in zip(first, second)]
        halves.append(own + far)
    for ref, pair in ((same_ref, zip(*halves)), (other_ref, zip(*halves[::-1]))):
        part = jnp.concatenate([jnp.where(half, a, b) for a, b in pair], axis=1)
        ref[0:64] = gate
        ref[64:128] = value
        ref[128:160] = jnp.concatenate([part[0:32], part[32:64]], axis=1).astype(BF16)
        ref[160:168] = misc
    first = flag(where_ref, 4, 32)
    micro = [micro_ref[m].astype(F32) for m in range(2)]
    near_ref[...] = jnp.where(first, micro[0], micro[1]).astype(BF16)
    away_ref[...] = jnp.where(first, micro[1], micro[0]).astype(BF16)


def block_kernel(where_ref, r0_ref, r1_ref, r2_ref, r3_ref, send_ref):
    y = 2 * where_ref[4:5, :128] + where_ref[0:1, :128]
    group = lanes((24, 128)) // 32
    blank = jnp.zeros((24, 96), F32)
    block = jnp.zeros((24, 128), F32)
    for bits, ref in enumerate((r0_ref, r1_ref, r2_ref, r3_ref)):
        wide = jnp.concatenate([ref[...].astype(F32), blank], axis=1)
        for k in range(4):
            moved = wide if k == 0 else pltpu.roll(wide, 32 * k, 1)
            block = jnp.where((group == k) & ((y ^ bits) == group), moved, block)
    block = block.astype(BF16)
    for peer in range(32):
        send_ref[peer] = block


def nt_dot(a, b):
    return lax.dot_general(a, b, (((1,), (1,)), ((), ())), preferred_element_type=F32)


def nn_dot(a, b):
    return lax.dot_general(a, b, (((1,), (0,)), ((), ())), preferred_element_type=F32)


def silu(v):
    return v * jax.nn.sigmoid(v)


def section_body(quarters, weight_refs, write_ref, read_ref, gain_ref, taps_refs, own_ref, far_ref, pad_ref):
    low = lanes((T, 128)) < 64
    total = None
    for pair in quarters:
        for q in pair:
            sq = q * q
            sq = sq[:, :128] + sq[:, 128:]
            total = sq if total is None else total + sq
    scale = lax.rsqrt(jnp.sum(total, axis=1, keepdims=True) * (1.0 / D) + EPS)
    blocks = []
    for h in range(2):
        for c in range(2):
            n = (2 * h + c) * 256
            blocks.append((quarters[h][c] * scale * gain_ref[:, n : n + 256]).astype(BF16))
    normed = jnp.concatenate(blocks, axis=1)

    step_rows = jnp.concatenate([w[160:168].astype(F32)[0:2] for w in weight_refs], axis=0)
    step_raw = nt_dot(step_rows.astype(BF16), normed)
    small = []
    for w in weight_refs:
        misc = w[160:168].astype(F32)
        small.append((misc[2:3] + misc[3:4] + misc[4:5], misc[5:6] + misc[6:7] + misc[7:8]))
    bias = jnp.concatenate([s[0][:, 640 + 128 * d : 640 + 128 * d + T] for s in small for d in range(2)], axis=0)
    decay = jnp.concatenate([s[1][:, 128 * d : 128 * d + T] for s in small for d in range(2)], axis=0)
    raw = step_raw + bias
    dt = jnp.maximum(raw, 0.0) + jnp.log1p(jnp.exp(-jnp.abs(raw)))
    log_decay = dt * (-jnp.exp(decay))
    parts = [s.astype(BF16) for s in split3(log_decay)]
    row_id = lax.broadcasted_iota(jnp.int32, (T, T), 0)
    col_id = lax.broadcasted_iota(jnp.int32, (T, T), 1)
    upto = (row_id <= col_id).astype(F32).astype(BF16)
    since = (row_id >= col_id).astype(F32).astype(BF16)
    fwd_all = (nn_dot(parts[0], upto) + nn_dot(parts[1], upto)) + nn_dot(parts[2], upto)
    bwd_all = (nn_dot(parts[0], since) + nn_dot(parts[1], since)) + nn_dot(parts[2], since)
    odd = lax.broadcasted_iota(jnp.int32, (8, T), 0) % 2 == 1
    cum = jnp.where(odd, bwd_all, fwd_all)
    cum_pad = jnp.concatenate([cum, jnp.zeros((8, 128 - T), F32)], axis=1)
    cum_cols = cum_pad.T[:T]

    gv01 = nt_dot(normed, jnp.concatenate([weight_refs[0][0:128], weight_refs[1][0:128]], axis=0))
    gv23 = nt_dot(normed, jnp.concatenate([weight_refs[2][0:128], weight_refs[3][0:128]], axis=0))
    wr_rows = [
        jnp.concatenate([r[n * 128 + y * 32 : n * 128 + y * 32 + 32] for r in (write_ref, read_ref)], axis=1)
        for h in range(2)
        for c in range(2)
        for n in (c, 2 + c, 4 + c, 6 + c)
        for y in (h, 2 + h)
    ]
    wr = nn_dot(normed, jnp.concatenate(wr_rows, axis=0))
    pad_ref[0:8] = jnp.zeros((8, 768), F32)
    pad_ref[8 + T : 16 + T] = jnp.zeros((8, 768), F32)
    pad_ref[8 : 8 + T, 0:256] = gv01.astype(BF16).astype(F32)
    pad_ref[8 : 8 + T, 256:512] = gv23.astype(BF16).astype(F32)
    pad_ref[8 : 8 + T, 512:768] = wr.astype(BF16).astype(F32)
    acts = []
    for g in range(6):
        span = slice(g * 128, (g + 1) * 128)
        acc = None
        for k in range(5):
            tap = small[g][0][:, k * 128 : (k + 1) * 128] if g < 4 else taps_refs[g - 4][k]
            term = pad_ref[6 + k : 6 + k + T, span] * tap
            acc = term if acc is None else acc + term
        acts.append(silu(acc).astype(BF16))
    scores = nt_dot(acts[5], acts[4])
    lower = row_id >= col_id
    diagonal = row_id == col_id
    gated = []
    for j in range(4):
        fc = cum_cols[:, 2 * j : 2 * j + 1]
        bc = cum_cols[:, 2 * j + 1 : 2 * j + 2]
        fr = cum[2 * j : 2 * j + 1]
        br = cum[2 * j + 1 : 2 * j + 2]
        d0 = dt[2 * j : 2 * j + 1]
        d1 = dt[2 * j + 1 : 2 * j + 2]
        mix = jnp.exp(jnp.where(lower, fc - fr, bc - br)) * jnp.where(lower, d0, d1)
        mix = mix + jnp.where(diagonal, d1, 0.0)
        combined = scores * mix
        high = combined.astype(BF16)
        rest = (combined - high.astype(F32)).astype(BF16)
        y = nn_dot(high, acts[j]) + nn_dot(rest, acts[j])
        y = y + small[j][1][:, 256:384] * acts[j].astype(F32)
        gate = pltpu.roll(pad_ref[8 : 8 + T, j * 128 : (j + 1) * 128], 64, 1)
        gated.append(y * silu(gate))
    pairs = [jnp.where(low, pltpu.roll(gated[2 * i], 64, 1), gated[2 * i + 1]).astype(BF16) for i in range(2)]
    gated_all = jnp.concatenate(pairs, axis=1)
    for side, ref in ((0, own_ref), (1, far_ref)):
        weight = jnp.concatenate(
            [
                w[128:160, 512 * r + 256 * side : 512 * r + 256 * side + 256]
                for w in weight_refs
                for r in range(2)
            ],
            axis=0,
        )
        ref[...] = nn_dot(gated_all, weight).astype(ref.dtype)


def entry_section_kernel(where_ref, recv_ref, *refs):
    *rest, quarter_out, own_ref, far_ref, pad_ref, quarter_ref = refs
    tokens = [
        jnp.concatenate([recv_ref[x * 8 + n].astype(F32) for x in range(4)], axis=0) for n in range(8)
    ]
    blocks = permuted(jnp.concatenate(tokens, axis=1))
    for q in range(4):
        quarter_ref[q] = jnp.concatenate(blocks[2 * q : 2 * q + 2], axis=1)
    quarters = [[quarter_ref[2 * h + c] for c in range(2)] for h in range(2)]
    half, core = flag(where_ref, 0), flag(where_ref, 1)
    mine = jnp.where(half, jnp.where(core, *quarters[0]), jnp.where(core, *quarters[1]))
    quarter_out[...] = mine.astype(BF16)
    section_body(quarters, rest[0:4], *rest[4:7], rest[7:9], own_ref, far_ref, pad_ref)


def relay_section_kernel(where_ref, a_ref, b_ref, c_ref, d_ref, *refs):
    *rest, own_ref, far_ref, pad_ref = refs
    half, core = flag(where_ref, 0), flag(where_ref, 1)
    a, b, c, d = [r[...].astype(F32) for r in (a_ref, b_ref, c_ref, d_ref)]
    own0, own1 = jnp.where(half, a, c), jnp.where(half, c, a)
    far0, far1 = jnp.where(half, b, d), jnp.where(half, d, b)
    quarters = [
        [jnp.where(core, own0, far0), jnp.where(core, far0, own0)],
        [jnp.where(core, own1, far1), jnp.where(core, far1, own1)],
    ]
    section_body(quarters, rest[0:4], *rest[4:7], rest[7:9], own_ref, far_ref, pad_ref)


def exit_pack_kernel(where_ref, mine_ref, m0_ref, m1_ref, m2_ref, m3_ref, send_ref):
    branch = (m0_ref[...].astype(F32) + m1_ref[...].astype(F32)) + (m2_ref[...].astype(F32) + m3_ref[...].astype(F32))
    branch = branch.astype(BF16).astype(F32)
    final = (mine_ref[...].astype(F32) + 0.5 * branch).astype(BF16).astype(F32)
    squares = final * final
    squares = jnp.sum(squares[:, :128] + squares[:, 128:], axis=1, keepdims=True)
    squares = jnp.broadcast_to(squares, (T, 128))
    own = jnp.where(flag(where_ref, 2, 128), final[:, :128], final[:, 128:])
    own = jnp.where(flag(where_ref, 3, 128), own, pltpu.roll(own, 64, 1))
    turned = {d: own if d == 0 else pltpu.roll(own, (32 * d) % 128, 1) for d in (-1, 0, 1, 2, 3)}
    lane = lanes((6, 128))
    group = lane // 32
    spot = lane % 32 == lax.broadcasted_iota(jnp.int32, (6, 128), 0)
    for x in range(4):
        rows = [slice(x * 24 + k * 6, x * 24 + k * 6 + 6) for k in range(4)]
        total = squares[rows[0]]
        for k in range(1, 4):
            total = jnp.where(group == k, squares[rows[k]], total)
        total = jnp.sum(jnp.where(spot, total, 0.0), axis=0, keepdims=True)
        parts = split3(total)
        for m in range(2):
            block = turned[-m][rows[0]]
            for k in range(1, 4):
                block = jnp.where(group == k, turned[k - m][rows[k]], block)
            message = jnp.concatenate([block, parts[0], parts[1]], axis=0).astype(BF16)
            for peer in range(4):
                send_ref[(x * 2 + m) * 4 + peer] = message


def exit_unpack_kernel(where_ref, recv_ref, out_ref):
    half, core = flag(where_ref, 0, 128), flag(where_ref, 1, 128)
    lane = lanes((8, 128))
    spot = lane % 32 == lax.broadcasted_iota(jnp.int32, (8, 128), 0)
    same_group = (
        lax.broadcasted_iota(jnp.int32, (128, 128), 0) // 32 == lanes((128, 128)) // 32
    ).astype(F32).astype(BF16)
    parts = []
    for m in range(2):
        first = (6 + m) * 4
        sums = [recv_ref[first + i].astype(F32) for i in range(4)]
        total = (sums[0][6:7] + sums[0][7:8]) + (sums[1][6:7] + sums[1][7:8])
        total = total + ((sums[2][6:7] + sums[2][7:8]) + (sums[3][6:7] + sums[3][7:8]))
        parts += split3(jnp.where(spot, jnp.broadcast_to(total, (8, 128)), 0.0))
    spread = nn_dot(jnp.concatenate(parts, axis=0).astype(BF16), same_group)
    for m in range(2):
        total = (spread[24 * m : 24 * m + 8] + spread[24 * m + 8 : 24 * m + 16]) + spread[24 * m + 16 : 24 * m + 24]
        blocks = [recv_ref[(6 + m) * 4 + i].astype(F32) for i in range(4)]
        block = jnp.where(half, jnp.where(core, *blocks[:2]), jnp.where(core, *blocks[2:]))
        block = block * lax.rsqrt(total * (1.0 / D) + EPS)
        rows = [block if k == 0 else pltpu.roll(block, 128 - 32 * k, 1) for k in range(4)]
        out_ref[m] = jnp.concatenate([r[:6, :32] for r in rows], axis=0).astype(BF16)


VMEM_SPEC = pl.BlockSpec(memory_space=pltpu.VMEM)


def call_kernel(kernel, out_shape, count, scratch=()):
    return pl.pallas_call(
        kernel,
        out_shape=out_shape,
        in_specs=[VMEM_SPEC] + [VMEM_SPEC] * count,
        out_specs=[VMEM_SPEC] * len(out_shape),
        scratch_shapes=scratch,
        compiler_params=pltpu.CompilerParams(vmem_limit_bytes=24 * 1024 * 1024),
    )


def flip(v, axes, bits):
    size = lax.axis_size(axes)
    return lax.ppermute(v, axes, [(i, i ^ bits) for i in range(size)])


def sum_pairs(active, sections, bits):
    pairs = []
    for i in range(sections):
        for z in range(4):
            for c in range(2):
                target = 2 * (z ^ bits) + c if i == active else 2 * z + 1 - c
                pairs.append((8 * i + 2 * z + c, 8 * i + target))
    return pairs


def per_device(
    micro_in,
    norm_gain,
    proj_gate,
    proj_value,
    proj_write,
    proj_read,
    proj_step,
    step_bias,
    decay_log,
    skip_gain,
    conv_value,
    conv_write,
    conv_read,
    proj_out,
):
    sections = lax.axis_size("pp")
    half = lax.axis_index("yh")
    micro = lax.axis_index("ym")
    core = lax.axis_index("tc")
    zpos = lax.axis_index("tz")
    where = jnp.stack([half, core, zpos // 2, zpos % 2, micro]).astype(jnp.int32)
    where = jnp.broadcast_to(where[:, None], (5, 256))

    shape = jax.ShapeDtypeStruct
    raw = (
        micro_in,
        proj_gate[0, :, 0, 0, :].T,
        proj_value[0, :, 0, 0, :].T,
        proj_step[0, :, :, 0, 0].T,
        proj_out[0, 0, 0],
        conv_value.reshape(5, 1, 64),
        step_bias.reshape(1, 2),
        decay_log.reshape(1, 2),
        skip_gain.reshape(1, 1),
        norm_gain,
        conv_write.reshape(5, 1, 128),
        conv_read.reshape(5, 1, 128),
    )
    order = (1, 2, 4, 3, 5, 6, 7, 8, 9, 0)
    near, away, same, other, gain, taps_w, taps_r = pl.pallas_call(
        pack_kernel,
        out_shape=[
            shape((T // 4, 32), BF16),
            shape((T // 4, 32), BF16),
            shape((ROWS, D), BF16),
            shape((ROWS, D), BF16),
            shape((1, D), F32),
            shape((5, 1, 128), F32),
            shape((5, 1, 128), F32),
        ],
        in_specs=[VMEM_SPEC] + [pl.BlockSpec(memory_space=pltpu.HBM)] * len(raw),
        out_specs=[VMEM_SPEC] * 7,
        scratch_shapes=[pltpu.VMEM(raw[i].shape, raw[i].dtype) for i in order]
        + [pltpu.SemaphoreType.DMA((len(raw),))],
        compiler_params=pltpu.CompilerParams(vmem_limit_bytes=24 * 1024 * 1024),
    )(where, *[pltpu.with_memory_space_constraint(v, pltpu.HBM) if i != 8 else v for i, v in enumerate(raw)])
    r1 = flip(near, FS, 1)
    r2 = flip(away, FS, 2)
    r3 = flip(away, FS, 3)
    w1 = flip(other, FS, 1)
    w2 = flip(same, FS, 2)
    w3 = flip(other, FS, 3)
    (send,) = call_kernel(block_kernel, [shape((32, T // 4, 128), BF16)], 4)(where, near, r1, r2, r3)
    recv = lax.all_to_all(send, BLOCKS, 0, 0)

    params = (same, w1, w2, w3, proj_write[0, :, 0, :], proj_read[0, :, 0, :], gain, taps_w, taps_r)
    quarter = shape((T, 256), BF16)
    outs = [shape((T, 256), F32), quarter]
    pad = pltpu.VMEM((T + 16, 768), F32)
    mine, own, far = call_kernel(
        entry_section_kernel, [quarter, *outs], 10, [pad, pltpu.VMEM((4, T, 256), F32)]
    )(where, recv, *params)
    hop = [(i, (i + 1) % sections) for i in range(sections)]
    hop_flip = [(2 * i + h, 2 * j + 1 - h) for i, j in hop for h in range(2)]
    for s in range(sections):
        got = flip(far, "tc", 1)
        mixed = (own + got.astype(F32)).astype(BF16)
        others = []
        for d in (1, 2, 3):
            others.append(lax.ppermute(mixed, ("pp", "tz", "tc"), sum_pairs(s, sections, d)))
        if s + 1 == sections:
            break
        r1, r2, r3 = [v.astype(F32) for v in others]
        branch = ((mixed.astype(F32) + r1) + (r2 + r3)).astype(BF16).astype(F32)
        produced = (mine.astype(F32) + 0.5 * branch).astype(BF16)
        a = lax.ppermute(produced, "pp", hop)
        c = lax.ppermute(produced, ("pp", "yh"), hop_flip)
        b = flip(a, "tc", 1)
        d = flip(c, "tc", 1)
        mine = a
        own, far = call_kernel(relay_section_kernel, outs, 13, [pad])(where, a, b, c, d, *params)

    (send,) = call_kernel(exit_pack_kernel, [shape((32, 8, 128), BF16)], 5)(where, mine, mixed, *others)
    recv = lax.all_to_all(send, ("pp", "ym", "yh", "tc"), 0, 0)
    (result,) = call_kernel(exit_unpack_kernel, [shape((2, T // sections, 32), BF16)], 1)(where, recv)
    return result


def solution(mesh):
    split = Mesh(
        mesh.devices.reshape(mesh.shape["pp"], 2, 2, 4, 2), ("pp", "ym", "yh", "tz", "tc")
    )
    in_specs = (
        P(None, "pp", TP + FS),
        P("pp", None),
        P("pp", None, TP, FS, None),
        P("pp", None, TP, FS, None),
        P("pp", None, TP, None),
        P("pp", None, TP, None),
        P("pp", None, None, TP, FS),
        P("pp", None, TP, FS),
        P("pp", None, TP, FS),
        P("pp", TP, FS),
        P("pp", None, TP, FS, None),
        P("pp", None, TP, None),
        P("pp", None, TP, None),
        P("pp", TP, FS, None, None),
    )
    out_specs = P(None, "pp", TP + FS)
    return jax.shard_map(
        per_device, mesh=split, in_specs=in_specs, out_specs=out_specs, check_vma=False
    )
```

```python
import jax
import jax.numpy as jnp
from jax import lax
from jax.experimental import pallas as pl
from jax.experimental.pallas import tpu as pltpu
from jax.sharding import Mesh
from jax.sharding import PartitionSpec as P


FS = ("ym", "yh")
TP = ("tz", "tc")
BLOCKS = ("pp", "tz", "tc")
EPS = 1e-06
T = 96
D = 1024
F32 = jnp.float32
BF16 = jnp.bfloat16
ROWS = 168


def lanes(shape):
    return lax.broadcasted_iota(jnp.int32, shape, len(shape) - 1)


def split3(v):
    hi = v.astype(BF16).astype(F32)
    mid = (v - hi).astype(BF16).astype(F32)
    low = v - hi - mid
    return hi, mid, low


def flag(where_ref, row, width=256):
    return where_ref[row : row + 1, :width] == 0


def permuted(v):
    group = lanes((v.shape[0], 128)) // 32
    out = []
    for h in range(2):
        for c in range(2):
            for p in range(2):
                block = None
                for g in range(4):
                    zz, m = g // 2, g % 2
                    n = (2 * p + zz) * 2 + c
                    moved = v[:, n * 128 : (n + 1) * 128]
                    turn = (64 * zz - 32 * m - 32 * h) % 128
                    if turn:
                        moved = pltpu.roll(moved, turn, 1)
                    block = moved if block is None else jnp.where(group == g, moved, block)
                out.append(block)
    return out


def pack_kernel(
    where_ref,
    micro_hbm,
    gate_hbm,
    value_hbm,
    step_hbm,
    out_hbm,
    taps_hbm,
    bias_hbm,
    decay_hbm,
    skip_hbm,
    gain_hbm,
    taps_w_hbm,
    taps_r_hbm,
    near_ref,
    away_ref,
    same_ref,
    other_ref,
    gain_out,
    taps_w_out,
    taps_r_out,
    *scratch,
):
    sources = (
        gate_hbm,
        value_hbm,
        out_hbm,
        step_hbm,
        taps_hbm,
        bias_hbm,
        decay_hbm,
        skip_hbm,
        gain_hbm,
        micro_hbm,
        taps_w_hbm,
        taps_r_hbm,
    )
    buffers, sems = (*scratch[:-1], taps_w_out, taps_r_out), scratch[-1]
    copies = [pltpu.make_async_copy(s, b, sems.at[i]) for i, (s, b) in enumerate(zip(sources, buffers))]
    for copy in copies:
        copy.start()
    for copy in copies:
        copy.wait()
    gate_ref, value_ref, out_ref, step_ref, taps_ref, bias_ref, decay_ref, skip_ref, gain_ref, micro_ref = buffers[:10]
    core = flag(where_ref, 1, 128)
    half = flag(where_ref, 0, 128)
    gate = jnp.concatenate(permuted(gate_ref[...].astype(F32)), axis=1).astype(BF16)
    value = jnp.concatenate(permuted(value_ref[...].astype(F32)), axis=1).astype(BF16)
    step = jnp.concatenate(permuted(step_ref[...].astype(F32)), axis=1)
    gain_out[...] = jnp.concatenate(permuted(gain_ref[...]), axis=1)
    blank = jnp.zeros((1, 64), F32)
    wide = lambda ref, k: jnp.broadcast_to(ref[:, k : k + 1], (1, 128))
    row_a = [taps_ref[k] for k in range(5) for _ in range(2)]
    row_a = jnp.concatenate(row_a + [wide(bias_ref, 0), wide(bias_ref, 1), blank, blank], axis=1)
    row_b = [wide(decay_ref, 0), wide(decay_ref, 1), wide(skip_ref, 0)] + [blank] * 10
    row_b = jnp.concatenate(row_b, axis=1)
    misc = jnp.concatenate([step, *split3(row_a), *split3(row_b)], axis=0).astype(BF16)
    out = permuted(out_ref[...].astype(F32))
    halves = []
    for h in range(2):
        first, second = out[4 * h : 4 * h + 2], out[4 * h + 2 : 4 * h + 4]
        own = [jnp.where(core, a, b) for a, b in zip(first, second)]
        far = [jnp.where(core, b, a) for a, b in zip(first, second)]
        halves.append(own + far)
    for ref, pair in ((same_ref, zip(*halves)), (other_ref, zip(*halves[::-1]))):
        part = jnp.concatenate([jnp.where(half, a, b) for a, b in pair], axis=1)
        ref[0:64] = gate
        ref[64:128] = value
        ref[128:160] = jnp.concatenate([part[0:32], part[32:64]], axis=1).astype(BF16)
        ref[160:168] = misc
    first = flag(where_ref, 4, 32)
    micro = [micro_ref[m].astype(F32) for m in range(2)]
    near_ref[...] = jnp.where(first, micro[0], micro[1]).astype(BF16)
    away_ref[...] = jnp.where(first, micro[1], micro[0]).astype(BF16)


def block_kernel(where_ref, r0_ref, r1_ref, r2_ref, r3_ref, send_ref):
    y = 2 * where_ref[4:5, :128] + where_ref[0:1, :128]
    group = lanes((24, 128)) // 32
    blank = jnp.zeros((24, 96), F32)
    block = jnp.zeros((24, 128), F32)
    for bits, ref in enumerate((r0_ref, r1_ref, r2_ref, r3_ref)):
        wide = jnp.concatenate([ref[...].astype(F32), blank], axis=1)
        for k in range(4):
            moved = wide if k == 0 else pltpu.roll(wide, 32 * k, 1)
            block = jnp.where((group == k) & ((y ^ bits) == group), moved, block)
    block = block.astype(BF16)
    for peer in range(32):
        send_ref[peer] = block


def nt_dot(a, b):
    return lax.dot_general(a, b, (((1,), (1,)), ((), ())), preferred_element_type=F32)


def nn_dot(a, b):
    return lax.dot_general(a, b, (((1,), (0,)), ((), ())), preferred_element_type=F32)


def silu(v):
    return v * jax.nn.sigmoid(v)


def section_body(quarters, weight_refs, write_ref, read_ref, gain_ref, taps_refs, own_ref, far_ref, pad_ref):
    low = lanes((T, 128)) < 64
    total = None
    for pair in quarters:
        for q in pair:
            sq = q * q
            sq = sq[:, :128] + sq[:, 128:]
            total = sq if total is None else total + sq
    scale = lax.rsqrt(jnp.sum(total, axis=1, keepdims=True) * (1.0 / D) + EPS)
    blocks = []
    for h in range(2):
        for c in range(2):
            n = (2 * h + c) * 256
            blocks.append((quarters[h][c] * scale * gain_ref[:, n : n + 256]).astype(BF16))
    normed = jnp.concatenate(blocks, axis=1)

    step_rows = jnp.concatenate([w[160:168].astype(F32)[0:2] for w in weight_refs], axis=0)
    step_raw = nt_dot(step_rows.astype(BF16), normed)
    small = []
    for w in weight_refs:
        misc = w[160:168].astype(F32)
        small.append((misc[2:3] + misc[3:4] + misc[4:5], misc[5:6] + misc[6:7] + misc[7:8]))
    bias = jnp.concatenate([s[0][:, 640 + 128 * d : 640 + 128 * d + T] for s in small for d in range(2)], axis=0)
    decay = jnp.concatenate([s[1][:, 128 * d : 128 * d + T] for s in small for d in range(2)], axis=0)
    raw = step_raw + bias
    dt = jnp.maximum(raw, 0.0) + jnp.log1p(jnp.exp(-jnp.abs(raw)))
    log_decay = dt * (-jnp.exp(decay))
    parts = [s.astype(BF16) for s in split3(log_decay)]
    row_id = lax.broadcasted_iota(jnp.int32, (T, T), 0)
    col_id = lax.broadcasted_iota(jnp.int32, (T, T), 1)
    upto = (row_id <= col_id).astype(F32).astype(BF16)
    since = (row_id >= col_id).astype(F32).astype(BF16)
    fwd_all = (nn_dot(parts[0], upto) + nn_dot(parts[1], upto)) + nn_dot(parts[2], upto)
    bwd_all = (nn_dot(parts[0], since) + nn_dot(parts[1], since)) + nn_dot(parts[2], since)
    odd = lax.broadcasted_iota(jnp.int32, (8, T), 0) % 2 == 1
    cum = jnp.where(odd, bwd_all, fwd_all)
    cum_pad = jnp.concatenate([cum, jnp.zeros((8, 128 - T), F32)], axis=1)
    cum_cols = cum_pad.T[:T]

    wr_rows = [
        jnp.concatenate([r[n * 128 + y * 32 : n * 128 + y * 32 + 32] for r in (write_ref, read_ref)], axis=1)
        for h in range(2)
        for c in range(2)
        for n in (c, 2 + c, 4 + c, 6 + c)
        for y in (h, 2 + h)
    ]
    wr = nn_dot(normed, jnp.concatenate(wr_rows, axis=0))
    pad_ref[0:8, 0:512] = jnp.zeros((8, 512), F32)
    pad_ref[8 + T : 16 + T, 0:512] = jnp.zeros((8, 512), F32)
    for i in range(2):
        pair = weight_refs[2 * i : 2 * i + 2]
        rows = jnp.concatenate([w[k * 64 : k * 64 + 64] for k in range(2) for w in pair], axis=0)
        gate_value = nt_dot(normed, rows).astype(BF16).astype(F32)
        pad_ref[8 : 8 + T, 512 + 128 * i : 640 + 128 * i] = gate_value[:, :128]
        pad_ref[8 : 8 + T, 128 * i : 128 * i + 128] = gate_value[:, 128:]
    pad_ref[8 : 8 + T, 256:512] = wr.astype(BF16).astype(F32)
    low_row = lanes((1, 128)) < 64
    acts = []
    for g in range(4):
        span = slice(g * 128, (g + 1) * 128)
        acc = None
        for k in range(5):
            if g < 2:
                tap = jnp.where(low_row, *[small[2 * g + e][0][:, k * 128 : (k + 1) * 128] for e in range(2)])
            else:
                tap = taps_refs[g - 2][k]
            term = pad_ref[6 + k : 6 + k + T, span] * tap
            acc = term if acc is None else acc + term
        acts.append(silu(acc).astype(BF16))
    scores = nt_dot(acts[3], acts[2])
    lower = row_id >= col_id
    diagonal = row_id == col_id
    pairs = []
    for i in range(2):
        high = []
        for j in (2 * i, 2 * i + 1):
            fc = cum_cols[:, 2 * j : 2 * j + 1]
            bc = cum_cols[:, 2 * j + 1 : 2 * j + 2]
            fr = cum[2 * j : 2 * j + 1]
            br = cum[2 * j + 1 : 2 * j + 2]
            d0 = dt[2 * j : 2 * j + 1]
            d1 = dt[2 * j + 1 : 2 * j + 2]
            mix = jnp.exp(jnp.where(lower, fc - fr, bc - br)) * jnp.where(lower, d0, d1)
            mix = mix + jnp.where(diagonal, d1, 0.0)
            combined = scores * mix
            high.append(combined.astype(BF16))
        y = nn_dot(jnp.concatenate(high, axis=0), acts[i])
        skip = jnp.where(low_row, *[small[2 * i + e][1][:, 256:384] for e in range(2)])
        y = jnp.where(low, y[:T], y[T:]) + skip * acts[i].astype(F32)
        gate = pad_ref[8 : 8 + T, 512 + 128 * i : 640 + 128 * i]
        pairs.append((y * silu(gate)).astype(BF16))
    gated_all = jnp.concatenate(pairs, axis=1)
    for side, ref in ((0, own_ref), (1, far_ref)):
        weight = jnp.concatenate(
            [
                w[128:160, 512 * r + 256 * side : 512 * r + 256 * side + 256]
                for w in weight_refs
                for r in range(2)
            ],
            axis=0,
        )
        ref[...] = nn_dot(gated_all, weight).astype(ref.dtype)


def entry_section_kernel(where_ref, recv_ref, *refs):
    *rest, quarter_out, own_ref, far_ref, pad_ref, quarter_ref = refs
    tokens = [
        jnp.concatenate([recv_ref[x * 8 + n].astype(F32) for x in range(4)], axis=0) for n in range(8)
    ]
    blocks = permuted(jnp.concatenate(tokens, axis=1))
    for q in range(4):
        quarter_ref[q] = jnp.concatenate(blocks[2 * q : 2 * q + 2], axis=1)
    quarters = [[quarter_ref[2 * h + c] for c in range(2)] for h in range(2)]
    half, core = flag(where_ref, 0), flag(where_ref, 1)
    mine = jnp.where(half, jnp.where(core, *quarters[0]), jnp.where(core, *quarters[1]))
    quarter_out[...] = mine.astype(BF16)
    section_body(quarters, rest[0:4], *rest[4:7], rest[7:9], own_ref, far_ref, pad_ref)


def relay_section_kernel(where_ref, a_ref, b_ref, c_ref, d_ref, *refs):
    *rest, own_ref, far_ref, pad_ref = refs
    half, core = flag(where_ref, 0), flag(where_ref, 1)
    a, b, c, d = [r[...].astype(F32) for r in (a_ref, b_ref, c_ref, d_ref)]
    own0, own1 = jnp.where(half, a, c), jnp.where(half, c, a)
    far0, far1 = jnp.where(half, b, d), jnp.where(half, d, b)
    quarters = [
        [jnp.where(core, own0, far0), jnp.where(core, far0, own0)],
        [jnp.where(core, own1, far1), jnp.where(core, far1, own1)],
    ]
    section_body(quarters, rest[0:4], *rest[4:7], rest[7:9], own_ref, far_ref, pad_ref)


def exit_pack_kernel(where_ref, mine_ref, m0_ref, m1_ref, m2_ref, m3_ref, send_ref):
    branch = (m0_ref[...].astype(F32) + m1_ref[...].astype(F32)) + (m2_ref[...].astype(F32) + m3_ref[...].astype(F32))
    branch = branch.astype(BF16).astype(F32)
    final = (mine_ref[...].astype(F32) + 0.5 * branch).astype(BF16).astype(F32)
    squares = final * final
    squares = jnp.sum(squares[:, :128] + squares[:, 128:], axis=1, keepdims=True)
    squares = jnp.broadcast_to(squares, (T, 128))
    own = jnp.where(flag(where_ref, 2, 128), final[:, :128], final[:, 128:])
    own = jnp.where(flag(where_ref, 3, 128), own, pltpu.roll(own, 64, 1))
    turned = {d: own if d == 0 else pltpu.roll(own, (32 * d) % 128, 1) for d in (-1, 0, 1, 2, 3)}
    lane = lanes((6, 128))
    group = lane // 32
    spot = lane % 32 == lax.broadcasted_iota(jnp.int32, (6, 128), 0)
    for x in range(4):
        rows = [slice(x * 24 + k * 6, x * 24 + k * 6 + 6) for k in range(4)]
        total = squares[rows[0]]
        for k in range(1, 4):
            total = jnp.where(group == k, squares[rows[k]], total)
        total = jnp.sum(jnp.where(spot, total, 0.0), axis=0, keepdims=True)
        parts = split3(total)
        for m in range(2):
            block = turned[-m][rows[0]]
            for k in range(1, 4):
                block = jnp.where(group == k, turned[k - m][rows[k]], block)
            message = jnp.concatenate([block, parts[0], parts[1]], axis=0).astype(BF16)
            for peer in range(4):
                send_ref[(x * 2 + m) * 4 + peer] = message


def exit_unpack_kernel(where_ref, recv_ref, out_ref):
    half, core = flag(where_ref, 0, 128), flag(where_ref, 1, 128)
    lane = lanes((8, 128))
    spot = lane % 32 == lax.broadcasted_iota(jnp.int32, (8, 128), 0)
    same_group = (
        lax.broadcasted_iota(jnp.int32, (128, 128), 0) // 32 == lanes((128, 128)) // 32
    ).astype(F32).astype(BF16)
    parts = []
    for m in range(2):
        first = (6 + m) * 4
        sums = [recv_ref[first + i].astype(F32) for i in range(4)]
        total = (sums[0][6:7] + sums[0][7:8]) + (sums[1][6:7] + sums[1][7:8])
        total = total + ((sums[2][6:7] + sums[2][7:8]) + (sums[3][6:7] + sums[3][7:8]))
        parts += split3(jnp.where(spot, jnp.broadcast_to(total, (8, 128)), 0.0))
    spread = nn_dot(jnp.concatenate(parts, axis=0).astype(BF16), same_group)
    for m in range(2):
        total = (spread[24 * m : 24 * m + 8] + spread[24 * m + 8 : 24 * m + 16]) + spread[24 * m + 16 : 24 * m + 24]
        blocks = [recv_ref[(6 + m) * 4 + i].astype(F32) for i in range(4)]
        block = jnp.where(half, jnp.where(core, *blocks[:2]), jnp.where(core, *blocks[2:]))
        block = block * lax.rsqrt(total * (1.0 / D) + EPS)
        rows = [block if k == 0 else pltpu.roll(block, 128 - 32 * k, 1) for k in range(4)]
        out_ref[m] = jnp.concatenate([r[:6, :32] for r in rows], axis=0).astype(BF16)


VMEM_SPEC = pl.BlockSpec(memory_space=pltpu.VMEM)


def call_kernel(kernel, out_shape, count, scratch=()):
    return pl.pallas_call(
        kernel,
        out_shape=out_shape,
        in_specs=[VMEM_SPEC] + [VMEM_SPEC] * count,
        out_specs=[VMEM_SPEC] * len(out_shape),
        scratch_shapes=scratch,
        compiler_params=pltpu.CompilerParams(vmem_limit_bytes=24 * 1024 * 1024),
    )


def flip(v, axes, bits):
    size = lax.axis_size(axes)
    return lax.ppermute(v, axes, [(i, i ^ bits) for i in range(size)])


def sum_pairs(active, sections, bits):
    pairs = []
    for i in range(sections):
        for z in range(4):
            for c in range(2):
                target = 2 * (z ^ bits) + c if i == active else 2 * z + 1 - c
                pairs.append((8 * i + 2 * z + c, 8 * i + target))
    return pairs


def per_device(
    micro_in,
    norm_gain,
    proj_gate,
    proj_value,
    proj_write,
    proj_read,
    proj_step,
    step_bias,
    decay_log,
    skip_gain,
    conv_value,
    conv_write,
    conv_read,
    proj_out,
):
    sections = lax.axis_size("pp")
    half = lax.axis_index("yh")
    micro = lax.axis_index("ym")
    core = lax.axis_index("tc")
    zpos = lax.axis_index("tz")
    where = jnp.stack([half, core, zpos // 2, zpos % 2, micro]).astype(jnp.int32)
    where = jnp.broadcast_to(where[:, None], (5, 256))

    shape = jax.ShapeDtypeStruct
    raw = (
        micro_in,
        proj_gate[0, :, 0, 0, :].T,
        proj_value[0, :, 0, 0, :].T,
        proj_step[0, :, :, 0, 0].T,
        proj_out[0, 0, 0],
        conv_value.reshape(5, 1, 64),
        step_bias.reshape(1, 2),
        decay_log.reshape(1, 2),
        skip_gain.reshape(1, 1),
        norm_gain,
        conv_write.reshape(5, 1, 128),
        conv_read.reshape(5, 1, 128),
    )
    order = (1, 2, 4, 3, 5, 6, 7, 8, 9, 0)
    near, away, same, other, gain, taps_w, taps_r = pl.pallas_call(
        pack_kernel,
        out_shape=[
            shape((T // 4, 32), BF16),
            shape((T // 4, 32), BF16),
            shape((ROWS, D), BF16),
            shape((ROWS, D), BF16),
            shape((1, D), F32),
            shape((5, 1, 128), F32),
            shape((5, 1, 128), F32),
        ],
        in_specs=[VMEM_SPEC] + [pl.BlockSpec(memory_space=pltpu.HBM)] * len(raw),
        out_specs=[VMEM_SPEC] * 7,
        scratch_shapes=[pltpu.VMEM(raw[i].shape, raw[i].dtype) for i in order]
        + [pltpu.SemaphoreType.DMA((len(raw),))],
        compiler_params=pltpu.CompilerParams(vmem_limit_bytes=24 * 1024 * 1024),
    )(where, *[pltpu.with_memory_space_constraint(v, pltpu.HBM) if i != 8 else v for i, v in enumerate(raw)])
    r1 = flip(near, FS, 1)
    r2 = flip(away, FS, 2)
    r3 = flip(away, FS, 3)
    w1 = flip(other, FS, 1)
    w2 = flip(same, FS, 2)
    w3 = flip(other, FS, 3)
    (send,) = call_kernel(block_kernel, [shape((32, T // 4, 128), BF16)], 4)(where, near, r1, r2, r3)
    recv = lax.all_to_all(send, BLOCKS, 0, 0)

    params = (same, w1, w2, w3, proj_write[0, :, 0, :], proj_read[0, :, 0, :], gain, taps_w, taps_r)
    quarter = shape((T, 256), BF16)
    outs = [shape((T, 256), F32), quarter]
    pad = pltpu.VMEM((T + 16, 768), F32)
    mine, own, far = call_kernel(
        entry_section_kernel, [quarter, *outs], 10, [pad, pltpu.VMEM((4, T, 256), F32)]
    )(where, recv, *params)
    hop = [(i, (i + 1) % sections) for i in range(sections)]
    hop_flip = [(2 * i + h, 2 * j + 1 - h) for i, j in hop for h in range(2)]
    for s in range(sections):
        got = flip(far, "tc", 1)
        mixed = (own + got.astype(F32)).astype(BF16)
        others = []
        for d in (1, 2, 3):
            others.append(lax.ppermute(mixed, ("pp", "tz", "tc"), sum_pairs(s, sections, d)))
        if s + 1 == sections:
            break
        r1, r2, r3 = [v.astype(F32) for v in others]
        branch = ((mixed.astype(F32) + r1) + (r2 + r3)).astype(BF16).astype(F32)
        produced = (mine.astype(F32) + 0.5 * branch).astype(BF16)
        a = lax.ppermute(produced, "pp", hop)
        c = lax.ppermute(produced, ("pp", "yh"), hop_flip)
        b = flip(a, "tc", 1)
        d = flip(c, "tc", 1)
        mine = a
        own, far = call_kernel(relay_section_kernel, outs, 13, [pad])(where, a, b, c, d, *params)

    (send,) = call_kernel(exit_pack_kernel, [shape((32, 8, 128), BF16)], 5)(where, mine, mixed, *others)
    recv = lax.all_to_all(send, ("pp", "ym", "yh", "tc"), 0, 0)
    (result,) = call_kernel(exit_unpack_kernel, [shape((2, T // sections, 32), BF16)], 1)(where, recv)
    return result


def solution(mesh):
    split = Mesh(
        mesh.devices.reshape(mesh.shape["pp"], 2, 2, 4, 2), ("pp", "ym", "yh", "tz", "tc")
    )
    in_specs = (
        P(None, "pp", TP + FS),
        P("pp", None),
        P("pp", None, TP, FS, None),
        P("pp", None, TP, FS, None),
        P("pp", None, TP, None),
        P("pp", None, TP, None),
        P("pp", None, None, TP, FS),
        P("pp", None, TP, FS),
        P("pp", None, TP, FS),
        P("pp", TP, FS),
        P("pp", None, TP, FS, None),
        P("pp", None, TP, None),
        P("pp", None, TP, None),
        P("pp", TP, FS, None, None),
    )
    out_specs = P(None, "pp", TP + FS)
    return jax.shard_map(
        per_device, mesh=split, in_specs=in_specs, out_specs=out_specs, check_vma=False
    )
```

```python
import jax
import jax.numpy as jnp
from jax import lax
from jax.experimental import pallas as pl
from jax.experimental.pallas import tpu as pltpu
from jax.sharding import Mesh
from jax.sharding import PartitionSpec as P


FS = ("ym", "yh")
TP = ("tz", "tc")
BLOCKS = ("pp", "tz", "tc")
EPS = 1e-06
T = 96
D = 1024
F32 = jnp.float32
BF16 = jnp.bfloat16
ROWS = 168


def lanes(shape):
    return lax.broadcasted_iota(jnp.int32, shape, len(shape) - 1)


def split3(v):
    hi = v.astype(BF16).astype(F32)
    mid = (v - hi).astype(BF16).astype(F32)
    low = v - hi - mid
    return hi, mid, low


def flag(where_ref, row, width=256):
    return where_ref[row : row + 1, :width] == 0


def permuted(v):
    group = lanes((v.shape[0], 128)) // 32
    out = []
    for h in range(2):
        for c in range(2):
            for p in range(2):
                block = None
                for g in range(4):
                    zz, m = g // 2, g % 2
                    n = (2 * p + zz) * 2 + c
                    moved = v[:, n * 128 : (n + 1) * 128]
                    turn = (64 * zz - 32 * m - 32 * h) % 128
                    if turn:
                        moved = pltpu.roll(moved, turn, 1)
                    block = moved if block is None else jnp.where(group == g, moved, block)
                out.append(block)
    return out


def pack_kernel(
    where_ref,
    micro_hbm,
    gate_hbm,
    value_hbm,
    step_hbm,
    out_hbm,
    taps_hbm,
    bias_hbm,
    decay_hbm,
    skip_hbm,
    gain_hbm,
    taps_w_hbm,
    taps_r_hbm,
    near_ref,
    away_ref,
    same_ref,
    other_ref,
    gain_out,
    taps_w_out,
    taps_r_out,
    *scratch,
):
    sources = (
        gate_hbm,
        value_hbm,
        out_hbm,
        step_hbm,
        taps_hbm,
        bias_hbm,
        decay_hbm,
        skip_hbm,
        gain_hbm,
        micro_hbm,
        taps_w_hbm,
        taps_r_hbm,
    )
    buffers, sems = (*scratch[:-1], taps_w_out, taps_r_out), scratch[-1]
    copies = [pltpu.make_async_copy(s, b, sems.at[i]) for i, (s, b) in enumerate(zip(sources, buffers))]
    for copy in copies:
        copy.start()
    for copy in copies:
        copy.wait()
    gate_ref, value_ref, out_ref, step_ref, taps_ref, bias_ref, decay_ref, skip_ref, gain_ref, micro_ref = buffers[:10]
    core = flag(where_ref, 1, 128)
    half = flag(where_ref, 0, 128)
    gate = jnp.concatenate(permuted(gate_ref[...].astype(F32)), axis=1).astype(BF16)
    value = jnp.concatenate(permuted(value_ref[...].astype(F32)), axis=1).astype(BF16)
    step = jnp.concatenate(permuted(step_ref[...].astype(F32)), axis=1)
    gain_out[...] = jnp.concatenate(permuted(gain_ref[...]), axis=1)
    blank = jnp.zeros((1, 64), F32)
    wide = lambda ref, k: jnp.broadcast_to(ref[:, k : k + 1], (1, 128))
    row_a = [taps_ref[k] for k in range(5) for _ in range(2)]
    row_a = jnp.concatenate(row_a + [wide(bias_ref, 0), wide(bias_ref, 1), blank, blank], axis=1)
    row_b = [wide(decay_ref, 0), wide(decay_ref, 1), wide(skip_ref, 0)] + [blank] * 10
    row_b = jnp.concatenate(row_b, axis=1)
    misc = jnp.concatenate([step, *split3(row_a), *split3(row_b)], axis=0).astype(BF16)
    out = permuted(out_ref[...].astype(F32))
    halves = []
    for h in range(2):
        first, second = out[4 * h : 4 * h + 2], out[4 * h + 2 : 4 * h + 4]
        own = [jnp.where(core, a, b) for a, b in zip(first, second)]
        far = [jnp.where(core, b, a) for a, b in zip(first, second)]
        halves.append(own + far)
    for ref, pair in ((same_ref, zip(*halves)), (other_ref, zip(*halves[::-1]))):
        part = jnp.concatenate([jnp.where(half, a, b) for a, b in pair], axis=1)
        ref[0:64] = gate
        ref[64:128] = value
        ref[128:160] = jnp.concatenate([part[0:32], part[32:64]], axis=1).astype(BF16)
        ref[160:168] = misc
    first = flag(where_ref, 4, 32)
    micro = [micro_ref[m].astype(F32) for m in range(2)]
    near_ref[...] = jnp.where(first, micro[0], micro[1]).astype(BF16)
    away_ref[...] = jnp.where(first, micro[1], micro[0]).astype(BF16)


def block_kernel(where_ref, r0_ref, r1_ref, r2_ref, r3_ref, send_ref):
    y = 2 * where_ref[4:5, :128] + where_ref[0:1, :128]
    group = lanes((24, 128)) // 32
    blank = jnp.zeros((24, 96), F32)
    block = jnp.zeros((24, 128), F32)
    for bits, ref in enumerate((r0_ref, r1_ref, r2_ref, r3_ref)):
        wide = jnp.concatenate([ref[...].astype(F32), blank], axis=1)
        for k in range(4):
            moved = wide if k == 0 else pltpu.roll(wide, 32 * k, 1)
            block = jnp.where((group == k) & ((y ^ bits) == group), moved, block)
    block = block.astype(BF16)
    for peer in range(32):
        send_ref[peer] = block


def nt_dot(a, b):
    return lax.dot_general(a, b, (((1,), (1,)), ((), ())), preferred_element_type=F32)


def nn_dot(a, b):
    return lax.dot_general(a, b, (((1,), (0,)), ((), ())), preferred_element_type=F32)


def silu(v):
    return v * jax.nn.sigmoid(v)


def section_body(quarters, weight_refs, write_ref, read_ref, gain_ref, taps_refs, own_ref, far_ref, pad_ref):
    low = lanes((T, 128)) < 64
    total = None
    for pair in quarters:
        for q in pair:
            sq = q * q
            sq = sq[:, :128] + sq[:, 128:]
            total = sq if total is None else total + sq
    scale = lax.rsqrt(jnp.sum(total, axis=1, keepdims=True) * (1.0 / D) + EPS)
    blocks = []
    for h in range(2):
        for c in range(2):
            n = (2 * h + c) * 256
            blocks.append((quarters[h][c] * scale * gain_ref[:, n : n + 256]).astype(BF16))
    normed = jnp.concatenate(blocks, axis=1)

    step_rows = jnp.concatenate([w[160:168].astype(F32)[0:2] for w in weight_refs], axis=0)
    step_raw = nt_dot(step_rows.astype(BF16), normed)
    small = []
    for w in weight_refs:
        misc = w[160:168].astype(F32)
        small.append((misc[2:3] + misc[3:4] + misc[4:5], misc[5:6] + misc[6:7] + misc[7:8]))
    bias = jnp.concatenate([s[0][:, 640 + 128 * d : 640 + 128 * d + T] for s in small for d in range(2)], axis=0)
    decay = jnp.concatenate([s[1][:, 128 * d : 128 * d + T] for s in small for d in range(2)], axis=0)
    raw = step_raw + bias
    dt = jnp.maximum(raw, 0.0) + jnp.log1p(jnp.exp(-jnp.abs(raw)))
    log_decay = dt * (-jnp.exp(decay))
    parts = [s.astype(BF16) for s in split3(log_decay)]
    row_id = lax.broadcasted_iota(jnp.int32, (T, T), 0)
    col_id = lax.broadcasted_iota(jnp.int32, (T, T), 1)
    upto = (row_id <= col_id).astype(F32).astype(BF16)
    since = (row_id >= col_id).astype(F32).astype(BF16)
    fwd_all = (nn_dot(parts[0], upto) + nn_dot(parts[1], upto)) + nn_dot(parts[2], upto)
    bwd_all = (nn_dot(parts[0], since) + nn_dot(parts[1], since)) + nn_dot(parts[2], since)
    odd = lax.broadcasted_iota(jnp.int32, (8, T), 0) % 2 == 1
    cum = jnp.where(odd, bwd_all, fwd_all)
    cum_pad = jnp.concatenate([cum, jnp.zeros((8, 128 - T), F32)], axis=1)
    cum_cols = cum_pad.T[:T]

    wr_rows = [
        jnp.concatenate([r[n * 128 + y * 32 : n * 128 + y * 32 + 32] for r in (write_ref, read_ref)], axis=1)
        for h in range(2)
        for c in range(2)
        for n in (c, 2 + c, 4 + c, 6 + c)
        for y in (h, 2 + h)
    ]
    wr = nn_dot(normed, jnp.concatenate(wr_rows, axis=0))
    pad_ref[0:8, 0:512] = jnp.zeros((8, 512), F32)
    pad_ref[8 + T : 16 + T, 0:512] = jnp.zeros((8, 512), F32)
    for i in range(2):
        pair = weight_refs[2 * i : 2 * i + 2]
        rows = jnp.concatenate([w[k * 64 : k * 64 + 64] for k in range(2) for w in pair], axis=0)
        gate_value = nt_dot(normed, rows).astype(BF16).astype(F32)
        pad_ref[8 : 8 + T, 512 + 128 * i : 640 + 128 * i] = gate_value[:, :128]
        pad_ref[8 : 8 + T, 128 * i : 128 * i + 128] = gate_value[:, 128:]
    pad_ref[8 : 8 + T, 256:512] = wr.astype(BF16).astype(F32)
    low_row = lanes((1, 128)) < 64
    acts = []
    for g in range(4):
        span = slice(g * 128, (g + 1) * 128)
        acc = None
        for k in range(5):
            if g < 2:
                tap = jnp.where(low_row, *[small[2 * g + e][0][:, k * 128 : (k + 1) * 128] for e in range(2)])
            else:
                tap = taps_refs[g - 2][k]
            term = pad_ref[6 + k : 6 + k + T, span] * tap
            acc = term if acc is None else acc + term
        acts.append(silu(acc).astype(BF16))
    scores = nt_dot(acts[3], acts[2])
    lower = row_id >= col_id
    diagonal = row_id == col_id
    pairs = []
    for i in range(2):
        high, rest = [], []
        for j in (2 * i, 2 * i + 1):
            fc = cum_cols[:, 2 * j : 2 * j + 1]
            bc = cum_cols[:, 2 * j + 1 : 2 * j + 2]
            fr = cum[2 * j : 2 * j + 1]
            br = cum[2 * j + 1 : 2 * j + 2]
            d0 = dt[2 * j : 2 * j + 1]
            d1 = dt[2 * j + 1 : 2 * j + 2]
            mix = jnp.exp(jnp.where(lower, fc - fr, bc - br)) * jnp.where(lower, d0, d1)
            mix = mix + jnp.where(diagonal, d1, 0.0)
            combined = scores * mix
            high.append(combined.astype(BF16))
            rest.append((combined - high[-1].astype(F32)).astype(BF16))
        y = nn_dot(jnp.concatenate(high + rest, axis=0), acts[i])
        y = y[: 2 * T] + y[2 * T :]
        skip = jnp.where(low_row, *[small[2 * i + e][1][:, 256:384] for e in range(2)])
        y = jnp.where(low, y[:T], y[T:]) + skip * acts[i].astype(F32)
        gate = pad_ref[8 : 8 + T, 512 + 128 * i : 640 + 128 * i]
        pairs.append((y * silu(gate)).astype(BF16))
    gated_all = jnp.concatenate(pairs, axis=1)
    for side, ref in ((0, own_ref), (1, far_ref)):
        weight = jnp.concatenate(
            [
                w[128:160, 512 * r + 256 * side : 512 * r + 256 * side + 256]
                for w in weight_refs
                for r in range(2)
            ],
            axis=0,
        )
        ref[...] = nn_dot(gated_all, weight).astype(ref.dtype)


def entry_section_kernel(where_ref, recv_ref, *refs):
    *rest, quarter_out, own_ref, far_ref, pad_ref, quarter_ref = refs
    tokens = [
        jnp.concatenate([recv_ref[x * 8 + n].astype(F32) for x in range(4)], axis=0) for n in range(8)
    ]
    blocks = permuted(jnp.concatenate(tokens, axis=1))
    for q in range(4):
        quarter_ref[q] = jnp.concatenate(blocks[2 * q : 2 * q + 2], axis=1)
    quarters = [[quarter_ref[2 * h + c] for c in range(2)] for h in range(2)]
    half, core = flag(where_ref, 0), flag(where_ref, 1)
    mine = jnp.where(half, jnp.where(core, *quarters[0]), jnp.where(core, *quarters[1]))
    quarter_out[...] = mine.astype(BF16)
    section_body(quarters, rest[0:4], *rest[4:7], rest[7:9], own_ref, far_ref, pad_ref)


def relay_section_kernel(where_ref, a_ref, b_ref, c_ref, d_ref, *refs):
    *rest, own_ref, far_ref, pad_ref = refs
    half, core = flag(where_ref, 0), flag(where_ref, 1)
    a, b, c, d = [r[...].astype(F32) for r in (a_ref, b_ref, c_ref, d_ref)]
    own0, own1 = jnp.where(half, a, c), jnp.where(half, c, a)
    far0, far1 = jnp.where(half, b, d), jnp.where(half, d, b)
    quarters = [
        [jnp.where(core, own0, far0), jnp.where(core, far0, own0)],
        [jnp.where(core, own1, far1), jnp.where(core, far1, own1)],
    ]
    section_body(quarters, rest[0:4], *rest[4:7], rest[7:9], own_ref, far_ref, pad_ref)


def exit_pack_kernel(where_ref, mine_ref, m0_ref, m1_ref, m2_ref, m3_ref, send_ref):
    branch = (m0_ref[...].astype(F32) + m1_ref[...].astype(F32)) + (m2_ref[...].astype(F32) + m3_ref[...].astype(F32))
    branch = branch.astype(BF16).astype(F32)
    final = (mine_ref[...].astype(F32) + 0.5 * branch).astype(BF16).astype(F32)
    squares = final * final
    squares = jnp.sum(squares[:, :128] + squares[:, 128:], axis=1, keepdims=True)
    squares = jnp.broadcast_to(squares, (T, 128))
    own = jnp.where(flag(where_ref, 2, 128), final[:, :128], final[:, 128:])
    own = jnp.where(flag(where_ref, 3, 128), own, pltpu.roll(own, 64, 1))
    turned = {d: own if d == 0 else pltpu.roll(own, (32 * d) % 128, 1) for d in (-1, 0, 1, 2, 3)}
    lane = lanes((6, 128))
    group = lane // 32
    spot = lane % 32 == lax.broadcasted_iota(jnp.int32, (6, 128), 0)
    for x in range(4):
        rows = [slice(x * 24 + k * 6, x * 24 + k * 6 + 6) for k in range(4)]
        total = squares[rows[0]]
        for k in range(1, 4):
            total = jnp.where(group == k, squares[rows[k]], total)
        total = jnp.sum(jnp.where(spot, total, 0.0), axis=0, keepdims=True)
        parts = split3(total)
        for m in range(2):
            block = turned[-m][rows[0]]
            for k in range(1, 4):
                block = jnp.where(group == k, turned[k - m][rows[k]], block)
            message = jnp.concatenate([block, parts[0], parts[1]], axis=0).astype(BF16)
            for peer in range(4):
                send_ref[(x * 2 + m) * 4 + peer] = message


def exit_unpack_kernel(where_ref, recv_ref, out_ref):
    half, core = flag(where_ref, 0, 128), flag(where_ref, 1, 128)
    lane = lanes((8, 128))
    spot = lane % 32 == lax.broadcasted_iota(jnp.int32, (8, 128), 0)
    same_group = (
        lax.broadcasted_iota(jnp.int32, (128, 128), 0) // 32 == lanes((128, 128)) // 32
    ).astype(F32).astype(BF16)
    parts = []
    for m in range(2):
        first = (6 + m) * 4
        sums = [recv_ref[first + i].astype(F32) for i in range(4)]
        total = (sums[0][6:7] + sums[0][7:8]) + (sums[1][6:7] + sums[1][7:8])
        total = total + ((sums[2][6:7] + sums[2][7:8]) + (sums[3][6:7] + sums[3][7:8]))
        parts += split3(jnp.where(spot, jnp.broadcast_to(total, (8, 128)), 0.0))
    spread = nn_dot(jnp.concatenate(parts, axis=0).astype(BF16), same_group)
    for m in range(2):
        total = (spread[24 * m : 24 * m + 8] + spread[24 * m + 8 : 24 * m + 16]) + spread[24 * m + 16 : 24 * m + 24]
        blocks = [recv_ref[(6 + m) * 4 + i].astype(F32) for i in range(4)]
        block = jnp.where(half, jnp.where(core, *blocks[:2]), jnp.where(core, *blocks[2:]))
        block = block * lax.rsqrt(total * (1.0 / D) + EPS)
        rows = [block if k == 0 else pltpu.roll(block, 128 - 32 * k, 1) for k in range(4)]
        out_ref[m] = jnp.concatenate([r[:6, :32] for r in rows], axis=0).astype(BF16)


VMEM_SPEC = pl.BlockSpec(memory_space=pltpu.VMEM)


def call_kernel(kernel, out_shape, count, scratch=()):
    return pl.pallas_call(
        kernel,
        out_shape=out_shape,
        in_specs=[VMEM_SPEC] + [VMEM_SPEC] * count,
        out_specs=[VMEM_SPEC] * len(out_shape),
        scratch_shapes=scratch,
        compiler_params=pltpu.CompilerParams(vmem_limit_bytes=24 * 1024 * 1024),
    )


def flip(v, axes, bits):
    size = lax.axis_size(axes)
    return lax.ppermute(v, axes, [(i, i ^ bits) for i in range(size)])


def sum_pairs(active, sections, bits):
    pairs = []
    for i in range(sections):
        for z in range(4):
            for c in range(2):
                target = 2 * (z ^ bits) + c if i == active else 2 * z + 1 - c
                pairs.append((8 * i + 2 * z + c, 8 * i + target))
    return pairs


def per_device(
    micro_in,
    norm_gain,
    proj_gate,
    proj_value,
    proj_write,
    proj_read,
    proj_step,
    step_bias,
    decay_log,
    skip_gain,
    conv_value,
    conv_write,
    conv_read,
    proj_out,
):
    sections = lax.axis_size("pp")
    half = lax.axis_index("yh")
    micro = lax.axis_index("ym")
    core = lax.axis_index("tc")
    zpos = lax.axis_index("tz")
    where = jnp.stack([half, core, zpos // 2, zpos % 2, micro]).astype(jnp.int32)
    where = jnp.broadcast_to(where[:, None], (5, 256))

    shape = jax.ShapeDtypeStruct
    raw = (
        micro_in,
        proj_gate[0, :, 0, 0, :].T,
        proj_value[0, :, 0, 0, :].T,
        proj_step[0, :, :, 0, 0].T,
        proj_out[0, 0, 0],
        conv_value.reshape(5, 1, 64),
        step_bias.reshape(1, 2),
        decay_log.reshape(1, 2),
        skip_gain.reshape(1, 1),
        norm_gain,
        conv_write.reshape(5, 1, 128),
        conv_read.reshape(5, 1, 128),
    )
    order = (1, 2, 4, 3, 5, 6, 7, 8, 9, 0)
    near, away, same, other, gain, taps_w, taps_r = pl.pallas_call(
        pack_kernel,
        out_shape=[
            shape((T // 4, 32), BF16),
            shape((T // 4, 32), BF16),
            shape((ROWS, D), BF16),
            shape((ROWS, D), BF16),
            shape((1, D), F32),
            shape((5, 1, 128), F32),
            shape((5, 1, 128), F32),
        ],
        in_specs=[VMEM_SPEC] + [pl.BlockSpec(memory_space=pltpu.HBM)] * len(raw),
        out_specs=[VMEM_SPEC] * 7,
        scratch_shapes=[pltpu.VMEM(raw[i].shape, raw[i].dtype) for i in order]
        + [pltpu.SemaphoreType.DMA((len(raw),))],
        compiler_params=pltpu.CompilerParams(vmem_limit_bytes=24 * 1024 * 1024),
    )(where, *[pltpu.with_memory_space_constraint(v, pltpu.HBM) if i != 8 else v for i, v in enumerate(raw)])
    r1 = flip(near, FS, 1)
    r2 = flip(away, FS, 2)
    r3 = flip(away, FS, 3)
    w1 = flip(other, FS, 1)
    w2 = flip(same, FS, 2)
    w3 = flip(other, FS, 3)
    (send,) = call_kernel(block_kernel, [shape((32, T // 4, 128), BF16)], 4)(where, near, r1, r2, r3)
    recv = lax.all_to_all(send, BLOCKS, 0, 0)

    params = (same, w1, w2, w3, proj_write[0, :, 0, :], proj_read[0, :, 0, :], gain, taps_w, taps_r)
    quarter = shape((T, 256), BF16)
    outs = [shape((T, 256), F32), quarter]
    pad = pltpu.VMEM((T + 16, 768), F32)
    mine, own, far = call_kernel(
        entry_section_kernel, [quarter, *outs], 10, [pad, pltpu.VMEM((4, T, 256), F32)]
    )(where, recv, *params)
    hop = [(i, (i + 1) % sections) for i in range(sections)]
    hop_flip = [(2 * i + h, 2 * j + 1 - h) for i, j in hop for h in range(2)]
    for s in range(sections):
        got = flip(far, "tc", 1)
        mixed = (own + got.astype(F32)).astype(BF16)
        others = []
        for d in (1, 2, 3):
            others.append(lax.ppermute(mixed, ("pp", "tz", "tc"), sum_pairs(s, sections, d)))
        if s + 1 == sections:
            break
        r1, r2, r3 = [v.astype(F32) for v in others]
        branch = ((mixed.astype(F32) + r1) + (r2 + r3)).astype(BF16).astype(F32)
        produced = (mine.astype(F32) + 0.5 * branch).astype(BF16)
        a = lax.ppermute(produced, "pp", hop)
        c = lax.ppermute(produced, ("pp", "yh"), hop_flip)
        b = flip(a, "tc", 1)
        d = flip(c, "tc", 1)
        mine = a
        own, far = call_kernel(relay_section_kernel, outs, 13, [pad])(where, a, b, c, d, *params)

    (send,) = call_kernel(exit_pack_kernel, [shape((32, 8, 128), BF16)], 5)(where, mine, mixed, *others)
    recv = lax.all_to_all(send, ("pp", "ym", "yh", "tc"), 0, 0)
    (result,) = call_kernel(exit_unpack_kernel, [shape((2, T // sections, 32), BF16)], 1)(where, recv)
    return result


def solution(mesh):
    split = Mesh(
        mesh.devices.reshape(mesh.shape["pp"], 2, 2, 4, 2), ("pp", "ym", "yh", "tz", "tc")
    )
    in_specs = (
        P(None, "pp", TP + FS),
        P("pp", None),
        P("pp", None, TP, FS, None),
        P("pp", None, TP, FS, None),
        P("pp", None, TP, None),
        P("pp", None, TP, None),
        P("pp", None, None, TP, FS),
        P("pp", None, TP, FS),
        P("pp", None, TP, FS),
        P("pp", TP, FS),
        P("pp", None, TP, FS, None),
        P("pp", None, TP, None),
        P("pp", None, TP, None),
        P("pp", TP, FS, None, None),
    )
    out_specs = P(None, "pp", TP + FS)
    return jax.shard_map(
        per_device, mesh=split, in_specs=in_specs, out_specs=out_specs, check_vma=False
    )
```
